32 devices in a mesh: fs: 8 (over z, y), tp: 4 (over x, core).
Axes of the slice: x: 2, y: 2, z: 4, core: 2. Of those that a mesh axis runs over, the one named last changes fastest.
Arguments:
- stream: bfloat16 [3072, 2048], P('fs', 'tp'), may hold values from -3 to 3
- gain_first: float32 [2048], replicated, may hold values from 0.1 to 1.9
- gain_mixer: float32 [2048], replicated, may hold values from 0.1 to 1.9
- gain_second: float32 [2048], replicated, may hold values from 0.1 to 1.9
- gate_weight: float32 [2048, 5632], P('fs', 'tp'), may hold values from -0.125 to 0.125
- gate_scale: float32 [5632], P('tp'), may hold values from 0.5 to 2
- up_weight: float32 [2048, 5632], P('fs', 'tp'), may hold values from -0.125 to 0.125
- up_scale: float32 [5632], P('tp'), may hold values from 0.5 to 2
- down_weight: float32 [5632, 2048], P('tp', 'fs'), may hold values from -0.109375 to 0.109375
- down_scale: float32 [2048], P('tp'), may hold values from 0.5 to 2
- pool_in_weight: float32 [2048, 512], P('fs', 'tp'), may hold values from -0.125 to 0.125
- pool_in_scale: float32 [512], P('tp'), may hold values from 0.5 to 2
- pool_out_weight: float32 [512, 2048], P('tp', 'fs'), may hold values from -0.375 to 0.375
- pool_out_scale: float32 [2048], P('tp'), may hold values from 0.5 to 2
Outputs:
- layer_out: bfloat16 [3072, 2048], P('fs', 'tp')
The draws below stay inside these ranges and needn't reach their ends.
All inputs are finite; a program needn't handle non-finite values.
Results may differ from the reference program's by a relative error of at most 0.025.
Values may be sent and summed in bfloat16 or wider, within the bound.
A program may use at most 64 MiB of HBM per device.

```python
import math
import jax
import jax.numpy as jnp
from jax import lax

D = 2048
FF = 5632
P_SIZE = 512
SEQ = 128
TOKENS = 3072
N_TP = 4


def strengthened(drawn, rng, source, target, blocks, factor):
    owner, partner = [(jnp.arange(drawn.shape[dim]) // (drawn.shape[dim] // blocks)).reshape([-1 if axis == dim else 1 for axis in range(drawn.ndim)]) for dim in (source, target)]
    chosen = jax.random.permutation(rng, blocks)[partner]
    strong = (owner == chosen) | (owner == (partner + blocks // 2) % blocks)
    return jnp.where(strong, factor * drawn, drawn)


def level_of(stream_key, extent, cuts, least, top_value):
    level, own = 1.0, jax.random.fold_in(stream_key, 6)
    for axis_at, blocks in cuts:
        steps = jnp.exp(jax.random.uniform(jax.random.fold_in(own, axis_at), (blocks,), jnp.float32, least / len(cuts), top_value / len(cuts)))
        level = level * jnp.repeat(steps, extent[axis_at] // blocks).reshape([-1 if axis == axis_at else 1 for axis in range(len(extent))])
    return level


def normal_values(own_key, extent, scale, limit, cuts=(), kind=jnp.bfloat16):
    values = jax.random.normal(own_key, extent, jnp.float32) * scale
    if len(cuts) > 0:
        values = level_of(own_key, extent, cuts, -0.22, 0.18) * values
    return jnp.clip(values, min=-limit, max=limit).astype(kind)


def heavy_noise(key, shape, width, bound, pieces, heavy, dtype=jnp.bfloat16):
    result = width * jax.random.normal(key, shape, jnp.float32)
    if pieces:
        result = result * level_of(key, shape, pieces, -0.22, 0.18)
    return jnp.clip(strengthened(result, jax.random.fold_in(key, 3), *heavy), -bound, bound).astype(dtype)


def setup_inputs(seed: int = 0) -> dict:
    streams_of = jax.random.split(jax.random.key(seed), 15)
    return {
        "stream": normal_values(streams_of[0], (TOKENS, D), 0.5, 3.0, ((0, 8), (1, 4))),
        "gain_first": jnp.clip(1.0 + 0.18 * jax.random.normal(streams_of[1], (D,), jnp.float32), 0.1, 1.9),
        "gain_mixer": jnp.clip(1.0 + 0.18 * jax.random.normal(streams_of[2], (D,), jnp.float32), 0.1, 1.9),
        "gain_second": jnp.clip(1.0 + 0.18 * jax.random.normal(streams_of[3], (D,), jnp.float32), 0.1, 1.9),
        "gate_weight": normal_values(streams_of[4], (D, FF), D ** -0.5, 0.125, ((0, 8), (1, 4)), jnp.float32),
        "gate_scale": jnp.clip(jnp.exp(math.log(2.0) - 1.3862944 * jax.random.uniform(streams_of[5], (FF,), jnp.float32) ** level_of(streams_of[5], (FF,), ((0, 4),), -0.2, 0.2)), 0.5, 2.0),
        "up_weight": normal_values(streams_of[6], (D, FF), D ** -0.5, 0.125, ((0, 8), (1, 4)), jnp.float32),
        "up_scale": jnp.clip(jnp.exp(math.log(2.0) - 1.3862944 * jax.random.uniform(streams_of[7], (FF,), jnp.float32) ** level_of(streams_of[7], (FF,), ((0, 4),), -0.2, 0.2)), 0.5, 2.0),
        "down_weight": heavy_noise(streams_of[8], (FF, D), FF ** -0.5, 0.109375, ((0, 4), (1, 8)), (0, 1, 8, 2.0), jnp.float32),
        "down_scale": jnp.clip(jnp.exp(math.log(2.0) - 1.3862944 * jax.random.uniform(streams_of[9], (D,), jnp.float32) ** level_of(streams_of[9], (D,), ((0, 4),), -0.2, 0.2)), 0.5, 2.0),
        "pool_in_weight": normal_values(streams_of[10], (D, P_SIZE), D ** -0.5, 0.125, ((0, 8), (1, 4)), jnp.float32),
        "pool_in_scale": jnp.clip(jnp.exp(math.log(2.0) - 1.3862944 * jax.random.uniform(streams_of[11], (P_SIZE,), jnp.float32) ** level_of(streams_of[11], (P_SIZE,), ((0, 4),), -0.2, 0.2)), 0.5, 2.0),
        "pool_out_weight": heavy_noise(streams_of[12], (P_SIZE, D), P_SIZE ** -0.5, 0.375, ((0, 4), (1, 8)), (0, 1, 8, 2.0), jnp.float32),
        "pool_out_scale": jnp.clip(jnp.exp(math.log(2.0) - 1.3862944 * jax.random.uniform(streams_of[13], (D,), jnp.float32) ** level_of(streams_of[13], (D,), ((0, 4),), -0.2, 0.2)), 0.5, 2.0),
    }


eps = 1e-06
WINDOWS = (2, 4, 8, 16)

def rms_norm(values, norm_gain):
    floats = values.astype(jnp.float32)
    scaled = floats * lax.rsqrt(lax.optimization_barrier(jnp.mean(floats * floats, axis=-1, keepdims=True)) + eps)
    return (scaled * norm_gain).astype(jnp.bfloat16)

def block_sum(left_rows, right_rows, column_scale):
    block_rows = right_rows.shape[0] // N_TP
    running = jnp.zeros((left_rows.shape[0], right_rows.shape[1]), jnp.float32)
    for blocks in range(N_TP):
        block_part = jnp.dot(left_rows[:, blocks * block_rows:(blocks + 1) * block_rows], right_rows[blocks * block_rows:(blocks + 1) * block_rows], preferred_element_type=jnp.float32).astype(jnp.bfloat16)
        block_part = lax.optimization_barrier(block_part)
        running = running + block_part.astype(jnp.float32)
    return running * column_scale

def feed_forward(normed, gate_half, gate_scale, up_half, up_scale, down_half, down_scale):
    gate_sum = jnp.dot(normed, gate_half, preferred_element_type=jnp.float32) * gate_scale
    up_sum = jnp.dot(normed, up_half, preferred_element_type=jnp.float32) * up_scale
    hidden = (jax.nn.silu(gate_sum) * up_sum).astype(jnp.bfloat16)
    return block_sum(hidden, down_half, down_scale)

def pooling(pool_input):
    channels = pool_input.shape[1]
    floats = pool_input.astype(jnp.float32).reshape(-1, SEQ, channels)
    csum = jnp.concatenate([jnp.zeros((floats.shape[0], 1, channels), jnp.float32), jnp.cumsum(floats, axis=1)], axis=1)
    position = jnp.arange(SEQ)
    channel_group = jnp.arange(channels) * 4 // channels
    pooled = -floats
    for group_index, window in enumerate(WINDOWS):
        before = window // 2
        after_span = window - before
        upper_sum = jnp.pad(csum, ((0, 0), (0, after_span), (0, 0)), mode='edge')[:, after_span:after_span + SEQ]
        lower_sum = jnp.pad(csum, ((0, 0), (before, 0), (0, 0)), mode='edge')[:, :SEQ]
        counts = (jnp.minimum(position + after_span, SEQ) - jnp.maximum(position - before, 0)).astype(jnp.float32)
        window_mean = (upper_sum - lower_sum) / counts[None, :, None]
        select = (channel_group == group_index).astype(jnp.float32)
        pooled = pooled + window_mean * select
    return pooled.reshape(-1, channels).astype(jnp.bfloat16)

def reference(stream, gain_first, gain_mixer, gain_second, gate_weight, gate_scale, up_weight, up_scale, down_weight, down_scale, pool_in_weight, pool_in_scale, pool_out_weight, pool_out_scale):
    gate_half = gate_weight.astype(jnp.bfloat16)
    up_half = up_weight.astype(jnp.bfloat16)
    down_half = down_weight.astype(jnp.bfloat16)
    in_half = pool_in_weight.astype(jnp.bfloat16)
    out_half = pool_out_weight.astype(jnp.bfloat16)
    first_branch = feed_forward(rms_norm(stream, gain_first), gate_half, gate_scale, up_half, up_scale, down_half, down_scale)
    after_first = (stream.astype(jnp.float32) + 0.5 * first_branch).astype(jnp.bfloat16)
    mixer_normed = rms_norm(after_first, gain_mixer)
    pool_input = (jnp.dot(mixer_normed, in_half, preferred_element_type=jnp.float32) * pool_in_scale).astype(jnp.bfloat16)
    pooled = pooling(pool_input)
    after_mix = (after_first.astype(jnp.float32) + block_sum(pooled, out_half, pool_out_scale)).astype(jnp.bfloat16)
    second_branch = feed_forward(rms_norm(after_mix, gain_second), gate_half, gate_scale, up_half, up_scale, down_half, down_scale)
    return (after_mix.astype(jnp.float32) + 0.5 * second_branch).astype(jnp.bfloat16)
```

```python
import functools

import jax
import jax.numpy as jnp
from jax import lax
from jax.experimental import pallas as pl
from jax.experimental.pallas import tpu as pltpu
from jax.sharding import PartitionSpec as P

SEQ = 128
MESH = pl.DeviceIdType.MESH

eps = 1e-06
WINDOWS = (2, 4, 8, 16)


def fs_grid(count):
    ny = 1
    while (2 * ny) * (2 * ny) <= count and count % (2 * ny) == 0:
        ny *= 2
    return ny, count // ny


def grid_shape(row_blocks, col_blocks, block):
    rows, cols = block
    if cols % 128 == 0:
        return (row_blocks * rows, col_blocks * cols)
    return (row_blocks, col_blocks, rows, cols)


def place(whole, block, row_block, col_block, part=(0, None)):
    rows, cols = block
    first, count = part[0], rows if part[1] is None else part[1]
    if len(whole.shape) == 2:
        return whole.at[
            pl.ds(pl.multiple_of(row_block * rows + first, 16), count),
            pl.ds(pl.multiple_of(col_block * cols, 128), cols),
        ]
    return whole.at[row_block, col_block, pl.ds(first, count)]


def flat(whole):
    if whole.ndim == 2:
        return whole
    return whole.transpose(0, 2, 1, 3).reshape(whole.shape[0] * whole.shape[2], -1)


def gather_kernel(nfs, ntp, pool_in, pool_out, gate, up, down, stream, scales,
                  in_all, out_all, gate_all, up_all, down_all, stream_all, scales_all,
                  send_sem, recv_sem, local_sem, tsend, trecv, psend, precv, ssend, srecv):
    ny, nz = fs_grid(nfs)
    nx = ntp // 2
    fs, tp = lax.axis_index("fs"), lax.axis_index("tp")
    z, y = fs // ny, fs % ny
    x, core = tp // 2, tp % 2
    partner = x * 2 + (1 - core)
    alternate = ny == 2 and nz > 1

    barrier = pltpu.get_barrier_semaphore()

    def greet(cond, f, t):
        @pl.when(cond)
        def _():
            pl.semaphore_signal(barrier, inc=1, device_id={"fs": f, "tp": t}, device_id_type=MESH)

    greet(z > 0, fs - ny, tp)
    greet(z < nz - 1, fs + ny, tp)
    greet(y > 0, fs - 1, tp)
    greet(y < ny - 1, fs + 1, tp)
    for k in range(1, ntp):
        pl.semaphore_signal(
            barrier, inc=1, device_id={"fs": fs, "tp": (tp + k) % ntp}, device_id_type=MESH
        )
    peers = ntp - 1
    for cond in (z > 0, z < nz - 1, y > 0, y < ny - 1):
        peers = peers + jnp.where(cond, 1, 0)
    pl.semaphore_wait(barrier, peers)

    pieces = [
        (lambda: pool_in, lambda f: place(in_all, pool_in.shape, f, tp)),
        (lambda: pool_out, lambda f: place(out_all, pool_out.shape, tp, f)),
    ]
    npool = len(pieces)
    for own, whole, by_rows in ((gate, gate_all, True), (up, up_all, True), (down, down_all, False)):
        rows = own.shape[0]
        halves = 2 if alternate else 1
        for h in range(halves):
            part = (h * (rows // halves), rows // halves)

            def own_part(own=own, part=part):
                return own.at[pl.ds(*part)]

            def whole_part(f, own=own, whole=whole, part=part, by_rows=by_rows):
                return place(whole, own.shape, f if by_rows else 0, 0 if by_rows else f, part)

            pieces.append((own_part, whole_part))
    started = []

    def remote(piece, f, direction, target, mine=False):
        own, whole = pieces[piece]
        return pltpu.make_async_remote_copy(
            src_ref=own() if mine else whole(f),
            dst_ref=whole(f),
            send_sem=send_sem.at[piece, f, direction],
            recv_sem=recv_sem.at[piece, f],
            device_id={"fs": target, "tp": tp},
            device_id_type=MESH,
        )

    def send(cond, piece, f, direction, mine=False):
        target = fs + (-ny, ny, -1, 1)[direction]

        @pl.when(cond)
        def _():
            remote(piece, f, direction, target, mine).start()

        started.append((cond, piece, f, direction, target, mine))

    def arrived(cond, piece, f):
        @pl.when(cond)
        def _():
            remote(piece, f, 0, fs, False).wait_recv()

    def by_y(cond, piece, f, mine=False):
        send(cond & (y > 0), piece, f, 2, mine)
        send(cond & (y < ny - 1), piece, f, 3, mine)

    yes = z >= 0

    def stream_place(slot):
        return place(stream_all, stream.shape, 0, slot)

    def stream_copy(src, slot, t_target, k):
        return pltpu.make_async_remote_copy(
            src_ref=src, dst_ref=stream_place(slot), send_sem=tsend.at[k], recv_sem=trecv.at[slot],
            device_id={"fs": fs, "tp": t_target}, device_id_type=MESH)

    def slab(which, slot):
        if which == 0:
            if len(in_all.shape) == 2:
                cols = pool_in.shape[1]
                return in_all.at[:, pl.ds(pl.multiple_of(slot * cols, 128), cols)]
            return in_all.at[:, slot]
        if len(out_all.shape) == 2:
            rows = pool_out.shape[0]
            return out_all.at[pl.ds(pl.multiple_of(slot * rows, 16), rows)]
        return out_all.at[slot]

    def pool_copy(which, slot, t_target, k):
        return pltpu.make_async_remote_copy(
            src_ref=slab(which, slot), dst_ref=slab(which, slot),
            send_sem=psend.at[which, k], recv_sem=precv.at[which, slot],
            device_id={"fs": fs, "tp": t_target}, device_id_type=MESH)

    def scale_copy(k, slot, t_target):
        return pltpu.make_async_remote_copy(
            src_ref=scales, dst_ref=scales_all.at[slot], send_sem=ssend.at[k], recv_sem=srecv.at[slot],
            device_id={"fs": fs, "tp": t_target}, device_id_type=MESH)

    npieces = len(pieces)
    locals_ = [pltpu.make_async_copy(own(), whole(fs), local_sem.at[i]) for i, (own, whole) in enumerate(pieces)]
    locals_.append(pltpu.make_async_copy(stream, stream_place(tp), local_sem.at[npieces]))
    locals_.append(pltpu.make_async_copy(scales, scales_all.at[tp], local_sem.at[npieces + 1]))
    for piece in range(npieces):
        send(z > 0, piece, fs, 0, True)
        send(z < nz - 1, piece, fs, 1, True)
        by_y(yes, piece, fs, True)
    stream_sends = []
    for k in range(1, nx):
        stream_sends.append(stream_copy(stream, tp, (x + k) % nx * 2 + core, k - 1))
    stream_sends.append(stream_copy(stream, tp, partner, nx - 1))
    stream_sends += [scale_copy(k - 1, tp, (tp + k) % ntp) for k in range(1, ntp)]
    for copy in stream_sends:
        copy.start()
    for copy in locals_:
        copy.start()

    def row_arrivals(piece, d, alt):
        low, high = fs - d * ny, fs + d * ny
        has_low, has_high = z >= d, z + d <= nz - 1
        for cond, f, direction, ahead, end in (
            (has_low, low, 1, z < nz - 1, z == d),
            (has_high, high, 0, z > 0, z + d == nz - 1),
        ):
            arrived(cond, piece, f)
            send(cond & ahead, piece, f, direction)
            if alt:
                by_y(cond & jnp.logical_not(end), piece, f)
                other = f + 1 - 2 * y
                arrived(cond & end, piece, other)
                send(cond & end & ahead, piece, other, direction)
            else:
                by_y(cond, piece, f)

    def column_arrivals(piece, alt):
        for d in range(nz):
            for sign in ((1,) if d == 0 else (-1, 1)):
                row_ok = (z + sign * d >= 0) & (z + sign * d <= nz - 1)
                if alt:
                    at = z + sign * d
                    if d == 0:
                        continue
                    row_ok = row_ok & (at != 0) & (at != nz - 1)
                base = fs + sign * d * ny
                for e in range(1, ny):
                    for step, direction, ok, ahead in (
                        (-e, 3, y >= e, y < ny - 1),
                        (e, 2, y + e <= ny - 1, y > 0),
                    ):
                        arrived(row_ok & ok, piece, base + step)
                        if ny > 2:
                            send(row_ok & ok & ahead, piece, base + step, direction)

    is_alt = [alternate and p >= npool and p % 2 == 1 for p in range(npieces)]

    for d in range(1, nz):
        for p in range(npool):
            row_arrivals(p, d, False)
    pool_sends = []
    for p in range(npool):
        column_arrivals(p, False)
        locals_[p].wait()
        pool_sends += [pool_copy(p, tp, (x + k) % nx * 2 + core, k - 1) for k in range(1, nx)]
        pool_sends.append(pool_copy(p, tp, partner, nx - 1))
    for copy in pool_sends:
        copy.start()
    for k in range(1, nx):
        slot = (x + k) % nx * 2 + core
        stream_copy(stream, slot, partner, 0).wait_recv()
        copy = stream_copy(stream_place(slot), slot, partner, nx - 1 + k)
        copy.start()
        stream_sends.append(copy)

    for p in range(npieces):
        if is_alt[p]:
            other = fs + 1 - 2 * y
            arrived(yes, p, other)
            send(z == 0, p, other, 1)
            send(z == nz - 1, p, other, 0)
    for d in range(1, nz):
        for p in range(npool, npieces):
            row_arrivals(p, d, is_alt[p])
        if d == 1:
            for k in range(1, nx):
                slot = (x + k) % nx * 2 + core
                for p in range(npool):
                    pool_copy(p, slot, partner, 0).wait_recv()
                    copy = pool_copy(p, slot, partner, nx - 1 + k)
                    copy.start()
                    pool_sends.append(copy)
    for p in range(npool, npieces):
        column_arrivals(p, is_alt[p])
    for k in range(nx):
        slot = (x + k) % nx * 2 + (1 - core)
        stream_copy(stream, slot, partner, 0).wait_recv()
        for p in range(npool):
            pool_copy(p, slot, partner, 0).wait_recv()
    for k in range(1, ntp):
        scale_copy(0, (tp + k) % ntp, partner).wait_recv()
    for copy in locals_[npool:]:
        copy.wait()
    for copy in stream_sends + pool_sends:
        copy.wait_send()
    for cond, piece, f, direction, target, mine in started:
        @pl.when(cond)
        def _():
            remote(piece, f, direction, target, mine).wait_send()


def gather_all(nfs, ntp, pool_in, pool_out, gate, up, down, stream, scales):
    ny, nz = fs_grid(nfs)
    nx = ntp // 2
    npieces = 8 if (ny == 2 and nz > 1) else 5
    any_spec = pl.BlockSpec(memory_space=pl.ANY)
    shapes = (
        grid_shape(nfs, ntp, pool_in.shape),
        grid_shape(ntp, nfs, pool_out.shape),
        grid_shape(nfs, 1, gate.shape),
        grid_shape(nfs, 1, up.shape),
        grid_shape(1, nfs, down.shape),
        grid_shape(1, ntp, stream.shape),
    )
    dma = pltpu.SemaphoreType.DMA
    return pl.pallas_call(
        functools.partial(gather_kernel, nfs, ntp),
        name="collect_weights",
        out_shape=tuple(jax.ShapeDtypeStruct(shape, jnp.bfloat16) for shape in shapes)
        + (jax.ShapeDtypeStruct((ntp,) + scales.shape, jnp.float32),),
        in_specs=[any_spec] * 7,
        out_specs=[any_spec] * 7,
        scratch_shapes=[
            dma((npieces, nfs, 4)),
            dma((npieces, nfs)),
            dma((npieces + 2,)),
            dma((2 * nx,)),
            dma((ntp,)),
            dma((2, 2 * nx)),
            dma((2, ntp)),
            dma((ntp,)),
            dma((ntp,)),
        ],
        compiler_params=pltpu.CompilerParams(collective_id=0, has_side_effects=True, vmem_limit_bytes=1 << 20),
    )(pool_in, pool_out, gate, up, down, stream, scales)


def sum_kernel(ntp, gathers, pieces, partial, resid, scale, out, pair, pair_sum, cross, *sems):
    pair_send, pair_recv, cross_send, cross_recv = sems[:4]
    nx = ntp // 2
    tp, fs = lax.axis_index("tp"), lax.axis_index("fs")
    x, core = tp // 2, tp % 2
    partner = x * 2 + (1 - core)
    rows, width = resid.shape
    step = rows // pieces
    barrier = pltpu.get_barrier_semaphore()
    pl.semaphore_signal(barrier, inc=1, device_id={"fs": fs, "tp": partner}, device_id_type=MESH)
    for k in range(1, nx):
        pl.semaphore_signal(
            barrier, inc=1, device_id={"fs": fs, "tp": (x + k) % nx * 2 + core}, device_id_type=MESH
        )
    pl.semaphore_wait(barrier, nx)

    def remote(src, dst, send, recv, target):
        return pltpu.make_async_remote_copy(
            src_ref=src, dst_ref=dst, send_sem=send, recv_sem=recv,
            device_id={"fs": fs, "tp": target}, device_id_type=MESH)

    def columns(t):
        return pl.ds(pl.multiple_of(t * width, width), width)

    parts = [pl.ds(i * step, step) for i in range(pieces)]
    offsets = list(range(1, nx)) + [0]
    sends = []
    for k in offsets:
        for i, part in enumerate(parts):
            copy = remote(partial.at[part, columns((x + k) % nx * 2 + (1 - core))], pair.at[k, part],
                          pair_send.at[k, i], pair_recv.at[k, i], partner)
            copy.start()
            sends.append(copy)
    for k in offsets[:-1]:
        target = (x + k) % nx * 2 + core
        for i, part in enumerate(parts):
            remote(pair.at[k, part], pair.at[k, part], pair_send.at[k, i], pair_recv.at[k, i], partner).wait_recv()
            pair_sum[k - 1, part] = (
                partial[part, columns(target)].astype(jnp.float32) + pair[k, part].astype(jnp.float32)
            ).astype(jnp.bfloat16)
            copy = remote(pair_sum.at[k - 1, part], cross.at[k - 1, part],
                          cross_send.at[k - 1, i], cross_recv.at[k - 1, i], target)
            copy.start()
            sends.append(copy)
    factor = 0.5 * scale[...]
    for i, part in enumerate(parts):
        remote(pair.at[0, part], pair.at[0, part], pair_send.at[0, i], pair_recv.at[0, i], partner).wait_recv()
        total = partial[part, columns(tp)].astype(jnp.float32) + pair[0, part].astype(jnp.float32)
        for k in range(1, nx):
            remote(cross.at[k - 1, part], cross.at[k - 1, part], cross_send.at[k - 1, i],
                   cross_recv.at[k - 1, i], partner).wait_recv()
            total = total + cross[k - 1, part].astype(jnp.float32)
        result = (resid[part].astype(jnp.float32) + total * factor).astype(jnp.bfloat16)
        if not gathers:
            out[part] = result
            continue
        out[part, columns(tp)] = result
        gather_send, gather_recv = sems[4:]
        for k in range(1, nx):
            copy = remote(out.at[part, columns(tp)], out.at[part, columns(tp)], gather_send.at[k - 1, i], gather_recv.at[tp, i],
                          (x + k) % nx * 2 + core)
            copy.start()
            sends.append(copy)
        copy = remote(out.at[part, columns(tp)], out.at[part, columns(tp)], gather_send.at[nx - 1, i], gather_recv.at[tp, i], partner)
        copy.start()
        sends.append(copy)
    if gathers:
        for k in range(1, nx):
            slot = (x + k) % nx * 2 + core
            for i, part in enumerate(parts):
                remote(out.at[part, columns(slot)], out.at[part, columns(slot)], gather_send.at[0, i], gather_recv.at[slot, i],
                       partner).wait_recv()
                copy = remote(out.at[part, columns(slot)], out.at[part, columns(slot)], gather_send.at[nx - 1 + k, i],
                              gather_recv.at[slot, i], partner)
                copy.start()
                sends.append(copy)
        for k in range(nx):
            slot = (x + k) % nx * 2 + (1 - core)
            for i, part in enumerate(parts):
                remote(out.at[part, columns(slot)], out.at[part, columns(slot)], gather_send.at[0, i], gather_recv.at[slot, i],
                       partner).wait_recv()
    for copy in sends:
        copy.wait_send()


def summed(ntp, gathers, identity, partial, resid, scale):
    nx = ntp // 2
    rows, width = resid.shape
    pieces = 3 if rows % 48 == 0 else 1
    vmem = pl.BlockSpec(memory_space=pltpu.VMEM)
    dma = pltpu.SemaphoreType.DMA
    scratch = [
        pltpu.VMEM((nx, rows, width), jnp.bfloat16),
        pltpu.VMEM((max(nx - 1, 1), rows, width), jnp.bfloat16),
        pltpu.VMEM((max(nx - 1, 1), rows, width), jnp.bfloat16),
        dma((nx, pieces)), dma((nx, pieces)), dma((nx, pieces)), dma((nx, pieces)),
    ]
    if gathers:
        scratch += [dma((2 * nx, pieces)), dma((ntp, pieces))]
    return pl.pallas_call(
        functools.partial(sum_kernel, ntp, gathers, pieces),
        name="sum_and_share" if gathers else "sum_last",
        out_shape=jax.ShapeDtypeStruct((rows, width * (ntp if gathers else 1)), jnp.bfloat16),
        in_specs=[vmem] * 3,
        out_specs=vmem,
        scratch_shapes=scratch,
        compiler_params=pltpu.CompilerParams(
            collective_id=identity, has_side_effects=True, vmem_limit_bytes=32 << 20
        ),
    )(partial, resid, scale.reshape(1, width))


def rms(floats, norm_gain):
    scaled = floats * lax.rsqrt(jnp.mean(floats * floats, axis=-1, keepdims=True) + eps)
    return (scaled * norm_gain).astype(jnp.bfloat16)


def window_weights():
    position = jnp.arange(SEQ)
    rows, cols = position[:, None], position[None, :]
    mats = []
    for window in WINDOWS:
        low = jnp.maximum(rows - window // 2, 0)
        high = jnp.minimum(rows + window - window // 2, SEQ)
        mats.append(((cols >= low) & (cols < high)).astype(jnp.bfloat16))
    return mats


def pooling(pool_input):
    channels = pool_input.shape[1]
    group = channels // 4
    values = pool_input.reshape(-1, SEQ, channels)
    position = jnp.arange(SEQ)
    parts = []
    for index, (window, members) in enumerate(zip(WINDOWS, window_weights())):
        own = values[:, :, index * group:(index + 1) * group]
        sums = jnp.einsum("pq,sqc->spc", members, own, preferred_element_type=jnp.float32)
        before = window // 2
        counts = (
            jnp.minimum(position + window - before, SEQ) - jnp.maximum(position - before, 0)
        ).astype(jnp.float32)
        parts.append(sums / counts[None, :, None] - own.astype(jnp.float32))
    return jnp.concatenate(parts, axis=2).reshape(-1, channels).astype(jnp.bfloat16)


def layer_kernel(
    sizes, stream, gate, up, down, pool_in, pool_out, scales, gains, gate_scale, up_scale, down_scale, out,
    gate_all, up_all, down_all, in_all, out_all, scales_all, rows_all, first_all, mixed_all, normed,
    gate_sum, up_sum, hidden, pooled, partial, pair, shares,
    local_sem, z_send, y_send, w_recv, pl_zsend, pl_ysend, pl_recv, slab_send, slab_recv,
    sc_send, sc_recv, ag_send, ag_recv, pair_send, pair_recv, rs_send, rs_recv,
):
    rows, small, extra = sizes
    big = small + extra
    block = gate.shape[0]
    width = stream.shape[1]
    chans = pool_in.shape[1]
    features = gate_all.shape[0]
    every = 2 * rows
    f32, half = jnp.float32, jnp.bfloat16
    fs, tp = lax.axis_index("fs"), lax.axis_index("tp")
    z, y = fs // 2, fs % 2
    x, core = tp // 2, tp % 2
    low, pair_hi = z % 2, z // 2
    zp = z + 1 - 2 * low
    zs = [z, zp, 2 - pair_hi, 3 - 3 * pair_hi]
    fs_y, fs_z = fs + 1 - 2 * y, 2 * zp + y
    tp_c, tp_x = tp + 1 - 2 * core, (tp + 2) % 4
    tp_xc = tp_x + 1 - 2 * core

    def upper(at):
        return (((at + 1) // 2) % 2 + core) % 2

    barrier = pltpu.get_barrier_semaphore()
    peers = [(2 * at + y, tp) for at in zs[1:]] + [
        (fs_y, tp), (fs, tp_c), (fs, tp_x), (fs, tp_xc), (fs_z, tp_x)]
    for f, t in peers:
        pl.semaphore_signal(barrier, inc=1, device_id={"fs": f, "tp": t}, device_id_type=MESH)
    pl.semaphore_wait(barrier, len(peers))

    ends = []

    def remote(src, dst, send, recv, f, t):
        return pltpu.make_async_remote_copy(
            src_ref=src, dst_ref=dst, send_sem=send, recv_sem=recv,
            device_id={"fs": f, "tp": t}, device_id_type=MESH)

    def start(make, cond=None):
        if cond is None:
            make().start()
        else:
            pl.when(cond)(lambda: make().start())
        ends.append((make, cond))

    def arrive(dst, recv, cond=None):
        def wait():
            remote(dst, dst, recv, recv, fs, tp_c).wait_recv()
        if cond is None:
            wait()
        else:
            pl.when(cond)(wait)

    def lanes(at, count):
        return pl.ds(pl.multiple_of(at, 128), count)

    def subs(at, count):
        return pl.ds(pl.multiple_of(at, 16), count)

    own_rows = subs(low * rows, rows)

    def share_place(ref, chip_low, t, j):
        return ref.at[subs(chip_low * rows, rows), lanes(t * width + j * block, block)]

    def share_start(phase, ref, j, src):
        dst = share_place(ref, low, tp, j)
        chip = 2 * x + low
        for k, (f, t) in enumerate(((fs_z, tp), (fs, tp_x), (fs_z, tp_x), (fs, tp_c))):
            start(lambda f=f, t=t, k=k: remote(
                src, dst, ag_send.at[phase, j, k], ag_recv.at[phase, j, chip, core], f, t))

    def share_forward(phase, ref):
        for j in range(width // block):
            for k, (cl, t) in enumerate(((1 - low, tp), (low, tp_x), (1 - low, tp_x))):
                here = share_place(ref, cl, t, j)
                chip = 2 * (t // 2) + cl
                arrive(here, ag_recv.at[phase, j, chip, core])
                start(lambda here=here, chip=chip, k=k, j=j: remote(
                    here, here, ag_send.at[phase, j, 4 + k], ag_recv.at[phase, j, chip, core], fs, tp_c))

    def share_finish(phase, ref):
        for j in range(width // block):
            for cl, t in ((low, tp_c), (1 - low, tp_c), (low, tp_xc), (1 - low, tp_xc)):
                arrive(share_place(ref, cl, t, j), ag_recv.at[phase, j, 2 * (t // 2) + cl, 1 - core])

    stream_own = pltpu.make_async_copy(
        stream, rows_all.at[own_rows, lanes(tp * width, width)], local_sem.at[0])
    stream_own.start()
    for j in range(width // block):
        share_start(0, rows_all, j, stream.at[:, j * block:(j + 1) * block])

    def scale_copy(k, slot, t):
        return remote(scales, scales_all.at[slot], sc_send.at[k], sc_recv.at[slot], fs, t)

    for k, t in enumerate((tp_c, tp_x, tp_xc)):
        start(lambda k=k, t=t: scale_copy(k, tp, t))
    locals_ = [pltpu.make_async_copy(scales, scales_all.at[tp], local_sem.at[1])]

    def pool_place(which, f, t):
        if which == 0:
            return in_all.at[subs(f * block, block), lanes(t * chans, chans)]
        return out_all.at[subs(t * chans, chans), lanes(f * block, block)]

    def pool_slab(which, t):
        if which == 0:
            return in_all.at[:, lanes(t * chans, chans)]
        return out_all.at[subs(t * chans, chans)]

    for which, own in enumerate((pool_in, pool_out)):
        locals_.append(pltpu.make_async_copy(own, pool_place(which, fs, tp), local_sem.at[2 + which]))
        for k in range(1, 4):
            start(lambda k=k, which=which, own=own: remote(
                own, pool_place(which, fs, tp), pl_zsend.at[which, k], pl_recv.at[which, fs], 2 * zs[4 - k] + y, tp))
        start(lambda which=which, own=own: remote(
            own, pool_place(which, fs, tp), pl_ysend.at[which, 0], pl_recv.at[which, fs], fs_y, tp))

    def own_part(piece, part, side):
        first, count = (side * small, small) if part == 0 else (2 * small, extra)
        ref = (gate, up, down)[piece]
        return ref.at[subs(first, count)] if piece == 2 else ref.at[:, lanes(first, count)]

    def all_part(piece, part, f):
        first, count = (0, small) if part == 0 else (small, extra)
        if piece == 2:
            return down_all.at[f, pl.ds(first, count)]
        return (gate_all, up_all)[piece].at[subs(f * block, block), pl.ds(first, count)]

    def y_own(piece):
        for part in range(2):
            start(lambda part=part: remote(
                own_part(piece, part, upper(z)), all_part(piece, part, fs), y_send.at[0, piece, part],
                w_recv.at[fs, piece, part], fs_y, tp), None if part == 0 else upper(z) == 1)

    def own_copy(piece, part):
        return pltpu.make_async_copy(
            own_part(piece, part, upper(z)), all_part(piece, part, fs), local_sem.at[4 + 2 * piece + part])

    for copy in locals_:
        copy.start()
    for piece in range(3):
        for k in (3, 2, 1):
            at = zs[k]
            for part in range(2):
                start(lambda k=k, at=at, part=part, piece=piece: remote(
                    own_part(piece, part, upper(at)), all_part(piece, part, fs), z_send.at[k, piece, part],
                    w_recv.at[fs, piece, part], 2 * at + y, tp), None if part == 0 else upper(at) == 1)
        if piece < 2:
            y_own(piece)
        own_copy(piece, 0).start()
        pl.when(upper(z) == 1)(lambda piece=piece: own_copy(piece, 1).start())

    @pl.when(upper(z) == 0)
    def _():
        gate_all[:, small:big] = jnp.zeros((features, extra), half)
        up_all[:, small:big] = jnp.zeros((features, extra), half)
        down_all[:, small:big, :] = jnp.zeros((down_all.shape[0], extra, block), half)

    def weights_here(piece, f):
        arrive(all_part(piece, 0, f), w_recv.at[f, piece, 0])
        arrive(all_part(piece, 1, f), w_recv.at[f, piece, 1], upper(z) == 1)

    def by_z(piece, i):
        f = 2 * zs[i] + y
        weights_here(piece, f)
        for part in range(2):
            start(lambda part=part: remote(
                all_part(piece, part, f), all_part(piece, part, f), y_send.at[i, piece, part],
                w_recv.at[f, piece, part], fs_y, tp), None if part == 0 else upper(z) == 1)

    def own_here(piece):
        own_copy(piece, 0).wait()
        pl.when(upper(z) == 1)(lambda: own_copy(piece, 1).wait())

    step = 32

    def norm_rows(source, gain_row):
        def one(i, carry):
            part = pl.ds(pl.multiple_of(i * step, step), step)
            floats = source[part, :].astype(f32)
            scale = lax.rsqrt(jnp.mean(floats * floats, axis=-1, keepdims=True) + eps)
            normed[part, :] = ((floats * scale) * gains[gain_row:gain_row + 1, :]).astype(half)
            return carry
        return one

    stream_own.wait()
    share_forward(0, rows_all)
    share_finish(0, rows_all)
    lax.fori_loop(0, every // step, norm_rows(rows_all, 0), 0)

    for k in range(1, 4):
        for which in range(2):
            f = 2 * zs[k] + y
            here = pool_place(which, f, tp)
            arrive(here, pl_recv.at[which, f])
            start(lambda k=k, which=which, here=here, f=f: remote(
                here, here, pl_ysend.at[which, k], pl_recv.at[which, f], fs_y, tp))

    tile = 256

    def accumulate(weights, total, f, first):
        def one(i, carry):
            part = pl.ds(pl.multiple_of(i * tile, tile), tile)
            product = jnp.dot(normed[part, lanes(f * block, block)], weights[subs(f * block, block), :],
                              preferred_element_type=f32)
            total[part, :] = product if first else total[part, :] + product
            return carry
        lax.fori_loop(0, every // tile, one, 0)

    for i in range(4):
        f, g = 2 * zs[i] + y, 2 * zs[i] + 1 - y
        for piece, (weights, total) in enumerate(((gate_all, gate_sum), (up_all, up_sum))):
            if i == 0:
                own_here(piece)
            accumulate(weights, total, f, i == 0)
        if i < 3:
            by_z(0, i + 1)
            by_z(1, i + 1)
        else:
            y_own(2)
            own_here(2)
        for piece, (weights, total) in enumerate(((gate_all, gate_sum), (up_all, up_sum))):
            weights_here(piece, g)
            accumulate(weights, total, g, False)
        if i == 1:
            for which in range(2):
                locals_[1 + which].wait()
                for k in range(4):
                    if k:
                        arrive(pool_place(which, 2 * zs[k] + 1 - y, tp), pl_recv.at[which, 2 * zs[k] + 1 - y])
                    else:
                        arrive(pool_place(which, fs_y, tp), pl_recv.at[which, fs_y])
                slab = pool_slab(which, tp)
                start(lambda which=which, slab=slab: remote(
                    slab, slab, slab_send.at[which, 0], slab_recv.at[which, tp], fs, tp_x))
                start(lambda which=which, slab=slab: remote(
                    slab, slab, slab_send.at[which, 1], slab_recv.at[which, tp], fs, tp_c))

    side = lanes(upper(z) * small, big)

    def hide(i, carry):
        part = pl.ds(pl.multiple_of(i * step, step), step)
        a = gate_sum[part, :] * gate_scale[:, side]
        hidden[part, :] = (a / (1.0 + jnp.exp(-a)) * (up_sum[part, :] * up_scale[:, side])).astype(half)
        return carry

    lax.fori_loop(0, every // step, hide, 0)

    def block_product(phase, f):
        def one(i, carry):
            part = pl.ds(pl.multiple_of(i * tile, tile), tile)
            partial[phase, f, part, :] = jnp.dot(
                hidden[part, :], down_all[f], preferred_element_type=f32).astype(half)
            return carry
        lax.fori_loop(0, every // tile, one, 0)
        zz = f // 2
        slot = 2 * (zz // 2) + f % 2
        start(lambda: remote(
            partial.at[phase, f], pair.at[phase, slot], pair_send.at[phase, f], pair_recv.at[phase, slot], fs, tp_c),
            zz % 2 != core)

    def block_sum(phase, f):
        zz = f // 2
        slot = 2 * (zz // 2) + f % 2
        here, there = subs(low * rows, rows), subs((1 - low) * rows, rows)

        @pl.when(zz % 2 == core)
        def _():
            remote(pair.at[phase, slot], pair.at[phase, slot], pair_send.at[phase, f], pair_recv.at[phase, slot],
                   fs, tp_c).wait_recv()

            def one(i, carry):
                part = pl.ds(pl.multiple_of(i * 128, 128), 128)
                partial[phase, f, part, :] = (
                    partial[phase, f, part, :].astype(f32) + pair[phase, slot, part, :].astype(f32)).astype(half)
                return carry
            lax.fori_loop(0, every // 128, one, 0)

        mine = zz // 2 == x
        for k, (part, fd, td, cond) in enumerate((
            (here, fs, tp_x, jnp.logical_not(mine)), (there, fs_z, tp, mine), (there, fs_z, tp_x, jnp.logical_not(mine)),
        )):
            start(lambda k=k, part=part, fd=fd, td=td: remote(
                partial.at[phase, f, part], shares.at[phase, k, f % 2], rs_send.at[phase, slot, k],
                rs_recv.at[phase, k, f % 2], fd, td), (zz % 2 == core) & cond)

    def block_total(phase, j, resid, target):
        f = 2 * tp + j
        for k in range(3):
            arrive(shares.at[phase, k, j], rs_recv.at[phase, k, j])

        def one(i, carry):
            at = pl.multiple_of(i * 64, 64)
            total = partial[phase, f, pl.ds(pl.multiple_of(low * rows + at, 64), 64), :].astype(f32)
            for k in range(3):
                total = total + shares[phase, k, j, pl.ds(at, 64), :].astype(f32)
            cols = slice(j * block, (j + 1) * block)
            target(at, j, (resid(at, j) + total * (0.5 * down_scale[:, cols])).astype(half))
            return carry
        lax.fori_loop(0, rows // 64, one, 0)

    def stream_part(at, j):
        return stream[pl.ds(at, 64), j * block:(j + 1) * block].astype(f32)

    def first_part(at, j, value):
        first_all[pl.ds(pl.multiple_of(low * rows + at, 64), 64), lanes(tp * width + j * block, block)] = value

    def first_done(i):
        @pl.when(zs[i] == tp)
        def _():
            for j in range(2):
                block_total(0, j, stream_part, first_part)

    by_z(2, 1)
    for i in range(4):
        f, g = 2 * zs[i] + y, 2 * zs[i] + 1 - y
        block_product(0, f)
        block_sum(0, f)
        if 1 <= i < 3:
            by_z(2, i + 1)
        if i == 1:
            for which in range(2):
                slab = pool_slab(which, tp_x)
                arrive(slab, slab_recv.at[which, tp_x])
                start(lambda which=which, slab=slab: remote(
                    slab, slab, slab_send.at[which, 2], slab_recv.at[which, tp_x], fs, tp_c))
        weights_here(2, g)
        block_product(0, g)
        block_sum(0, g)
        if i == 2:
            first_done(0)
            first_done(1)
        if i == 3:
            first_done(2)
            first_done(3)
    for j in range(2):
        share_start(1, first_all, j, share_place(first_all, low, tp, j))
    for which in range(2):
        for t in (tp_c, tp_xc):
            arrive(pool_slab(which, t), slab_recv.at[which, t])
    locals_[0].wait()
    for t in (tp_c, tp_x, tp_xc):
        arrive(scales_all.at[t], sc_recv.at[t])
    share_forward(1, first_all)
    share_finish(1, first_all)

    in_scale = jnp.concatenate([scales_all[t, :, :chans] for t in range(4)], axis=1)
    lax.fori_loop(0, every // step, norm_rows(first_all, 1), 0)
    group = 4 * chans // 4
    pos_row = lax.broadcasted_iota(jnp.int32, (SEQ, SEQ), 0)
    pos_col = lax.broadcasted_iota(jnp.int32, (SEQ, SEQ), 1)
    pos = lax.broadcasted_iota(jnp.int32, (SEQ, 1), 0)

    def mix(h, carry):
        base = pl.multiple_of(h * rows, rows)
        part = pl.ds(base, rows)
        pool_input = (jnp.dot(normed[part, :], in_all[...], preferred_element_type=f32) * in_scale).astype(half)
        for index, window in enumerate(WINDOWS):
            before = window // 2
            first = jnp.maximum(pos_row - before, 0)
            last = jnp.minimum(pos_row + window - before, SEQ)
            members = jnp.where((pos_col >= first) & (pos_col < last), 1.0, 0.0).astype(half)
            counts = (jnp.minimum(pos + window - before, SEQ) - jnp.maximum(pos - before, 0)).astype(f32)
            for s in range(rows // SEQ):
                own = pool_input[s * SEQ:(s + 1) * SEQ, index * group:(index + 1) * group]
                sums = jnp.dot(members, own, preferred_element_type=f32)
                pooled[s * SEQ:(s + 1) * SEQ, index * group:(index + 1) * group] = (
                    sums / counts - own.astype(f32)).astype(half)
        for t in range(4):
            cols = slice(t * width, (t + 1) * width)
            mixed = jnp.dot(pooled[...], out_all[:, cols], preferred_element_type=f32)
            mixed_all[part, cols] = (
                first_all[part, cols].astype(f32) + mixed * scales_all[t, :, chans:]).astype(half)
        return carry

    lax.fori_loop(0, 2, mix, 0)
    lax.fori_loop(0, every // step, norm_rows(mixed_all, 2), 0)

    def both(i, carry):
        part = pl.ds(pl.multiple_of(i * tile, tile), tile)
        a = jnp.dot(normed[part, :], gate_all[...], preferred_element_type=f32) * gate_scale[:, side]
        b = jnp.dot(normed[part, :], up_all[...], preferred_element_type=f32) * up_scale[:, side]
        hidden[part, :] = (a / (1.0 + jnp.exp(-a)) * b).astype(half)
        return carry

    lax.fori_loop(0, every // tile, both, 0)
    order = [2 * zz + j for zz in (2 * (1 - x), 2 * (1 - x) + 1, 2 * x, 2 * x + 1) for j in range(2)]
    for k, f in enumerate(order):
        block_product(1, f)
        if k:
            block_sum(1, order[k - 1])
    block_sum(1, order[-1])

    def mixed_part(at, j):
        return mixed_all[pl.ds(pl.multiple_of(low * rows + at, 64), 64), lanes(tp * width + j * block, block)].astype(f32)

    def out_part(at, j, value):
        out[pl.ds(at, 64), j * block:(j + 1) * block] = value

    for j in range(2):
        block_total(1, j, mixed_part, out_part)

    for make, cond in ends:
        if cond is None:
            make().wait_send()
        else:
            pl.when(cond)(lambda make=make: make().wait_send())


def fits(nfs, ntp, stream, gate, pool_in):
    ny, nz = fs_grid(nfs)
    tiles = gate.shape[1] // 128
    return (
        (ny, nz, ntp) == (2, 4, 4) and gate.shape[1] % 128 == 0 and tiles % 2 == 1 and tiles > 1
        and stream.shape[0] % SEQ == 0 and stream.shape[0] % 128 == 0 and pool_in.shape[1] % 128 == 0
        and gate.shape[0] % 128 == 0 and stream.shape[1] == 2 * gate.shape[0]
        and 2 * stream.shape[0] % 256 == 0
    )


def whole_layer(stream, gains, gate, gate_scale, up, up_scale, down, down_scale, pool_in, pool_out, scales):
    rows, width = stream.shape
    block, units = gate.shape
    chans = pool_in.shape[1]
    features = 4 * width
    small = (units // 128 // 2) * 128
    extra = units - 2 * small
    big = small + extra
    every = 2 * rows
    f32, half = jnp.float32, jnp.bfloat16
    vmem = pl.BlockSpec(memory_space=pltpu.VMEM)
    dma = pltpu.SemaphoreType.DMA
    return pl.pallas_call(
        functools.partial(layer_kernel, (rows, small, extra)),
        name="whole_layer",
        out_shape=jax.ShapeDtypeStruct((rows, width), half),
        in_specs=[vmem] * 11,
        out_specs=vmem,
        scratch_shapes=[
            pltpu.VMEM((features, big), half), pltpu.VMEM((features, big), half), pltpu.VMEM((8, big, block), half),
            pltpu.VMEM((features, 4 * chans), half), pltpu.VMEM((4 * chans, features), half),
            pltpu.VMEM((4,) + scales.shape, f32),
            pltpu.VMEM((every, features), half), pltpu.VMEM((every, features), half),
            pltpu.VMEM((every, features), half), pltpu.VMEM((every, features), half),
            pltpu.VMEM((every, big), f32), pltpu.VMEM((every, big), f32), pltpu.VMEM((every, big), half),
            pltpu.VMEM((rows, 4 * chans), half),
            pltpu.VMEM((2, 8, every, block), half), pltpu.VMEM((2, 4, every, block), half),
            pltpu.VMEM((2, 3, 2, rows, block), half),
            dma((10,)), dma((4, 3, 2)), dma((4, 3, 2)), dma((8, 3, 2)),
            dma((2, 4)), dma((2, 4)), dma((2, 8)), dma((2, 3)), dma((2, 4)),
            dma((3,)), dma((4,)), dma((2, 2, 7)), dma((2, 2, 4, 2)),
            dma((2, 8)), dma((2, 4)), dma((2, 4, 3)), dma((2, 3, 2)),
        ],
        compiler_params=pltpu.CompilerParams(
            collective_id=0, has_side_effects=True, vmem_limit_bytes=58 << 20),
    )(stream, gate, up, down, pool_in, pool_out, scales, gains, gate_scale.reshape(1, -1), up_scale.reshape(1, -1),
      down_scale.reshape(1, -1))


def body(
    nfs, ntp,
    stream, gain_first, gain_mixer, gain_second,
    gate_weight, gate_scale, up_weight, up_scale, down_weight, down_scale,
    pool_in_weight, pool_in_scale, pool_out_weight, pool_out_scale,
):
    half = jnp.bfloat16
    in_half, out_half = pool_in_weight.astype(half), pool_out_weight.astype(half)
    width, channels = stream.shape[1], in_half.shape[1]
    scales = jnp.concatenate([pool_in_scale, pool_out_scale]).reshape(1, -1)
    if fits(nfs, ntp, stream, gate_weight, pool_in_weight):
        return whole_layer(
            stream, jnp.stack([gain_first, gain_mixer, gain_second]), gate_weight.astype(half), gate_scale,
            up_weight.astype(half), up_scale, down_weight.astype(half), down_scale, in_half, out_half, scales)
    in_all, out_all, gate_all, up_all, down_all, stream_all, scales_all = gather_all(
        nfs, ntp, in_half, out_half, gate_weight.astype(half), up_weight.astype(half), down_weight.astype(half),
        stream, scales,
    )
    in_whole, out_whole = flat(in_all), flat(out_all)
    gate_whole, up_whole, down_whole = flat(gate_all), flat(up_all), flat(down_all)
    in_scale = scales_all[:, 0, :channels].reshape(-1)
    out_scale = scales_all[:, 0, channels:].reshape(-1)
    tp = lax.axis_index("tp")

    def feed_forward(rows):
        gate_sum = jnp.dot(rows, gate_whole, preferred_element_type=jnp.float32) * gate_scale
        up_sum = jnp.dot(rows, up_whole, preferred_element_type=jnp.float32) * up_scale
        hidden = (jax.nn.silu(gate_sum) * up_sum).astype(half)
        return jnp.dot(hidden, down_whole, preferred_element_type=jnp.float32).astype(half)

    first = rms(flat(stream_all).astype(jnp.float32), gain_first)
    after_first = summed(ntp, True, 1, feed_forward(first), stream, down_scale)
    mixer_normed = rms(after_first.astype(jnp.float32), gain_mixer)
    pool_input = (
        jnp.dot(mixer_normed, in_whole, preferred_element_type=jnp.float32) * in_scale
    ).astype(half)
    mixed = jnp.dot(pooling(pool_input), out_whole, preferred_element_type=jnp.float32)
    after_mix = (after_first.astype(jnp.float32) + mixed * out_scale).astype(half)
    second = rms(after_mix.astype(jnp.float32), gain_second)
    own = lax.dynamic_slice_in_dim(after_mix, tp * stream.shape[1], stream.shape[1], axis=1)
    return summed(ntp, False, 2, feed_forward(second), own, down_scale)


def solution(mesh):
    placed = (
        P("fs", "tp"), P(), P(), P(),
        P("fs", "tp"), P("tp"), P("fs", "tp"), P("tp"), P("tp", "fs"), P("tp"),
        P("fs", "tp"), P("tp"), P("tp", "fs"), P("tp"),
    )
    return jax.shard_map(
        functools.partial(body, mesh.shape["fs"], mesh.shape["tp"]),
        mesh=mesh, in_specs=placed, out_specs=P("fs", "tp"), check_vma=False,
    )
```

```python
import functools

import jax
import jax.numpy as jnp
from jax import lax
from jax.experimental import pallas as pl
from jax.experimental.pallas import tpu as pltpu
from jax.sharding import PartitionSpec as P

SEQ = 128
MESH = pl.DeviceIdType.MESH

eps = 1e-06
WINDOWS = (2, 4, 8, 16)


def fs_grid(count):
    ny = 1
    while (2 * ny) * (2 * ny) <= count and count % (2 * ny) == 0:
        ny *= 2
    return ny, count // ny


def grid_shape(row_blocks, col_blocks, block):
    rows, cols = block
    if cols % 128 == 0:
        return (row_blocks * rows, col_blocks * cols)
    return (row_blocks, col_blocks, rows, cols)


def place(whole, block, row_block, col_block, part=(0, None)):
    rows, cols = block
    first, count = part[0], rows if part[1] is None else part[1]
    if len(whole.shape) == 2:
        return whole.at[
            pl.ds(pl.multiple_of(row_block * rows + first, 16), count),
            pl.ds(pl.multiple_of(col_block * cols, 128), cols),
        ]
    return whole.at[row_block, col_block, pl.ds(first, count)]


def flat(whole):
    if whole.ndim == 2:
        return whole
    return whole.transpose(0, 2, 1, 3).reshape(whole.shape[0] * whole.shape[2], -1)


def gather_kernel(nfs, ntp, pool_in, pool_out, gate, up, down, stream, scales,
                  in_all, out_all, gate_all, up_all, down_all, stream_all, scales_all,
                  send_sem, recv_sem, local_sem, tsend, trecv, psend, precv, ssend, srecv):
    ny, nz = fs_grid(nfs)
    nx = ntp // 2
    fs, tp = lax.axis_index("fs"), lax.axis_index("tp")
    z, y = fs // ny, fs % ny
    x, core = tp // 2, tp % 2
    partner = x * 2 + (1 - core)
    alternate = ny == 2 and nz > 1

    barrier = pltpu.get_barrier_semaphore()

    def greet(cond, f, t):
        @pl.when(cond)
        def _():
            pl.semaphore_signal(barrier, inc=1, device_id={"fs": f, "tp": t}, device_id_type=MESH)

    greet(z > 0, fs - ny, tp)
    greet(z < nz - 1, fs + ny, tp)
    greet(y > 0, fs - 1, tp)
    greet(y < ny - 1, fs + 1, tp)
    for k in range(1, ntp):
        pl.semaphore_signal(
            barrier, inc=1, device_id={"fs": fs, "tp": (tp + k) % ntp}, device_id_type=MESH
        )
    peers = ntp - 1
    for cond in (z > 0, z < nz - 1, y > 0, y < ny - 1):
        peers = peers + jnp.where(cond, 1, 0)
    pl.semaphore_wait(barrier, peers)

    pieces = [
        (lambda: pool_in, lambda f: place(in_all, pool_in.shape, f, tp)),
        (lambda: pool_out, lambda f: place(out_all, pool_out.shape, tp, f)),
    ]
    npool = len(pieces)
    for own, whole, by_rows in ((gate, gate_all, True), (up, up_all, True), (down, down_all, False)):
        rows = own.shape[0]
        halves = 2 if alternate else 1
        for h in range(halves):
            part = (h * (rows // halves), rows // halves)

            def own_part(own=own, part=part):
                return own.at[pl.ds(*part)]

            def whole_part(f, own=own, whole=whole, part=part, by_rows=by_rows):
                return place(whole, own.shape, f if by_rows else 0, 0 if by_rows else f, part)

            pieces.append((own_part, whole_part))
    started = []

    def remote(piece, f, direction, target, mine=False):
        own, whole = pieces[piece]
        return pltpu.make_async_remote_copy(
            src_ref=own() if mine else whole(f),
            dst_ref=whole(f),
            send_sem=send_sem.at[piece, f, direction],
            recv_sem=recv_sem.at[piece, f],
            device_id={"fs": target, "tp": tp},
            device_id_type=MESH,
        )

    def send(cond, piece, f, direction, mine=False):
        target = fs + (-ny, ny, -1, 1)[direction]

        @pl.when(cond)
        def _():
            remote(piece, f, direction, target, mine).start()

        started.append((cond, piece, f, direction, target, mine))

    def arrived(cond, piece, f):
        @pl.when(cond)
        def _():
            remote(piece, f, 0, fs, False).wait_recv()

    def by_y(cond, piece, f, mine=False):
        send(cond & (y > 0), piece, f, 2, mine)
        send(cond & (y < ny - 1), piece, f, 3, mine)

    yes = z >= 0

    def stream_place(slot):
        return place(stream_all, stream.shape, 0, slot)

    def stream_copy(src, slot, t_target, k):
        return pltpu.make_async_remote_copy(
            src_ref=src, dst_ref=stream_place(slot), send_sem=tsend.at[k], recv_sem=trecv.at[slot],
            device_id={"fs": fs, "tp": t_target}, device_id_type=MESH)

    def slab(which, slot):
        if which == 0:
            if len(in_all.shape) == 2:
                cols = pool_in.shape[1]
                return in_all.at[:, pl.ds(pl.multiple_of(slot * cols, 128), cols)]
            return in_all.at[:, slot]
        if len(out_all.shape) == 2:
            rows = pool_out.shape[0]
            return out_all.at[pl.ds(pl.multiple_of(slot * rows, 16), rows)]
        return out_all.at[slot]

    def pool_copy(which, slot, t_target, k):
        return pltpu.make_async_remote_copy(
            src_ref=slab(which, slot), dst_ref=slab(which, slot),
            send_sem=psend.at[which, k], recv_sem=precv.at[which, slot],
            device_id={"fs": fs, "tp": t_target}, device_id_type=MESH)

    def scale_copy(k, slot, t_target):
        return pltpu.make_async_remote_copy(
            src_ref=scales, dst_ref=scales_all.at[slot], send_sem=ssend.at[k], recv_sem=srecv.at[slot],
            device_id={"fs": fs, "tp": t_target}, device_id_type=MESH)

    npieces = len(pieces)
    locals_ = [pltpu.make_async_copy(own(), whole(fs), local_sem.at[i]) for i, (own, whole) in enumerate(pieces)]
    locals_.append(pltpu.make_async_copy(stream, stream_place(tp), local_sem.at[npieces]))
    locals_.append(pltpu.make_async_copy(scales, scales_all.at[tp], local_sem.at[npieces + 1]))
    for piece in range(npieces):
        send(z > 0, piece, fs, 0, True)
        send(z < nz - 1, piece, fs, 1, True)
        by_y(yes, piece, fs, True)
    stream_sends = []
    for k in range(1, nx):
        stream_sends.append(stream_copy(stream, tp, (x + k) % nx * 2 + core, k - 1))
    stream_sends.append(stream_copy(stream, tp, partner, nx - 1))
    stream_sends += [scale_copy(k - 1, tp, (tp + k) % ntp) for k in range(1, ntp)]
    for copy in stream_sends:
        copy.start()
    for copy in locals_:
        copy.start()

    def row_arrivals(piece, d, alt):
        low, high = fs - d * ny, fs + d * ny
        has_low, has_high = z >= d, z + d <= nz - 1
        for cond, f, direction, ahead, end in (
            (has_low, low, 1, z < nz - 1, z == d),
            (has_high, high, 0, z > 0, z + d == nz - 1),
        ):
            arrived(cond, piece, f)
            send(cond & ahead, piece, f, direction)
            if alt:
                by_y(cond & jnp.logical_not(end), piece, f)
                other = f + 1 - 2 * y
                arrived(cond & end, piece, other)
                send(cond & end & ahead, piece, other, direction)
            else:
                by_y(cond, piece, f)

    def column_arrivals(piece, alt):
        for d in range(nz):
            for sign in ((1,) if d == 0 else (-1, 1)):
                row_ok = (z + sign * d >= 0) & (z + sign * d <= nz - 1)
                if alt:
                    at = z + sign * d
                    if d == 0:
                        continue
                    row_ok = row_ok & (at != 0) & (at != nz - 1)
                base = fs + sign * d * ny
                for e in range(1, ny):
                    for step, direction, ok, ahead in (
                        (-e, 3, y >= e, y < ny - 1),
                        (e, 2, y + e <= ny - 1, y > 0),
                    ):
                        arrived(row_ok & ok, piece, base + step)
                        if ny > 2:
                            send(row_ok & ok & ahead, piece, base + step, direction)

    is_alt = [alternate and p >= npool and p % 2 == 1 for p in range(npieces)]

    for d in range(1, nz):
        for p in range(npool):
            row_arrivals(p, d, False)
    pool_sends = []
    for p in range(npool):
        column_arrivals(p, False)
        locals_[p].wait()
        pool_sends += [pool_copy(p, tp, (x + k) % nx * 2 + core, k - 1) for k in range(1, nx)]
        pool_sends.append(pool_copy(p, tp, partner, nx - 1))
    for copy in pool_sends:
        copy.start()
    for k in range(1, nx):
        slot = (x + k) % nx * 2 + core
        stream_copy(stream, slot, partner, 0).wait_recv()
        copy = stream_copy(stream_place(slot), slot, partner, nx - 1 + k)
        copy.start()
        stream_sends.append(copy)

    for p in range(npieces):
        if is_alt[p]:
            other = fs + 1 - 2 * y
            arrived(yes, p, other)
            send(z == 0, p, other, 1)
            send(z == nz - 1, p, other, 0)
    for d in range(1, nz):
        for p in range(npool, npieces):
            row_arrivals(p, d, is_alt[p])
        if d == 1:
            for k in range(1, nx):
                slot = (x + k) % nx * 2 + core
                for p in range(npool):
                    pool_copy(p, slot, partner, 0).wait_recv()
                    copy = pool_copy(p, slot, partner, nx - 1 + k)
                    copy.start()
                    pool_sends.append(copy)
    for p in range(npool, npieces):
        column_arrivals(p, is_alt[p])
    for k in range(nx):
        slot = (x + k) % nx * 2 + (1 - core)
        stream_copy(stream, slot, partner, 0).wait_recv()
        for p in range(npool):
            pool_copy(p, slot, partner, 0).wait_recv()
    for k in range(1, ntp):
        scale_copy(0, (tp + k) % ntp, partner).wait_recv()
    for copy in locals_[npool:]:
        copy.wait()
    for copy in stream_sends + pool_sends:
        copy.wait_send()
    for cond, piece, f, direction, target, mine in started:
        @pl.when(cond)
        def _():
            remote(piece, f, direction, target, mine).wait_send()


def gather_all(nfs, ntp, pool_in, pool_out, gate, up, down, stream, scales):
    ny, nz = fs_grid(nfs)
    nx = ntp // 2
    npieces = 8 if (ny == 2 and nz > 1) else 5
    any_spec = pl.BlockSpec(memory_space=pl.ANY)
    shapes = (
        grid_shape(nfs, ntp, pool_in.shape),
        grid_shape(ntp, nfs, pool_out.shape),
        grid_shape(nfs, 1, gate.shape),
        grid_shape(nfs, 1, up.shape),
        grid_shape(1, nfs, down.shape),
        grid_shape(1, ntp, stream.shape),
    )
    dma = pltpu.SemaphoreType.DMA
    return pl.pallas_call(
        functools.partial(gather_kernel, nfs, ntp),
        name="collect_weights",
        out_shape=tuple(jax.ShapeDtypeStruct(shape, jnp.bfloat16) for shape in shapes)
        + (jax.ShapeDtypeStruct((ntp,) + scales.shape, jnp.float32),),
        in_specs=[any_spec] * 7,
        out_specs=[any_spec] * 7,
        scratch_shapes=[
            dma((npieces, nfs, 4)),
            dma((npieces, nfs)),
            dma((npieces + 2,)),
            dma((2 * nx,)),
            dma((ntp,)),
            dma((2, 2 * nx)),
            dma((2, ntp)),
            dma((ntp,)),
            dma((ntp,)),
        ],
        compiler_params=pltpu.CompilerParams(collective_id=0, has_side_effects=True, vmem_limit_bytes=1 << 20),
    )(pool_in, pool_out, gate, up, down, stream, scales)


def sum_kernel(ntp, gathers, pieces, partial, resid, scale, out, pair, pair_sum, cross, *sems):
    pair_send, pair_recv, cross_send, cross_recv = sems[:4]
    nx = ntp // 2
    tp, fs = lax.axis_index("tp"), lax.axis_index("fs")
    x, core = tp // 2, tp % 2
    partner = x * 2 + (1 - core)
    rows, width = resid.shape
    step = rows // pieces
    barrier = pltpu.get_barrier_semaphore()
    pl.semaphore_signal(barrier, inc=1, device_id={"fs": fs, "tp": partner}, device_id_type=MESH)
    for k in range(1, nx):
        pl.semaphore_signal(
            barrier, inc=1, device_id={"fs": fs, "tp": (x + k) % nx * 2 + core}, device_id_type=MESH
        )
    pl.semaphore_wait(barrier, nx)

    def remote(src, dst, send, recv, target):
        return pltpu.make_async_remote_copy(
            src_ref=src, dst_ref=dst, send_sem=send, recv_sem=recv,
            device_id={"fs": fs, "tp": target}, device_id_type=MESH)

    def columns(t):
        return pl.ds(pl.multiple_of(t * width, width), width)

    parts = [pl.ds(i * step, step) for i in range(pieces)]
    offsets = list(range(1, nx)) + [0]
    sends = []
    for k in offsets:
        for i, part in enumerate(parts):
            copy = remote(partial.at[part, columns((x + k) % nx * 2 + (1 - core))], pair.at[k, part],
                          pair_send.at[k, i], pair_recv.at[k, i], partner)
            copy.start()
            sends.append(copy)
    for k in offsets[:-1]:
        target = (x + k) % nx * 2 + core
        for i, part in enumerate(parts):
            remote(pair.at[k, part], pair.at[k, part], pair_send.at[k, i], pair_recv.at[k, i], partner).wait_recv()
            pair_sum[k - 1, part] = (
                partial[part, columns(target)].astype(jnp.float32) + pair[k, part].astype(jnp.float32)
            ).astype(jnp.bfloat16)
            copy = remote(pair_sum.at[k - 1, part], cross.at[k - 1, part],
                          cross_send.at[k - 1, i], cross_recv.at[k - 1, i], target)
            copy.start()
            sends.append(copy)
    factor = 0.5 * scale[...]
    for i, part in enumerate(parts):
        remote(pair.at[0, part], pair.at[0, part], pair_send.at[0, i], pair_recv.at[0, i], partner).wait_recv()
        total = partial[part, columns(tp)].astype(jnp.float32) + pair[0, part].astype(jnp.float32)
        for k in range(1, nx):
            remote(cross.at[k - 1, part], cross.at[k - 1, part], cross_send.at[k - 1, i],
                   cross_recv.at[k - 1, i], partner).wait_recv()
            total = total + cross[k - 1, part].astype(jnp.float32)
        result = (resid[part].astype(jnp.float32) + total * factor).astype(jnp.bfloat16)
        if not gathers:
            out[part] = result
            continue
        out[part, columns(tp)] = result
        gather_send, gather_recv = sems[4:]
        for k in range(1, nx):
            copy = remote(out.at[part, columns(tp)], out.at[part, columns(tp)], gather_send.at[k - 1, i], gather_recv.at[tp, i],
                          (x + k) % nx * 2 + core)
            copy.start()
            sends.append(copy)
        copy = remote(out.at[part, columns(tp)], out.at[part, columns(tp)], gather_send.at[nx - 1, i], gather_recv.at[tp, i], partner)
        copy.start()
        sends.append(copy)
    if gathers:
        for k in range(1, nx):
            slot = (x + k) % nx * 2 + core
            for i, part in enumerate(parts):
                remote(out.at[part, columns(slot)], out.at[part, columns(slot)], gather_send.at[0, i], gather_recv.at[slot, i],
                       partner).wait_recv()
                copy = remote(out.at[part, columns(slot)], out.at[part, columns(slot)], gather_send.at[nx - 1 + k, i],
                              gather_recv.at[slot, i], partner)
                copy.start()
                sends.append(copy)
        for k in range(nx):
            slot = (x + k) % nx * 2 + (1 - core)
            for i, part in enumerate(parts):
                remote(out.at[part, columns(slot)], out.at[part, columns(slot)], gather_send.at[0, i], gather_recv.at[slot, i],
                       partner).wait_recv()
    for copy in sends:
        copy.wait_send()


def summed(ntp, gathers, identity, partial, resid, scale):
    nx = ntp // 2
    rows, width = resid.shape
    pieces = 3 if rows % 48 == 0 else 1
    vmem = pl.BlockSpec(memory_space=pltpu.VMEM)
    dma = pltpu.SemaphoreType.DMA
    scratch = [
        pltpu.VMEM((nx, rows, width), jnp.bfloat16),
        pltpu.VMEM((max(nx - 1, 1), rows, width), jnp.bfloat16),
        pltpu.VMEM((max(nx - 1, 1), rows, width), jnp.bfloat16),
        dma((nx, pieces)), dma((nx, pieces)), dma((nx, pieces)), dma((nx, pieces)),
    ]
    if gathers:
        scratch += [dma((2 * nx, pieces)), dma((ntp, pieces))]
    return pl.pallas_call(
        functools.partial(sum_kernel, ntp, gathers, pieces),
        name="sum_and_share" if gathers else "sum_last",
        out_shape=jax.ShapeDtypeStruct((rows, width * (ntp if gathers else 1)), jnp.bfloat16),
        in_specs=[vmem] * 3,
        out_specs=vmem,
        scratch_shapes=scratch,
        compiler_params=pltpu.CompilerParams(
            collective_id=identity, has_side_effects=True, vmem_limit_bytes=32 << 20
        ),
    )(partial, resid, scale.reshape(1, width))


def rms(floats, norm_gain):
    scaled = floats * lax.rsqrt(jnp.mean(floats * floats, axis=-1, keepdims=True) + eps)
    return (scaled * norm_gain).astype(jnp.bfloat16)


def window_weights():
    position = jnp.arange(SEQ)
    rows, cols = position[:, None], position[None, :]
    mats = []
    for window in WINDOWS:
        low = jnp.maximum(rows - window // 2, 0)
        high = jnp.minimum(rows + window - window // 2, SEQ)
        mats.append(((cols >= low) & (cols < high)).astype(jnp.bfloat16))
    return mats


def pooling(pool_input):
    channels = pool_input.shape[1]
    group = channels // 4
    values = pool_input.reshape(-1, SEQ, channels)
    position = jnp.arange(SEQ)
    parts = []
    for index, (window, members) in enumerate(zip(WINDOWS, window_weights())):
        own = values[:, :, index * group:(index + 1) * group]
        sums = jnp.einsum("pq,sqc->spc", members, own, preferred_element_type=jnp.float32)
        before = window // 2
        counts = (
            jnp.minimum(position + window - before, SEQ) - jnp.maximum(position - before, 0)
        ).astype(jnp.float32)
        parts.append(sums / counts[None, :, None] - own.astype(jnp.float32))
    return jnp.concatenate(parts, axis=2).reshape(-1, channels).astype(jnp.bfloat16)


def layer_kernel(
    sizes, stream, gate_in, up_in, down_in, in_in, out_in, vectors, out,
    gate, up, down, pool_in, pool_out, gate_wide, up_wide, down_wide, in_wide, out_wide,
    gate_all, up_all, down_all, in_all, out_all, scales_all, rows_all, first_all, mixed_all, normed,
    gate_sum, up_sum, hidden, pooled, partial, pair, shares,
    load_sem, local_sem, z_send, y_send, w_recv, pl_zsend, pl_ysend, pl_recv, slab_send, slab_recv,
    sc_send, sc_recv, ag_send, ag_recv, pair_send, pair_recv, rs_send, rs_recv,
):
    rows, small, extra = sizes
    big = small + extra
    block = gate.shape[0]
    width = stream.shape[1]
    chans = pool_in.shape[1]
    units = gate.shape[1]
    features = gate_all.shape[0]
    starts = [0]
    for count in (chans, width, width, features, features, features, units, units):
        starts.append(starts[-1] + count)
    scales = vectors.at[:, :chans + 2 * width]

    def vector(at, first, count):
        return vectors[:, pl.ds(pl.multiple_of(starts[at] + first, 128), count)]

    every = 2 * rows
    f32, half = jnp.float32, jnp.bfloat16
    fs, tp = lax.axis_index("fs"), lax.axis_index("tp")
    z, y = fs // 2, fs % 2
    x, core = tp // 2, tp % 2
    low, pair_hi = z % 2, z // 2
    zp = z + 1 - 2 * low
    zs = [z, zp, 2 - pair_hi, 3 - 3 * pair_hi]
    fs_y, fs_z = fs + 1 - 2 * y, 2 * zp + y
    tp_c, tp_x = tp + 1 - 2 * core, (tp + 2) % 4
    tp_xc = tp_x + 1 - 2 * core

    def upper(at):
        return (((at + 1) // 2) % 2 + core) % 2

    own_rows = pl.ds(pl.multiple_of(low * rows, 16), rows)
    stream_own = pltpu.make_async_copy(
        stream, rows_all.at[own_rows, pl.ds(pl.multiple_of(tp * width, 128), width)], local_sem.at[0])
    stream_own.start()
    loads = []
    for i, (wide, ref, narrow) in enumerate((
        (in_wide, in_in, pool_in), (out_wide, out_in, pool_out), (gate_wide, gate_in, gate),
        (up_wide, up_in, up), (down_wide, down_in, down),
    )):
        copy = pltpu.make_async_copy(ref, wide, load_sem.at[i])
        copy.start()
        loads.append((copy, wide, narrow))

    barrier = pltpu.get_barrier_semaphore()
    peers = [(2 * at + y, tp) for at in zs[1:]] + [
        (fs_y, tp), (fs, tp_c), (fs, tp_x), (fs, tp_xc), (fs_z, tp_x)]
    for f, t in peers:
        pl.semaphore_signal(barrier, inc=1, device_id={"fs": f, "tp": t}, device_id_type=MESH)

    def narrowed(copy, wide, narrow):
        copy.wait()
        count = wide.shape[0]
        each = 64 if count % 64 == 0 else 16

        def one(i, carry):
            part = pl.ds(pl.multiple_of(i * each, each), each)
            narrow[part, :] = wide[part, :].astype(half)
            return carry
        lax.fori_loop(0, count // each, one, 0)

    for load in loads:
        narrowed(*load)
    stream_own.wait()
    pl.semaphore_wait(barrier, len(peers))

    ends = []

    def remote(src, dst, send, recv, f, t):
        return pltpu.make_async_remote_copy(
            src_ref=src, dst_ref=dst, send_sem=send, recv_sem=recv,
            device_id={"fs": f, "tp": t}, device_id_type=MESH)

    def start(make, cond=None):
        if cond is None:
            make().start()
        else:
            pl.when(cond)(lambda: make().start())
        ends.append((make, cond))

    def arrive(dst, recv, cond=None):
        def wait():
            remote(dst, dst, recv, recv, fs, tp_c).wait_recv()
        if cond is None:
            wait()
        else:
            pl.when(cond)(wait)

    def lanes(at, count):
        return pl.ds(pl.multiple_of(at, 128), count)

    def subs(at, count):
        return pl.ds(pl.multiple_of(at, 16), count)

    pieces = width // block

    def column_block(phase, j, xx, cc):
        if phase == 0:
            return (2 * xx + cc) * pieces + j
        return (2 * j + cc) * pieces + xx

    def share_place(phase, ref, chip_low, j, xx, cc):
        return ref.at[subs(chip_low * rows, rows), lanes(column_block(phase, j, xx, cc) * block, block)]

    def share_start(phase, ref, j, cond=None):
        here = share_place(phase, ref, low, j, x, core)
        for k, (f, t) in enumerate(((fs_z, tp), (fs, tp_x), (fs, tp_c))):
            start(lambda f=f, t=t, k=k: remote(
                here, here, ag_send.at[phase, j, k], ag_recv.at[phase, j, 2 * x + low, core], f, t), cond)

    def share_relay(phase, ref, j, k, chip_low, xx, targets, cond=None):
        here = share_place(phase, ref, chip_low, j, xx, core)
        flag = ag_recv.at[phase, j, 2 * xx + chip_low, core]
        arrive(here, flag, cond)
        for n, target in enumerate(targets):
            start(lambda n=n, target=target: remote(
                here, here, ag_send.at[phase, j, 3 + k + n], flag, fs, target), cond)

    def relay_own(phase, ref, j, cond=None):
        share_relay(phase, ref, j, 0, 1 - low, x, (tp_x, tp_c), cond)

    def relay_across(phase, ref, j, cond=None):
        share_relay(phase, ref, j, 2, low, 1 - x, (tp_c,), cond)
        share_relay(phase, ref, j, 3, 1 - low, 1 - x, (tp_c,), cond)

    def share_finish(phase, ref):
        for j in range(2):
            for xx in (x, 1 - x):
                for cl in (low, 1 - low):
                    arrive(share_place(phase, ref, cl, j, xx, 1 - core), ag_recv.at[phase, j, 2 * xx + cl, 1 - core])

    for j in range(2):
        share_start(0, rows_all, j)

    def scale_copy(k, slot, t):
        return remote(scales, scales_all.at[slot], sc_send.at[k], sc_recv.at[slot], fs, t)

    for k, t in enumerate((tp_c, tp_x, tp_xc)):
        start(lambda k=k, t=t: scale_copy(k, tp, t))
    locals_ = [pltpu.make_async_copy(scales, scales_all.at[tp], local_sem.at[1])]

    def pool_place(which, f, t):
        if which == 0:
            return in_all.at[subs(f * block, block), lanes(t * chans, chans)]
        return out_all.at[subs(t * chans, chans), lanes(f * block, block)]

    def pool_slab(which, t):
        if which == 0:
            return in_all.at[:, lanes(t * chans, chans)]
        return out_all.at[subs(t * chans, chans)]

    def pool_start():
        for which, own in enumerate((pool_in, pool_out)):
            for k in range(1, 4):
                start(lambda k=k, which=which, own=own: remote(
                    own, pool_place(which, fs, tp), pl_zsend.at[which, k], pl_recv.at[which, fs], 2 * zs[k] + y, tp))
            start(lambda which=which, own=own: remote(
                own, pool_place(which, fs, tp), pl_ysend.at[which, 0], pl_recv.at[which, fs], fs_y, tp))

    for which, own in enumerate((pool_in, pool_out)):
        locals_.append(pltpu.make_async_copy(own, pool_place(which, fs, tp), local_sem.at[2 + which]))

    def own_part(piece, part, side):
        first, count = (side * small, small) if part == 0 else (2 * small, extra)
        ref = (gate, up, down)[piece]
        return ref.at[subs(first, count)] if piece == 2 else ref.at[:, lanes(first, count)]

    def all_part(piece, part, f):
        first, count = (0, small) if part == 0 else (small, extra)
        if piece == 2:
            return down_all.at[pl.ds(first, count), lanes(f * block, block)]
        return (gate_all, up_all)[piece].at[subs(f * block, block), pl.ds(first, count)]

    def y_own(piece):
        for part in range(2):
            start(lambda part=part: remote(
                own_part(piece, part, upper(z)), all_part(piece, part, fs), y_send.at[0, piece, part],
                w_recv.at[fs, piece, part], fs_y, tp), None if part == 0 else upper(z) == 1)

    def own_copy(piece, part):
        return pltpu.make_async_copy(
            own_part(piece, part, upper(z)), all_part(piece, part, fs), local_sem.at[4 + 2 * piece + part])

    for copy in locals_:
        copy.start()
    inner = (z == 1) | (z == 2)

    def z_own(piece, cond=None, targets=(1, 2, 3)):
        for k in targets:
            at = zs[k]
            for part in range(2):
                ok = cond
                if part:
                    ok = upper(at) == 1 if cond is None else cond & (upper(at) == 1)
                start(lambda k=k, at=at, part=part: remote(
                    own_part(piece, part, upper(at)), all_part(piece, part, fs), z_send.at[k, piece, part],
                    w_recv.at[fs, piece, part], 2 * at + y, tp), ok)

    outer = jnp.logical_not(inner)
    z_own(0, None, (1,))
    y_own(0)
    z_own(1, outer, (1,))
    z_own(0, None, (2, 3))
    pool_start()
    z_own(1, inner, (1,))
    z_own(1, None, (2, 3))
    y_own(1)
    z_own(2, None, (1,))
    for piece in range(3):
        own_copy(piece, 0).start()
        pl.when(upper(z) == 1)(lambda piece=piece: own_copy(piece, 1).start())

    @pl.when(upper(z) == 0)
    def _():
        gate_all[:, small:big] = jnp.zeros((features, extra), half)
        up_all[:, small:big] = jnp.zeros((features, extra), half)
        down_all[small:big, :] = jnp.zeros((extra, features), half)

    def weights_here(piece, f):
        arrive(all_part(piece, 0, f), w_recv.at[f, piece, 0])
        arrive(all_part(piece, 1, f), w_recv.at[f, piece, 1], upper(z) == 1)

    def by_z(piece, i):
        f = 2 * zs[i] + y
        weights_here(piece, f)
        for part in range(2):
            start(lambda part=part: remote(
                all_part(piece, part, f), all_part(piece, part, f), y_send.at[i, piece, part],
                w_recv.at[f, piece, part], fs_y, tp), None if part == 0 else upper(z) == 1)

    def own_here(piece):
        own_copy(piece, 0).wait()
        pl.when(upper(z) == 1)(lambda: own_copy(piece, 1).wait())

    step = 32
    lane_tiles = features // 128

    def norm_rows(source, gain_at, base=0):
        def one(i, carry):
            part = pl.ds(pl.multiple_of(base + i * 128, 128), 128)
            total = jnp.zeros((128, 128), f32)
            for c in range(lane_tiles):
                floats = source[part, c * 128:(c + 1) * 128].astype(f32)
                total = total + floats * floats
            scale = lax.rsqrt(jnp.sum(total, axis=-1, keepdims=True) * (1.0 / features) + eps)
            for c in range(lane_tiles):
                floats = source[part, c * 128:(c + 1) * 128].astype(f32)
                normed[part, c * 128:(c + 1) * 128] = ((floats * scale) * vector(gain_at, c * 128, 128)).astype(half)
            return carry
        return one

    for j in range(2):
        relay_own(0, rows_all, j)
    for j in range(2):
        relay_across(0, rows_all, j)
    share_finish(0, rows_all)
    lax.fori_loop(0, every // 128, norm_rows(rows_all, 3), 0)

    def pool_by_y():
        for k in range(1, 4):
            for which in range(2):
                f = 2 * zs[k] + y
                here = pool_place(which, f, tp)
                arrive(here, pl_recv.at[which, f])
                start(lambda k=k, which=which, here=here, f=f: remote(
                    here, here, pl_ysend.at[which, k], pl_recv.at[which, f], fs_y, tp))

    tile = 256

    def accumulate(weights, total, f, first):
        for n in range(big // 128 // 2 + 1):
            cols = slice(n * tile, min((n + 1) * tile, big))
            if cols.start < cols.stop:
                product = jnp.dot(normed[:, lanes(f * block, block)], weights[subs(f * block, block), cols],
                                  preferred_element_type=f32)
                total[:, cols] = product if first else total[:, cols] + product

    def pool_across():
        for which in range(2):
            locals_[1 + which].wait()
            for k in range(4):
                f = fs_y if k == 0 else 2 * zs[k] + 1 - y
                arrive(pool_place(which, f, tp), pl_recv.at[which, f])
            slab = pool_slab(which, tp)
            for n, t in enumerate((tp_x, tp_c)):
                start(lambda which=which, slab=slab, n=n, t=t: remote(
                    slab, slab, slab_send.at[which, n], slab_recv.at[which, tp], fs, t))

    ahead = [(piece, i) for piece in range(3) for i in range(1, 4)]
    for piece, (weights, total) in enumerate(((gate_all, gate_sum), (up_all, up_sum))):
        for i in range(4):
            f, g = 2 * zs[i] + y, 2 * zs[i] + 1 - y
            if i == 0:
                own_here(piece)
            accumulate(weights, total, f, i == 0)
            if 4 * piece + i < 7:
                by_z(*ahead[4 * piece + i])
            weights_here(piece, g)
            accumulate(weights, total, g, False)
            if (piece, i) == (0, 2):
                pool_by_y()
            if (piece, i) == (0, 3):
                y_own(2)
            if (piece, i) == (1, 0):
                z_own(2, outer, (2, 3))
                pool_across()
            if (piece, i) == (1, 1):
                z_own(2, inner, (2, 3))
    own_here(2)

    def hide(i, carry):
        part = pl.ds(pl.multiple_of(i * step, step), step)
        a = gate_sum[part, :] * vector(6, upper(z) * small, big)
        hidden[part, :] = (a / (1.0 + jnp.exp(-a)) * (up_sum[part, :] * vector(7, upper(z) * small, big))).astype(half)
        return carry

    lax.fori_loop(0, every // step, hide, 0)

    sides = ((1 - low) * rows, low * rows)

    def block_send(phase, f, h):
        zz = f // 2
        slot = 2 * (zz // 2) + f % 2
        part = subs(sides[h], rows)
        start(lambda: remote(
            partial.at[phase, f, part], pair.at[phase, slot, part], pair_send.at[phase, f, h],
            pair_recv.at[phase, slot, h], fs, tp_c), zz % 2 != core)

    def core_sum(phase, f, h):
        zz = f // 2
        slot = 2 * (zz // 2) + f % 2

        @pl.when(zz % 2 == core)
        def _():
            here = pair.at[phase, slot, subs(sides[h], rows)]
            remote(here, here, pair_send.at[phase, f, h], pair_recv.at[phase, slot, h], fs, tp_c).wait_recv()

            def one(i, carry):
                at = pl.ds(pl.multiple_of(sides[h] + i * 128, 128), 128)
                partial[phase, f, at, :] = (
                    partial[phase, f, at, :].astype(f32) + pair[phase, slot, at, :].astype(f32)).astype(half)
                return carry
            lax.fori_loop(0, rows // 128, one, 0)

    def reduce_send(phase, f, h, k, dst, recv, fd, td, cond):
        start(lambda: remote(
            partial.at[phase, f, subs(sides[h], rows)], shares.at[phase, *dst],
            rs_send.at[phase, 2 * (f // 4) + f % 2, k], rs_recv.at[phase, *recv], fd, td),
            ((f // 2) % 2 == core) & cond)

    def add_rows(f, phase, dst, target):
        def one(i, carry):
            at = pl.multiple_of(i * 64, 64)
            here = pl.ds(pl.multiple_of(low * rows + at, 64), 64)
            total = partial[phase, f, here, :].astype(f32)
            for place_of in dst:
                total = total + shares[phase, *place_of, pl.ds(at, 64), :].astype(f32)
            target(at, here, total)
            return carry
        lax.fori_loop(0, rows // 64, one, 0)

    def first_sum(f):
        for h in range(2):
            core_sum(0, f, h)
            if h == 0:
                to = (f // 4, f % 2)
                reduce_send(0, f, 0, 0, to, to, fs_z, tp, True)

    def first_middle(f):
        q, j = f // 4, f % 2

        @pl.when((f // 2) % 2 == core)
        def _():
            here = shares.at[0, q, j]
            remote(here, here, rs_recv.at[0, q, j], rs_recv.at[0, q, j], fs, tp_c).wait_recv()

            def target(at, here, total):
                partial[0, f, here, :] = total.astype(half)
            add_rows(f, 0, ((q, j),), target)
        reduce_send(0, f, 1, 1, (2, q), (2, q), fs, tp_x, j != x)

    def first_done(f):
        q, j = f // 4, f % 2
        cond = ((f // 2) % 2 == core) & (j == x)

        @pl.when(cond)
        def _():
            here = shares.at[0, 2, q]
            remote(here, here, rs_recv.at[0, 2, q], rs_recv.at[0, 2, q], fs, tp_c).wait_recv()
            cols = lanes(f * block, block)
            factor = 0.5 * scales_all[f // 2, :, pl.ds(pl.multiple_of(chans + width + j * block, 128), block)]

            def target(at, here, total):
                first_all[here, cols] = (rows_all[here, cols].astype(f32) + total * factor).astype(half)
            add_rows(f, 0, ((2, q),), target)
        share_start(1, first_all, q, cond)

    def first_relay(f):
        q, j = f // 4, f % 2
        turn = (f // 2) % 2 == core
        relay_own(1, first_all, q, turn & (j == x))
        relay_across(1, first_all, q, turn & (j != x))

    def second_sum(f, h):
        core_sum(1, f, h)
        mine = f // 4 == x
        away = jnp.logical_not(mine)
        if h == 0:
            reduce_send(1, f, 0, 1, (1, f % 2), (1, f % 2), fs_z, tp, mine)
            reduce_send(1, f, 0, 2, (2, f % 2), (2, f % 2), fs_z, tp_x, away)
        else:
            reduce_send(1, f, 1, 0, (0, f % 2), (0, f % 2), fs, tp_x, away)

    blocks = [2 * zs[i] + j for i in range(4) for j in (y, 1 - y)]

    def slab_across():
        for which in range(2):
            slab = pool_slab(which, tp_x)
            arrive(slab, slab_recv.at[which, tp_x])
            start(lambda which=which, slab=slab: remote(
                slab, slab, slab_send.at[which, 2], slab_recv.at[which, tp_x], fs, tp_c))

    locals_[0].wait()
    for t in (tp_c, tp_x, tp_xc):
        arrive(scales_all.at[t], sc_recv.at[t])
    for n, f in enumerate(blocks):
        if n % 2:
            weights_here(2, f)
        partial[0, f, :, :] = jnp.dot(
            hidden[...], down_all[:, lanes(f * block, block)], preferred_element_type=f32).astype(half)
        for h in range(2):
            block_send(0, f, h)
        if n in (0, 2):
            by_z(2, 2 + n // 2)
        first_sum(f)
        if n == 3:
            slab_across()
        for m in {4: (0, 2), 5: (1, 3), 6: (4,), 7: (5,)}.get(n, ()):
            first_middle(blocks[m])
        for m in {6: (0, 2), 7: (1, 3)}.get(n, ()):
            first_done(blocks[m])
    first_middle(blocks[6])
    first_done(blocks[4])
    first_middle(blocks[7])
    for m in (0, 2, 1, 3):
        first_relay(blocks[m])
    for m in (5, 6, 7):
        first_done(blocks[m])
        first_relay(blocks[m - 1])
    first_relay(blocks[7])
    for which in range(2):
        for t in (tp_c, tp_xc):
            arrive(pool_slab(which, t), slab_recv.at[which, t])
    share_finish(1, first_all)

    in_scale = jnp.concatenate([scales_all[t, :, :chans] for t in range(4)], axis=1)
    group = 4 * chans // 4
    pos_row = lax.broadcasted_iota(jnp.int32, (SEQ, SEQ), 0)
    pos_col = lax.broadcasted_iota(jnp.int32, (SEQ, SEQ), 1)
    pos = lax.broadcasted_iota(jnp.int32, (SEQ, 1), 0)

    def mix(h):
        base = pl.multiple_of(sides[h], 128)
        part = pl.ds(base, rows)
        pool_input = (jnp.dot(normed[part, :], in_all[...], preferred_element_type=f32) * in_scale).astype(half)
        for index, window in enumerate(WINDOWS):
            before = window // 2
            first = jnp.maximum(pos_row - before, 0)
            last = jnp.minimum(pos_row + window - before, SEQ)
            members = jnp.where((pos_col >= first) & (pos_col < last), 1.0, 0.0).astype(half)
            counts = (jnp.minimum(pos + window - before, SEQ) - jnp.maximum(pos - before, 0)).astype(f32)
            for s in range(rows // SEQ):
                own = pool_input[s * SEQ:(s + 1) * SEQ, index * group:(index + 1) * group]
                sums = jnp.dot(members, own, preferred_element_type=f32)
                pooled[s * SEQ:(s + 1) * SEQ, index * group:(index + 1) * group] = (
                    sums / counts - own.astype(f32)).astype(half)
        for t in range(4):
            cols = slice(t * width, (t + 1) * width)
            mixed = jnp.dot(pooled[...], out_all[:, cols], preferred_element_type=f32)
            mixed_all[part, cols] = (
                first_all[part, cols].astype(f32) + mixed * scales_all[t, :, chans:chans + width]).astype(half)

    order = [2 * xx + cc for cc in (1 - core, core) for xx in (1 - x, x)]
    for h in range(2):
        lax.fori_loop(0, rows // 128, norm_rows(first_all, 4, sides[h]), 0)
        mix(h)
        lax.fori_loop(0, rows // 128, norm_rows(mixed_all, 5, sides[h]), 0)
        part = subs(sides[h], rows)
        a = jnp.dot(normed[part, :], gate_all[...], preferred_element_type=f32) * vector(6, upper(z) * small, big)
        b = jnp.dot(normed[part, :], up_all[...], preferred_element_type=f32) * vector(7, upper(z) * small, big)
        hidden[part, :] = (a / (1.0 + jnp.exp(-a)) * b).astype(half)
        for n, zz in enumerate(order):
            product = jnp.dot(hidden[part, :], down_all[:, lanes(zz * width, width)], preferred_element_type=f32)
            for j in range(2):
                partial[1, 2 * zz + j, part, :] = product[:, j * block:(j + 1) * block].astype(half)
            for j in range(2):
                block_send(1, 2 * zz + j, h)
            if n > 1:
                for j in range(2):
                    second_sum(2 * zz + j, h)

    for j in range(2):
        for k in range(3):
            arrive(shares.at[1, k, j], rs_recv.at[1, k, j])

        def target(at, here, total, j=j):
            value = mixed_all[here, lanes(tp * width + j * block, block)].astype(f32)
            factor = 0.5 * vector(2, j * block, block)
            out[pl.ds(at, 64), j * block:(j + 1) * block] = (value + total * factor).astype(half)
        add_rows(2 * tp + j, 1, ((0, j), (1, j), (2, j)), target)

    for make, cond in ends:
        if cond is None:
            make().wait_send()
        else:
            pl.when(cond)(lambda make=make: make().wait_send())


def fits(nfs, ntp, stream, gate, pool_in):
    ny, nz = fs_grid(nfs)
    tiles = gate.shape[1] // 128
    return (
        (ny, nz, ntp) == (2, 4, 4) and gate.shape[1] % 128 == 0 and tiles % 2 == 1 and tiles > 1
        and stream.shape[0] % SEQ == 0 and stream.shape[0] % 128 == 0 and pool_in.shape[1] % 128 == 0
        and gate.shape[0] % 128 == 0 and stream.shape[1] == 2 * gate.shape[0]
        and 2 * stream.shape[0] % 256 == 0
    )


def whole_layer(stream, gate, up, down, pool_in, pool_out, vectors):
    rows, width = stream.shape
    block, units = gate.shape
    chans = pool_in.shape[1]
    features = 4 * width
    small = (units // 128 // 2) * 128
    extra = units - 2 * small
    big = small + extra
    every = 2 * rows
    f32, half = jnp.float32, jnp.bfloat16
    vmem = pl.BlockSpec(memory_space=pltpu.VMEM)
    hbm = pl.BlockSpec(memory_space=pl.ANY)
    dma = pltpu.SemaphoreType.DMA
    weights = (gate, up, down, pool_in, pool_out)
    return pl.pallas_call(
        functools.partial(layer_kernel, (rows, small, extra)),
        name="whole_layer",
        out_shape=jax.ShapeDtypeStruct((rows, width), half),
        in_specs=[hbm] * 6 + [vmem],
        out_specs=vmem,
        scratch_shapes=[pltpu.VMEM(w.shape, half) for w in weights] + [pltpu.VMEM(w.shape, f32) for w in weights] + [
            pltpu.VMEM((features, big), half), pltpu.VMEM((features, big), half), pltpu.VMEM((big, features), half),
            pltpu.VMEM((features, 4 * chans), half), pltpu.VMEM((4 * chans, features), half),
            pltpu.VMEM((4, 1, chans + 2 * width), f32),
            pltpu.VMEM((every, features), half), pltpu.VMEM((every, features), half),
            pltpu.VMEM((every, features), half), pltpu.VMEM((every, features), half),
            pltpu.VMEM((every, big), f32), pltpu.VMEM((every, big), f32), pltpu.VMEM((every, big), half),
            pltpu.VMEM((rows, 4 * chans), half),
            pltpu.VMEM((2, 8, every, block), half), pltpu.VMEM((2, 4, every, block), half),
            pltpu.VMEM((2, 3, 2, rows, block), half),
            dma((5,)), dma((10,)), dma((4, 3, 2)), dma((4, 3, 2)), dma((8, 3, 2)),
            dma((2, 4)), dma((2, 4)), dma((2, 8)), dma((2, 3)), dma((2, 4)),
            dma((3,)), dma((4,)), dma((2, 2, 7)), dma((2, 2, 4, 2)),
            dma((2, 8, 2)), dma((2, 4, 2)), dma((2, 4, 3)), dma((2, 3, 2)),
        ],
        compiler_params=pltpu.CompilerParams(
            collective_id=0, has_side_effects=True, vmem_limit_bytes=60 << 20),
    )(stream, *weights, vectors)


def body(
    nfs, ntp,
    stream, gain_first, gain_mixer, gain_second,
    gate_weight, gate_scale, up_weight, up_scale, down_weight, down_scale,
    pool_in_weight, pool_in_scale, pool_out_weight, pool_out_scale,
):
    half = jnp.bfloat16
    if fits(nfs, ntp, stream, gate_weight, pool_in_weight):
        vectors = jnp.concatenate([
            pool_in_scale, pool_out_scale, down_scale, gain_first, gain_mixer, gain_second, gate_scale, up_scale])
        return whole_layer(
            stream, gate_weight, up_weight, down_weight, pool_in_weight, pool_out_weight, vectors.reshape(1, -1))
    in_half, out_half = pool_in_weight.astype(half), pool_out_weight.astype(half)
    width, channels = stream.shape[1], in_half.shape[1]
    scales = jnp.concatenate([pool_in_scale, pool_out_scale]).reshape(1, -1)
    in_all, out_all, gate_all, up_all, down_all, stream_all, scales_all = gather_all(
        nfs, ntp, in_half, out_half, gate_weight.astype(half), up_weight.astype(half), down_weight.astype(half),
        stream, scales,
    )
    in_whole, out_whole = flat(in_all), flat(out_all)
    gate_whole, up_whole, down_whole = flat(gate_all), flat(up_all), flat(down_all)
    in_scale = scales_all[:, 0, :channels].reshape(-1)
    out_scale = scales_all[:, 0, channels:].reshape(-1)
    tp = lax.axis_index("tp")

    def feed_forward(rows):
        gate_sum = jnp.dot(rows, gate_whole, preferred_element_type=jnp.float32) * gate_scale
        up_sum = jnp.dot(rows, up_whole, preferred_element_type=jnp.float32) * up_scale
        hidden = (jax.nn.silu(gate_sum) * up_sum).astype(half)
        return jnp.dot(hidden, down_whole, preferred_element_type=jnp.float32).astype(half)

    first = rms(flat(stream_all).astype(jnp.float32), gain_first)
    after_first = summed(ntp, True, 1, feed_forward(first), stream, down_scale)
    mixer_normed = rms(after_first.astype(jnp.float32), gain_mixer)
    pool_input = (
        jnp.dot(mixer_normed, in_whole, preferred_element_type=jnp.float32) * in_scale
    ).astype(half)
    mixed = jnp.dot(pooling(pool_input), out_whole, preferred_element_type=jnp.float32)
    after_mix = (after_first.astype(jnp.float32) + mixed * out_scale).astype(half)
    second = rms(after_mix.astype(jnp.float32), gain_second)
    own = lax.dynamic_slice_in_dim(after_mix, tp * stream.shape[1], stream.shape[1], axis=1)
    return summed(ntp, False, 2, feed_forward(second), own, down_scale)


def solution(mesh):
    placed = (
        P("fs", "tp"), P(), P(), P(),
        P("fs", "tp"), P("tp"), P("fs", "tp"), P("tp"), P("tp", "fs"), P("tp"),
        P("fs", "tp"), P("tp"), P("tp", "fs"), P("tp"),
    )
    return jax.shard_map(
        functools.partial(body, mesh.shape["fs"], mesh.shape["tp"]),
        mesh=mesh, in_specs=placed, out_specs=P("fs", "tp"), check_vma=False,
    )
```

```python
import functools

import jax
import jax.numpy as jnp
from jax import lax
from jax.experimental import pallas as pl
from jax.experimental.pallas import tpu as pltpu
from jax.sharding import PartitionSpec as P

SEQ = 128
MESH = pl.DeviceIdType.MESH

eps = 1e-06
WINDOWS = (2, 4, 8, 16)
Z_FIRST = (5, 7)


def fs_grid(count):
    ny = 1
    while (2 * ny) * (2 * ny) <= count and count % (2 * ny) == 0:
        ny *= 2
    return ny, count // ny


def grid_shape(row_blocks, col_blocks, block):
    rows, cols = block
    if cols % 128 == 0:
        return (row_blocks * rows, col_blocks * cols)
    return (row_blocks, col_blocks, rows, cols)


def place(whole, block, row_block, col_block, part=(0, None)):
    rows, cols = block
    first, count = part[0], rows if part[1] is None else part[1]
    if len(whole.shape) == 2:
        return whole.at[
            pl.ds(pl.multiple_of(row_block * rows + first, 16), count),
            pl.ds(pl.multiple_of(col_block * cols, 128), cols),
        ]
    return whole.at[row_block, col_block, pl.ds(first, count)]


def flat(whole):
    if whole.ndim == 2:
        return whole
    return whole.transpose(0, 2, 1, 3).reshape(whole.shape[0] * whole.shape[2], -1)


def gather_kernel(nfs, ntp, pool_in, pool_out, gate, up, down, stream, scales,
                  in_all, out_all, gate_all, up_all, down_all, stream_all, scales_all,
                  send_sem, recv_sem, local_sem, tsend, trecv, psend, precv, ssend, srecv):
    ny, nz = fs_grid(nfs)
    nx = ntp // 2
    fs, tp = lax.axis_index("fs"), lax.axis_index("tp")
    z, y = fs // ny, fs % ny
    x, core = tp // 2, tp % 2
    partner = x * 2 + (1 - core)
    alternate = ny == 2 and nz > 1

    barrier = pltpu.get_barrier_semaphore()

    def greet(cond, f, t):
        @pl.when(cond)
        def _():
            pl.semaphore_signal(barrier, inc=1, device_id={"fs": f, "tp": t}, device_id_type=MESH)

    greet(z > 0, fs - ny, tp)
    greet(z < nz - 1, fs + ny, tp)
    greet(y > 0, fs - 1, tp)
    greet(y < ny - 1, fs + 1, tp)
    for k in range(1, ntp):
        pl.semaphore_signal(
            barrier, inc=1, device_id={"fs": fs, "tp": (tp + k) % ntp}, device_id_type=MESH
        )
    peers = ntp - 1
    for cond in (z > 0, z < nz - 1, y > 0, y < ny - 1):
        peers = peers + jnp.where(cond, 1, 0)
    pl.semaphore_wait(barrier, peers)

    pieces = [
        (lambda: pool_in, lambda f: place(in_all, pool_in.shape, f, tp)),
        (lambda: pool_out, lambda f: place(out_all, pool_out.shape, tp, f)),
    ]
    npool = len(pieces)
    for own, whole, by_rows in ((gate, gate_all, True), (up, up_all, True), (down, down_all, False)):
        rows = own.shape[0]
        halves = 2 if alternate else 1
        for h in range(halves):
            part = (h * (rows // halves), rows // halves)

            def own_part(own=own, part=part):
                return own.at[pl.ds(*part)]

            def whole_part(f, own=own, whole=whole, part=part, by_rows=by_rows):
                return place(whole, own.shape, f if by_rows else 0, 0 if by_rows else f, part)

            pieces.append((own_part, whole_part))
    started = []

    def remote(piece, f, direction, target, mine=False):
        own, whole = pieces[piece]
        return pltpu.make_async_remote_copy(
            src_ref=own() if mine else whole(f),
            dst_ref=whole(f),
            send_sem=send_sem.at[piece, f, direction],
            recv_sem=recv_sem.at[piece, f],
            device_id={"fs": target, "tp": tp},
            device_id_type=MESH,
        )

    def send(cond, piece, f, direction, mine=False):
        target = fs + (-ny, ny, -1, 1)[direction]

        @pl.when(cond)
        def _():
            remote(piece, f, direction, target, mine).start()

        started.append((cond, piece, f, direction, target, mine))

    def arrived(cond, piece, f):
        @pl.when(cond)
        def _():
            remote(piece, f, 0, fs, False).wait_recv()

    def by_y(cond, piece, f, mine=False):
        send(cond & (y > 0), piece, f, 2, mine)
        send(cond & (y < ny - 1), piece, f, 3, mine)

    yes = z >= 0

    def stream_place(slot):
        return place(stream_all, stream.shape, 0, slot)

    def stream_copy(src, slot, t_target, k):
        return pltpu.make_async_remote_copy(
            src_ref=src, dst_ref=stream_place(slot), send_sem=tsend.at[k], recv_sem=trecv.at[slot],
            device_id={"fs": fs, "tp": t_target}, device_id_type=MESH)

    def slab(which, slot):
        if which == 0:
            if len(in_all.shape) == 2:
                cols = pool_in.shape[1]
                return in_all.at[:, pl.ds(pl.multiple_of(slot * cols, 128), cols)]
            return in_all.at[:, slot]
        if len(out_all.shape) == 2:
            rows = pool_out.shape[0]
            return out_all.at[pl.ds(pl.multiple_of(slot * rows, 16), rows)]
        return out_all.at[slot]

    def pool_copy(which, slot, t_target, k):
        return pltpu.make_async_remote_copy(
            src_ref=slab(which, slot), dst_ref=slab(which, slot),
            send_sem=psend.at[which, k], recv_sem=precv.at[which, slot],
            device_id={"fs": fs, "tp": t_target}, device_id_type=MESH)

    def scale_copy(k, slot, t_target):
        return pltpu.make_async_remote_copy(
            src_ref=scales, dst_ref=scales_all.at[slot], send_sem=ssend.at[k], recv_sem=srecv.at[slot],
            device_id={"fs": fs, "tp": t_target}, device_id_type=MESH)

    npieces = len(pieces)
    locals_ = [pltpu.make_async_copy(own(), whole(fs), local_sem.at[i]) for i, (own, whole) in enumerate(pieces)]
    locals_.append(pltpu.make_async_copy(stream, stream_place(tp), local_sem.at[npieces]))
    locals_.append(pltpu.make_async_copy(scales, scales_all.at[tp], local_sem.at[npieces + 1]))
    for piece in range(npieces):
        send(z > 0, piece, fs, 0, True)
        send(z < nz - 1, piece, fs, 1, True)
        by_y(yes, piece, fs, True)
    stream_sends = []
    for k in range(1, nx):
        stream_sends.append(stream_copy(stream, tp, (x + k) % nx * 2 + core, k - 1))
    stream_sends.append(stream_copy(stream, tp, partner, nx - 1))
    stream_sends += [scale_copy(k - 1, tp, (tp + k) % ntp) for k in range(1, ntp)]
    for copy in stream_sends:
        copy.start()
    for copy in locals_:
        copy.start()

    def row_arrivals(piece, d, alt):
        low, high = fs - d * ny, fs + d * ny
        has_low, has_high = z >= d, z + d <= nz - 1
        for cond, f, direction, ahead, end in (
            (has_low, low, 1, z < nz - 1, z == d),
            (has_high, high, 0, z > 0, z + d == nz - 1),
        ):
            arrived(cond, piece, f)
            send(cond & ahead, piece, f, direction)
            if alt:
                by_y(cond & jnp.logical_not(end), piece, f)
                other = f + 1 - 2 * y
                arrived(cond & end, piece, other)
                send(cond & end & ahead, piece, other, direction)
            else:
                by_y(cond, piece, f)

    def column_arrivals(piece, alt):
        for d in range(nz):
            for sign in ((1,) if d == 0 else (-1, 1)):
                row_ok = (z + sign * d >= 0) & (z + sign * d <= nz - 1)
                if alt:
                    at = z + sign * d
                    if d == 0:
                        continue
                    row_ok = row_ok & (at != 0) & (at != nz - 1)
                base = fs + sign * d * ny
                for e in range(1, ny):
                    for step, direction, ok, ahead in (
                        (-e, 3, y >= e, y < ny - 1),
                        (e, 2, y + e <= ny - 1, y > 0),
                    ):
                        arrived(row_ok & ok, piece, base + step)
                        if ny > 2:
                            send(row_ok & ok & ahead, piece, base + step, direction)

    is_alt = [alternate and p >= npool and p % 2 == 1 for p in range(npieces)]

    for d in range(1, nz):
        for p in range(npool):
            row_arrivals(p, d, False)
    pool_sends = []
    for p in range(npool):
        column_arrivals(p, False)
        locals_[p].wait()
        pool_sends += [pool_copy(p, tp, (x + k) % nx * 2 + core, k - 1) for k in range(1, nx)]
        pool_sends.append(pool_copy(p, tp, partner, nx - 1))
    for copy in pool_sends:
        copy.start()
    for k in range(1, nx):
        slot = (x + k) % nx * 2 + core
        stream_copy(stream, slot, partner, 0).wait_recv()
        copy = stream_copy(stream_place(slot), slot, partner, nx - 1 + k)
        copy.start()
        stream_sends.append(copy)

    for p in range(npieces):
        if is_alt[p]:
            other = fs + 1 - 2 * y
            arrived(yes, p, other)
            send(z == 0, p, other, 1)
            send(z == nz - 1, p, other, 0)
    for d in range(1, nz):
        for p in range(npool, npieces):
            row_arrivals(p, d, is_alt[p])
        if d == 1:
            for k in range(1, nx):
                slot = (x + k) % nx * 2 + core
                for p in range(npool):
                    pool_copy(p, slot, partner, 0).wait_recv()
                    copy = pool_copy(p, slot, partner, nx - 1 + k)
                    copy.start()
                    pool_sends.append(copy)
    for p in range(npool, npieces):
        column_arrivals(p, is_alt[p])
    for k in range(nx):
        slot = (x + k) % nx * 2 + (1 - core)
        stream_copy(stream, slot, partner, 0).wait_recv()
        for p in range(npool):
            pool_copy(p, slot, partner, 0).wait_recv()
    for k in range(1, ntp):
        scale_copy(0, (tp + k) % ntp, partner).wait_recv()
    for copy in locals_[npool:]:
        copy.wait()
    for copy in stream_sends + pool_sends:
        copy.wait_send()
    for cond, piece, f, direction, target, mine in started:
        @pl.when(cond)
        def _():
            remote(piece, f, direction, target, mine).wait_send()


def gather_all(nfs, ntp, pool_in, pool_out, gate, up, down, stream, scales):
    ny, nz = fs_grid(nfs)
    nx = ntp // 2
    npieces = 8 if (ny == 2 and nz > 1) else 5
    any_spec = pl.BlockSpec(memory_space=pl.ANY)
    shapes = (
        grid_shape(nfs, ntp, pool_in.shape),
        grid_shape(ntp, nfs, pool_out.shape),
        grid_shape(nfs, 1, gate.shape),
        grid_shape(nfs, 1, up.shape),
        grid_shape(1, nfs, down.shape),
        grid_shape(1, ntp, stream.shape),
    )
    dma = pltpu.SemaphoreType.DMA
    return pl.pallas_call(
        functools.partial(gather_kernel, nfs, ntp),
        name="collect_weights",
        out_shape=tuple(jax.ShapeDtypeStruct(shape, jnp.bfloat16) for shape in shapes)
        + (jax.ShapeDtypeStruct((ntp,) + scales.shape, jnp.float32),),
        in_specs=[any_spec] * 7,
        out_specs=[any_spec] * 7,
        scratch_shapes=[
            dma((npieces, nfs, 4)),
            dma((npieces, nfs)),
            dma((npieces + 2,)),
            dma((2 * nx,)),
            dma((ntp,)),
            dma((2, 2 * nx)),
            dma((2, ntp)),
            dma((ntp,)),
            dma((ntp,)),
        ],
        compiler_params=pltpu.CompilerParams(collective_id=0, has_side_effects=True, vmem_limit_bytes=1 << 20),
    )(pool_in, pool_out, gate, up, down, stream, scales)


def sum_kernel(ntp, gathers, pieces, partial, resid, scale, out, pair, pair_sum, cross, *sems):
    pair_send, pair_recv, cross_send, cross_recv = sems[:4]
    nx = ntp // 2
    tp, fs = lax.axis_index("tp"), lax.axis_index("fs")
    x, core = tp // 2, tp % 2
    partner = x * 2 + (1 - core)
    rows, width = resid.shape
    step = rows // pieces
    barrier = pltpu.get_barrier_semaphore()
    pl.semaphore_signal(barrier, inc=1, device_id={"fs": fs, "tp": partner}, device_id_type=MESH)
    for k in range(1, nx):
        pl.semaphore_signal(
            barrier, inc=1, device_id={"fs": fs, "tp": (x + k) % nx * 2 + core}, device_id_type=MESH
        )
    pl.semaphore_wait(barrier, nx)

    def remote(src, dst, send, recv, target):
        return pltpu.make_async_remote_copy(
            src_ref=src, dst_ref=dst, send_sem=send, recv_sem=recv,
            device_id={"fs": fs, "tp": target}, device_id_type=MESH)

    def columns(t):
        return pl.ds(pl.multiple_of(t * width, width), width)

    parts = [pl.ds(i * step, step) for i in range(pieces)]
    offsets = list(range(1, nx)) + [0]
    sends = []
    for k in offsets:
        for i, part in enumerate(parts):
            copy = remote(partial.at[part, columns((x + k) % nx * 2 + (1 - core))], pair.at[k, part],
                          pair_send.at[k, i], pair_recv.at[k, i], partner)
            copy.start()
            sends.append(copy)
    for k in offsets[:-1]:
        target = (x + k) % nx * 2 + core
        for i, part in enumerate(parts):
            remote(pair.at[k, part], pair.at[k, part], pair_send.at[k, i], pair_recv.at[k, i], partner).wait_recv()
            pair_sum[k - 1, part] = (
                partial[part, columns(target)].astype(jnp.float32) + pair[k, part].astype(jnp.float32)
            ).astype(jnp.bfloat16)
            copy = remote(pair_sum.at[k - 1, part], cross.at[k - 1, part],
                          cross_send.at[k - 1, i], cross_recv.at[k - 1, i], target)
            copy.start()
            sends.append(copy)
    factor = 0.5 * scale[...]
    for i, part in enumerate(parts):
        remote(pair.at[0, part], pair.at[0, part], pair_send.at[0, i], pair_recv.at[0, i], partner).wait_recv()
        total = partial[part, columns(tp)].astype(jnp.float32) + pair[0, part].astype(jnp.float32)
        for k in range(1, nx):
            remote(cross.at[k - 1, part], cross.at[k - 1, part], cross_send.at[k - 1, i],
                   cross_recv.at[k - 1, i], partner).wait_recv()
            total = total + cross[k - 1, part].astype(jnp.float32)
        result = (resid[part].astype(jnp.float32) + total * factor).astype(jnp.bfloat16)
        if not gathers:
            out[part] = result
            continue
        out[part, columns(tp)] = result
        gather_send, gather_recv = sems[4:]
        for k in range(1, nx):
            copy = remote(out.at[part, columns(tp)], out.at[part, columns(tp)], gather_send.at[k - 1, i], gather_recv.at[tp, i],
                          (x + k) % nx * 2 + core)
            copy.start()
            sends.append(copy)
        copy = remote(out.at[part, columns(tp)], out.at[part, columns(tp)], gather_send.at[nx - 1, i], gather_recv.at[tp, i], partner)
        copy.start()
        sends.append(copy)
    if gathers:
        for k in range(1, nx):
            slot = (x + k) % nx * 2 + core
            for i, part in enumerate(parts):
                remote(out.at[part, columns(slot)], out.at[part, columns(slot)], gather_send.at[0, i], gather_recv.at[slot, i],
                       partner).wait_recv()
                copy = remote(out.at[part, columns(slot)], out.at[part, columns(slot)], gather_send.at[nx - 1 + k, i],
                              gather_recv.at[slot, i], partner)
                copy.start()
                sends.append(copy)
        for k in range(nx):
            slot = (x + k) % nx * 2 + (1 - core)
            for i, part in enumerate(parts):
                remote(out.at[part, columns(slot)], out.at[part, columns(slot)], gather_send.at[0, i], gather_recv.at[slot, i],
                       partner).wait_recv()
    for copy in sends:
        copy.wait_send()


def summed(ntp, gathers, identity, partial, resid, scale):
    nx = ntp // 2
    rows, width = resid.shape
    pieces = 3 if rows % 48 == 0 else 1
    vmem = pl.BlockSpec(memory_space=pltpu.VMEM)
    dma = pltpu.SemaphoreType.DMA
    scratch = [
        pltpu.VMEM((nx, rows, width), jnp.bfloat16),
        pltpu.VMEM((max(nx - 1, 1), rows, width), jnp.bfloat16),
        pltpu.VMEM((max(nx - 1, 1), rows, width), jnp.bfloat16),
        dma((nx, pieces)), dma((nx, pieces)), dma((nx, pieces)), dma((nx, pieces)),
    ]
    if gathers:
        scratch += [dma((2 * nx, pieces)), dma((ntp, pieces))]
    return pl.pallas_call(
        functools.partial(sum_kernel, ntp, gathers, pieces),
        name="sum_and_share" if gathers else "sum_last",
        out_shape=jax.ShapeDtypeStruct((rows, width * (ntp if gathers else 1)), jnp.bfloat16),
        in_specs=[vmem] * 3,
        out_specs=vmem,
        scratch_shapes=scratch,
        compiler_params=pltpu.CompilerParams(
            collective_id=identity, has_side_effects=True, vmem_limit_bytes=32 << 20
        ),
    )(partial, resid, scale.reshape(1, width))


def rms(floats, norm_gain):
    scaled = floats * lax.rsqrt(jnp.mean(floats * floats, axis=-1, keepdims=True) + eps)
    return (scaled * norm_gain).astype(jnp.bfloat16)


def window_weights():
    position = jnp.arange(SEQ)
    rows, cols = position[:, None], position[None, :]
    mats = []
    for window in WINDOWS:
        low = jnp.maximum(rows - window // 2, 0)
        high = jnp.minimum(rows + window - window // 2, SEQ)
        mats.append(((cols >= low) & (cols < high)).astype(jnp.bfloat16))
    return mats


def pooling(pool_input):
    channels = pool_input.shape[1]
    group = channels // 4
    values = pool_input.reshape(-1, SEQ, channels)
    position = jnp.arange(SEQ)
    parts = []
    for index, (window, members) in enumerate(zip(WINDOWS, window_weights())):
        own = values[:, :, index * group:(index + 1) * group]
        sums = jnp.einsum("pq,sqc->spc", members, own, preferred_element_type=jnp.float32)
        before = window // 2
        counts = (
            jnp.minimum(position + window - before, SEQ) - jnp.maximum(position - before, 0)
        ).astype(jnp.float32)
        parts.append(sums / counts[None, :, None] - own.astype(jnp.float32))
    return jnp.concatenate(parts, axis=2).reshape(-1, channels).astype(jnp.bfloat16)


def layer_kernel(
    sizes, stream, gate_in, up_in, down_in, in_in, out_in, *refs):
    parts, (out, vectors, *rest) = refs[:8], refs[8:]
    layer_steps(sizes, stream, gate_in, up_in, down_in, in_in, out_in, parts, out, vectors, *rest)


def layer_steps(
    sizes, stream, gate_in, up_in, down_in, in_in, out_in, parts, out, vectors,
    gate, up, down, pool_in, pool_out, gate_wide, up_wide, down_wide, in_wide, out_wide,
    gate_all, up_all, down_all, in_all, out_all, scales_all, rows_all, first_all, mixed_all, normed,
    gate_sum, up_sum, hidden, pooled, partial, pair, shares, first_in,
    load_sem, vector_sem, local_sem, z_send, y_send, w_recv, pl_zsend, pl_ysend, pl_recv, slab_send, slab_recv,
    sc_send, sc_recv, ag_send, ag_recv, pair_send, pair_recv, two_send, two_recv, rs_send, rs_recv,
    fr_send, fr_recv, fr_core,
):
    rows, small, extra = sizes
    big = small + extra
    block = gate.shape[0]
    width = stream.shape[1]
    chans = pool_in.shape[1]
    units = gate.shape[1]
    features = gate_all.shape[0]
    starts = [0]
    for count in (chans, width, width, features, features, features, units, units):
        starts.append(starts[-1] + count)
    scales = vectors.at[:, :chans + 2 * width]

    def vector(at, first, count):
        return vectors[:, pl.ds(pl.multiple_of(starts[at] + first, 128), count)]

    every = 2 * rows
    f32, half = jnp.float32, jnp.bfloat16
    fs, tp = lax.axis_index("fs"), lax.axis_index("tp")
    z, y = fs // 2, fs % 2
    x, core = tp // 2, tp % 2
    low, pair_hi = z % 2, z // 2
    zp = z + 1 - 2 * low
    zs = [z, zp, 2 - pair_hi, 3 - 3 * pair_hi]
    fs_y, fs_z = fs + 1 - 2 * y, 2 * zp + y
    tp_c, tp_x = tp + 1 - 2 * core, (tp + 2) % 4
    tp_xc = tp_x + 1 - 2 * core

    def upper(at):
        return (((at + 1) // 2) % 2 + core) % 2

    own_rows = pl.ds(pl.multiple_of(low * rows, 16), rows)
    stream_own = pltpu.make_async_copy(
        stream, rows_all.at[own_rows, pl.ds(pl.multiple_of(tp * width, 128), width)], local_sem.at[0])
    stream_own.start()
    vector_copies = [
        pltpu.make_async_copy(ref, vectors.at[0, pl.ds(first, ref.shape[0])], vector_sem.at[i])
        for i, (ref, first) in enumerate(zip(parts, starts))]
    for copy in vector_copies:
        copy.start()
    loads = []
    for i, (wide, ref, narrow) in enumerate((
        (in_wide, in_in, pool_in), (out_wide, out_in, pool_out), (gate_wide, gate_in, gate),
        (up_wide, up_in, up), (down_wide, down_in, down),
    )):
        copy = pltpu.make_async_copy(ref, wide, load_sem.at[i])
        copy.start()
        loads.append((copy, wide, narrow))

    barrier = pltpu.get_barrier_semaphore()
    peers = [(2 * at + y, tp) for at in zs[1:]] + [
        (fs_y, tp), (fs, tp_c), (fs, tp_x), (fs, tp_xc), (fs_z, tp_x)]
    for f, t in peers:
        pl.semaphore_signal(barrier, inc=1, device_id={"fs": f, "tp": t}, device_id_type=MESH)

    def narrowed(copy, wide, narrow):
        copy.wait()
        count = wide.shape[0]
        each = 64 if count % 64 == 0 else 16

        def one(i, carry):
            part = pl.ds(pl.multiple_of(i * each, each), each)
            narrow[part, :] = wide[part, :].astype(half)
            return carry
        lax.fori_loop(0, count // each, one, 0)

    for load in loads:
        narrowed(*load)
    stream_own.wait()
    for copy in vector_copies:
        copy.wait()
    pl.semaphore_wait(barrier, len(peers))

    ends = []

    def remote(src, dst, send, recv, f, t):
        return pltpu.make_async_remote_copy(
            src_ref=src, dst_ref=dst, send_sem=send, recv_sem=recv,
            device_id={"fs": f, "tp": t}, device_id_type=MESH)

    def start(make, cond=None):
        if cond is None:
            make().start()
        else:
            pl.when(cond)(lambda: make().start())
        ends.append((make, cond))

    def flush():
        for make, cond in ends:
            if cond is None:
                make().wait_send()
            else:
                pl.when(cond)(lambda make=make: make().wait_send())
        ends.clear()

    def arrive(dst, recv, cond=None):
        def wait():
            remote(dst, dst, recv, recv, fs, tp_c).wait_recv()
        if cond is None:
            wait()
        else:
            pl.when(cond)(wait)

    def lanes(at, count):
        return pl.ds(pl.multiple_of(at, 128), count)

    def subs(at, count):
        return pl.ds(pl.multiple_of(at, 16), count)

    pieces = width // block

    def column_block(j, xx, cc):
        return (2 * xx + cc) * pieces + j

    def share_place(phase, ref, chip_low, j, xx, cc):
        return ref.at[subs(chip_low * rows, rows), lanes(column_block(j, xx, cc) * block, block)]

    def share_start(phase, ref, j, cond=None):
        here = share_place(phase, ref, low, j, x, core)
        for k, (f, t) in enumerate(((fs_z, tp), (fs, tp_x), (fs, tp_c))):
            start(lambda f=f, t=t, k=k: remote(
                here, here, ag_send.at[phase, j, k], ag_recv.at[phase, j, 2 * x + low, core], f, t), cond)

    def share_relay(phase, ref, j, k, chip_low, xx, targets, cond=None):
        here = share_place(phase, ref, chip_low, j, xx, core)
        flag = ag_recv.at[phase, j, 2 * xx + chip_low, core]
        arrive(here, flag, cond)
        for n, target in enumerate(targets):
            start(lambda n=n, target=target: remote(
                here, here, ag_send.at[phase, j, 3 + k + n], flag, fs, target), cond)

    def relay_own(phase, ref, j, cond=None):
        share_relay(phase, ref, j, 0, 1 - low, x, (tp_x, tp_c), cond)

    def relay_across(phase, ref, j, cond=None):
        share_relay(phase, ref, j, 2, low, 1 - x, (tp_c,), cond)
        share_relay(phase, ref, j, 3, 1 - low, 1 - x, (tp_c,), cond)

    def share_finish(phase, ref):
        for j in range(2):
            for xx in (x, 1 - x):
                for cl in (low, 1 - low):
                    arrive(share_place(phase, ref, cl, j, xx, 1 - core), ag_recv.at[phase, j, 2 * xx + cl, 1 - core])

    for j in range(2):
        share_start(0, rows_all, j)

    def scale_copy(k, slot, t):
        return remote(scales, scales_all.at[slot], sc_send.at[k], sc_recv.at[slot], fs, t)

    for k, t in enumerate((tp_c, tp_x, tp_xc)):
        start(lambda k=k, t=t: scale_copy(k, tp, t))
    locals_ = [pltpu.make_async_copy(scales, scales_all.at[tp], local_sem.at[1])]

    def pool_place(which, f, t):
        if which == 0:
            return in_all.at[subs(f * block, block), lanes(t * chans, chans)]
        return out_all.at[subs(t * chans, chans), lanes(f * block, block)]

    def pool_slab(which, t):
        if which == 0:
            return in_all.at[:, lanes(t * chans, chans)]
        return out_all.at[subs(t * chans, chans)]

    def pool_start():
        for which, own in enumerate((pool_in, pool_out)):
            for k in range(1, 4):
                start(lambda k=k, which=which, own=own: remote(
                    own, pool_place(which, fs, tp), pl_zsend.at[which, k], pl_recv.at[which, fs], 2 * zs[k] + y, tp))
            start(lambda which=which, own=own: remote(
                own, pool_place(which, fs, tp), pl_ysend.at[which, 0], pl_recv.at[which, fs], fs_y, tp))

    for which, own in enumerate((pool_in, pool_out)):
        locals_.append(pltpu.make_async_copy(own, pool_place(which, fs, tp), local_sem.at[2 + which]))

    def own_part(piece, part, side):
        first, count = (side * small, small) if part == 0 else (2 * small, extra)
        ref = (gate, up, down)[piece]
        return ref.at[subs(first, count)] if piece == 2 else ref.at[:, lanes(first, count)]

    def all_part(piece, part, f):
        first, count = (0, small) if part == 0 else (small, extra)
        if piece == 2:
            return down_all.at[pl.ds(first, count), lanes(f * block, block)]
        return (gate_all, up_all)[piece].at[subs(f * block, block), pl.ds(first, count)]

    def y_own(piece):
        for part in range(2):
            start(lambda part=part: remote(
                own_part(piece, part, upper(z)), all_part(piece, part, fs), y_send.at[0, piece, part],
                w_recv.at[fs, piece, part], fs_y, tp), None if part == 0 else upper(z) == 1)

    def own_copy(piece, part):
        return pltpu.make_async_copy(
            own_part(piece, part, upper(z)), all_part(piece, part, fs), local_sem.at[4 + 2 * piece + part])

    for copy in locals_:
        copy.start()
    inner = (z == 1) | (z == 2)

    def z_own(piece, cond=None, targets=(1, 2, 3)):
        for k in targets:
            at = zs[k]
            for part in range(2):
                ok = cond
                if part:
                    ok = upper(at) == 1 if cond is None else cond & (upper(at) == 1)
                start(lambda k=k, at=at, part=part: remote(
                    own_part(piece, part, upper(at)), all_part(piece, part, fs), z_send.at[k, piece, part],
                    w_recv.at[fs, piece, part], 2 * at + y, tp), ok)

    outer = jnp.logical_not(inner)
    z_own(0, None, (1,))
    y_own(0)
    z_own(1, outer, (1,))
    z_own(0, None, (2, 3))
    pool_start()
    z_own(1, inner, (1,))
    z_own(1, None, (2, 3))
    y_own(1)
    z_own(2, None, (1,))
    for piece in range(3):
        own_copy(piece, 0).start()
        pl.when(upper(z) == 1)(lambda piece=piece: own_copy(piece, 1).start())

    @pl.when(upper(z) == 0)
    def _():
        gate_all[:, small:big] = jnp.zeros((features, extra), half)
        up_all[:, small:big] = jnp.zeros((features, extra), half)
        down_all[small:big, :] = jnp.zeros((extra, features), half)

    def weights_here(piece, f):
        arrive(all_part(piece, 0, f), w_recv.at[f, piece, 0])
        arrive(all_part(piece, 1, f), w_recv.at[f, piece, 1], upper(z) == 1)

    def by_z(piece, i):
        f = 2 * zs[i] + y
        weights_here(piece, f)
        for part in range(2):
            start(lambda part=part: remote(
                all_part(piece, part, f), all_part(piece, part, f), y_send.at[i, piece, part],
                w_recv.at[f, piece, part], fs_y, tp), None if part == 0 else upper(z) == 1)

    def own_here(piece):
        own_copy(piece, 0).wait()
        pl.when(upper(z) == 1)(lambda: own_copy(piece, 1).wait())

    step = 32
    lane_tiles = features // 128

    def norm_rows(source, gain_at, base=0):
        def one(i, carry):
            part = pl.ds(pl.multiple_of(base + i * 128, 128), 128)
            total = jnp.zeros((128, 128), f32)
            for c in range(lane_tiles):
                floats = source[part, c * 128:(c + 1) * 128].astype(f32)
                total = total + floats * floats
            scale = lax.rsqrt(jnp.sum(total, axis=-1, keepdims=True) * (1.0 / features) + eps)
            for c in range(lane_tiles):
                floats = source[part, c * 128:(c + 1) * 128].astype(f32)
                normed[part, c * 128:(c + 1) * 128] = ((floats * scale) * vector(gain_at, c * 128, 128)).astype(half)
            return carry
        return one

    for j in range(2):
        relay_own(0, rows_all, j)
    for j in range(2):
        relay_across(0, rows_all, j)
    share_finish(0, rows_all)
    lax.fori_loop(0, every // 128, norm_rows(rows_all, 3), 0)

    def pool_by_y():
        for k in range(1, 4):
            for which in range(2):
                f = 2 * zs[k] + y
                here = pool_place(which, f, tp)
                arrive(here, pl_recv.at[which, f])
                start(lambda k=k, which=which, here=here, f=f: remote(
                    here, here, pl_ysend.at[which, k], pl_recv.at[which, f], fs_y, tp))

    tile = 256

    def accumulate(weights, total, f, first):
        for n in range(big // 128 // 2 + 1):
            cols = slice(n * tile, min((n + 1) * tile, big))
            if cols.start < cols.stop:
                product = jnp.dot(normed[:, lanes(f * block, block)], weights[subs(f * block, block), cols],
                                  preferred_element_type=f32)
                total[:, cols] = product if first else total[:, cols] + product

    def pool_across():
        for which in range(2):
            locals_[1 + which].wait()
            for k in range(4):
                f = fs_y if k == 0 else 2 * zs[k] + 1 - y
                arrive(pool_place(which, f, tp), pl_recv.at[which, f])
            slab = pool_slab(which, tp)
            for n, t in enumerate((tp_x, tp_c)):
                start(lambda which=which, slab=slab, n=n, t=t: remote(
                    slab, slab, slab_send.at[which, n], slab_recv.at[which, tp], fs, t))

    ahead = [(piece, i) for piece in range(3) for i in range(1, 4)]
    for piece, (weights, total) in enumerate(((gate_all, gate_sum), (up_all, up_sum))):
        for i in range(4):
            f, g = 2 * zs[i] + y, 2 * zs[i] + 1 - y
            if i == 0:
                own_here(piece)
            accumulate(weights, total, f, i == 0)
            if 4 * piece + i < 7:
                by_z(*ahead[4 * piece + i])
            weights_here(piece, g)
            accumulate(weights, total, g, False)
            if (piece, i) == (0, 2):
                pool_by_y()
            if (piece, i) == (0, 3):
                y_own(2)
            if (piece, i) == (1, 0):
                z_own(2, outer, (2, 3))
                pool_across()
            if (piece, i) == (1, 1):
                z_own(2, inner, (2, 3))
    own_here(2)

    def hide(i, carry):
        part = pl.ds(pl.multiple_of(i * step, step), step)
        a = gate_sum[part, :] * vector(6, upper(z) * small, big)
        hidden[part, :] = (a / (1.0 + jnp.exp(-a)) * (up_sum[part, :] * vector(7, upper(z) * small, big))).astype(half)
        return carry

    lax.fori_loop(0, every // step, hide, 0)

    def block_send(f, r):
        zz = f // 2
        slot = 2 * (zz // 2) + f % 2
        part = subs(r * rows, rows)
        start(lambda: remote(
            partial.at[f, part], pair.at[0, slot, part], pair_send.at[f, r],
            pair_recv.at[slot, r], fs, tp_c), zz % 2 != core)

    def core_sum(f, r):
        slot = 2 * (f // 4) + f % 2

        @pl.when((f // 2) % 2 == core)
        def _():
            here = pair.at[0, slot, subs(r * rows, rows)]
            remote(here, here, pair_send.at[f, r], pair_recv.at[slot, r], fs, tp_c).wait_recv()

            def one(i, carry):
                at = pl.ds(pl.multiple_of(r * rows + i * 128, 128), 128)
                partial[f, at, :] = (
                    partial[f, at, :].astype(f32) + pair[0, slot, at, :].astype(f32)).astype(half)
                return carry
            lax.fori_loop(0, rows // 128, one, 0)

    blocks = [2 * zs[i] + j for i in range(4) for j in (y, 1 - y)]

    def ways(n):
        across_x, across_z = (fs, tp_x), (fs_z, tp)
        return (across_z, across_x, low) if n in Z_FIRST else (across_x, across_z, x)

    def first_send(n, k, src, dst, recv, to):
        f = blocks[n]
        start(lambda: remote(src, dst, fr_send.at[2 * (f // 4) + f % 2, k], recv, *to), (f // 2) % 2 == core)

    def first_sum(n):
        f = blocks[n]
        slot = 2 * (f // 4) + f % 2
        to, _, r = ways(n)
        core_sum(f, 1 - r)
        first_send(n, 0, partial.at[f, subs((1 - r) * rows, rows)], first_in.at[0, slot], fr_recv.at[slot, 0], to)
        core_sum(f, r)

    def first_add(n):
        f = blocks[n]
        slot = 2 * (f // 4) + f % 2
        _, to, r = ways(n)
        part = subs(r * rows, rows)

        @pl.when((f // 2) % 2 == core)
        def _():
            arrive(first_in.at[0, slot], fr_recv.at[slot, 0])

            def one(i, carry):
                at = pl.ds(pl.multiple_of(r * rows + i * 128, 128), 128)
                got = first_in[0, slot, pl.ds(pl.multiple_of(i * 128, 128), 128), :].astype(f32)
                partial[f, at, :] = (partial[f, at, :].astype(f32) + got).astype(half)
                return carry
            lax.fori_loop(0, rows // 128, one, 0)
        first_send(n, 1, partial.at[f, part], first_in.at[1, slot], fr_recv.at[slot, 1], to)

    def first_done(n):
        f = blocks[n]
        slot = 2 * (f // 4) + f % 2
        to, _, r = ways(n)
        cols = lanes(f * block, block)

        @pl.when((f // 2) % 2 == core)
        def _():
            arrive(first_in.at[1, slot], fr_recv.at[slot, 1])
            factor = 0.5 * scales_all[f // 2, :, pl.ds(pl.multiple_of(chans + width + (f % 2) * block, 128), block)]

            def one(i, carry):
                at = pl.ds(pl.multiple_of(r * rows + i * 128, 128), 128)
                total = partial[f, at, :].astype(f32) + first_in[
                    1, slot, pl.ds(pl.multiple_of(i * 128, 128), 128), :].astype(f32)
                first_all[at, cols] = (rows_all[at, cols].astype(f32) + total * factor).astype(half)
                return carry
            lax.fori_loop(0, rows // 128, one, 0)
        here = first_all.at[subs(r * rows, rows), cols]
        first_send(n, 2, here, here, fr_recv.at[slot, 2], to)
        first_send(n, 3, here, here, fr_core.at[slot, r], (fs, tp_c))

    def first_pass(n):
        f = blocks[n]
        slot = 2 * (f // 4) + f % 2
        r = 1 - ways(n)[2]
        here = first_all.at[subs(r * rows, rows), lanes(f * block, block)]
        arrive(here, fr_recv.at[slot, 2], (f // 2) % 2 == core)
        first_send(n, 4, here, here, fr_core.at[slot, r], (fs, tp_c))

    def first_finish():
        for f in blocks:
            slot = 2 * (f // 4) + f % 2
            for r in range(2):
                arrive(first_all.at[r * rows:(r + 1) * rows, lanes(f * block, block)], fr_core.at[slot, r],
                       (f // 2) % 2 != core)

    def part_send(f, h, c, base, count):
        slot = 2 * (f // 4) + f % 2
        part = subs(base, count)
        start(lambda: remote(
            partial.at[f, part], pair.at[1, slot, part], two_send.at[f, h, c], two_recv.at[slot, h, c], fs, tp_c),
            (f // 2) % 2 != core)

    def part_sum(f, h, c, base, first, count):
        slot = 2 * (f // 4) + f % 2
        part = subs(base, count)

        @pl.when((f // 2) % 2 == core)
        def _():
            arrive(pair.at[1, slot, part], two_recv.at[slot, h, c])

            def one(i, carry):
                at = pl.ds(pl.multiple_of(base + i * 128, 128), 128)
                partial[f, at, :] = (partial[f, at, :].astype(f32) + pair[1, slot, at, :].astype(f32)).astype(half)
                return carry
            lax.fori_loop(0, count // 128, one, 0)
        mine = f // 4 == x
        away = jnp.logical_not(mine)
        ways = ((1, fs_z, tp, mine), (2, fs_z, tp_x, away)) if h == 0 else ((0, fs, tp_x, away),)
        for k, fd, td, cond in ways:
            start(lambda k=k, fd=fd, td=td: remote(
                partial.at[f, part], shares.at[k, f % 2, pl.ds(first, count)], rs_send.at[slot, k, c],
                rs_recv.at[k, f % 2, c], fd, td), ((f // 2) % 2 == core) & cond)

    cuts = (((0, SEQ), (SEQ, rows - SEQ)), ((0, rows - SEQ), (rows - SEQ, SEQ)))

    def slab_across():
        for which in range(2):
            slab = pool_slab(which, tp_x)
            arrive(slab, slab_recv.at[which, tp_x])
            start(lambda which=which, slab=slab: remote(
                slab, slab, slab_send.at[which, 2], slab_recv.at[which, tp_x], fs, tp_c))

    locals_[0].wait()
    for t in (tp_c, tp_x, tp_xc):
        arrive(scales_all.at[t], sc_recv.at[t])
    for n, f in enumerate(blocks):
        if n % 2:
            weights_here(2, f)
        partial[f, :, :] = jnp.dot(
            hidden[...], down_all[:, lanes(f * block, block)], preferred_element_type=f32).astype(half)
        for r in (1 - ways(n)[2], ways(n)[2]):
            block_send(f, r)
        first_sum(n)
        if n == 2:
            slab_across()
        if n in (3, 4):
            by_z(2, n - 1)
        for stage, members in {
            1: ((first_add, (0,)),), 2: ((first_add, (1,)),), 3: ((first_add, (2, 3)),),
            4: ((first_done, (0, 2, 1, 3)),), 5: ((first_add, (4,)), (first_pass, (0, 2))),
            6: ((first_add, (5,)), (first_pass, (1, 3))), 7: ((first_done, (4,)), (first_add, (6, 7))),
        }.get(n, ()):
            for m in members:
                stage(m)
    for stage, m in (
        (first_done, 5), (first_pass, 4), (first_done, 6), (first_pass, 5), (first_done, 7), (first_pass, 6),
        (first_pass, 7),
    ):
        stage(m)
    for which in range(2):
        for t in (tp_c, tp_xc):
            arrive(pool_slab(which, t), slab_recv.at[which, t])
    first_finish()
    flush()

    in_scale = jnp.concatenate([scales_all[t, :, :chans] for t in range(4)], axis=1)
    group = 4 * chans // 4
    pos_row = lax.broadcasted_iota(jnp.int32, (SEQ, SEQ), 0)
    pos_col = lax.broadcasted_iota(jnp.int32, (SEQ, SEQ), 1)
    pos = lax.broadcasted_iota(jnp.int32, (SEQ, 1), 0)

    def mix(base, count):
        part = pl.ds(pl.multiple_of(base, 128), count)
        pool_input = (jnp.dot(normed[part, :], in_all[...], preferred_element_type=f32) * in_scale).astype(half)
        for index, window in enumerate(WINDOWS):
            before = window // 2
            first = jnp.maximum(pos_row - before, 0)
            last = jnp.minimum(pos_row + window - before, SEQ)
            members = jnp.where((pos_col >= first) & (pos_col < last), 1.0, 0.0).astype(half)
            counts = (jnp.minimum(pos + window - before, SEQ) - jnp.maximum(pos - before, 0)).astype(f32)
            for s in range(count // SEQ):
                own = pool_input[s * SEQ:(s + 1) * SEQ, index * group:(index + 1) * group]
                sums = jnp.dot(members, own, preferred_element_type=f32)
                pooled[s * SEQ:(s + 1) * SEQ, index * group:(index + 1) * group] = (
                    sums / counts - own.astype(f32)).astype(half)
        for t in range(4):
            cols = slice(t * width, (t + 1) * width)
            mixed = jnp.dot(pooled[:count, :], out_all[:, cols], preferred_element_type=f32)
            mixed_all[part, cols] = (
                first_all[part, cols].astype(f32) + mixed * scales_all[t, :, chans:chans + width]).astype(half)

    order = [2 * xx + cc for cc in (1 - core, core) for xx in (1 - x, x)]
    sides = (1 - low, low)
    for h in range(2):
        for c, (first, count) in enumerate(cuts[h]):
            base = sides[h] * rows + first
            part = subs(base, count)
            lax.fori_loop(0, count // 128, norm_rows(first_all, 4, base), 0)
            mix(base, count)
            lax.fori_loop(0, count // 128, norm_rows(mixed_all, 5, base), 0)
            a = jnp.dot(normed[part, :], gate_all[...], preferred_element_type=f32) * vector(6, upper(z) * small, big)
            b = jnp.dot(normed[part, :], up_all[...], preferred_element_type=f32) * vector(7, upper(z) * small, big)
            hidden[part, :] = (a / (1.0 + jnp.exp(-a)) * b).astype(half)
            for n, zz in enumerate(order):
                product = jnp.dot(hidden[part, :], down_all[:, lanes(zz * width, width)], preferred_element_type=f32)
                for j in range(2):
                    partial[2 * zz + j, part, :] = product[:, j * block:(j + 1) * block].astype(half)
                for j in range(2):
                    part_send(2 * zz + j, h, c, base, count)
                if n > 1:
                    for j in range(2):
                        part_sum(2 * zz + j, h, c, base, first, count)

    for j in range(2):
        for k, h in ((0, 1), (1, 0), (2, 0)):
            for c, (first, count) in enumerate(cuts[h]):
                arrive(shares.at[k, j, pl.ds(first, count)], rs_recv.at[k, j, c])
        f = 2 * tp + j

        def total_rows(i, carry, j=j, f=f):
            at = pl.multiple_of(i * 128, 128)
            here = pl.ds(pl.multiple_of(low * rows + at, 128), 128)
            total = partial[f, here, :].astype(f32)
            for k in range(3):
                total = total + shares[k, j, pl.ds(at, 128), :].astype(f32)
            value = mixed_all[here, lanes(f * block, block)].astype(f32)
            out[pl.ds(at, 128), j * block:(j + 1) * block] = (
                value + total * (0.5 * vector(2, j * block, block))).astype(half)
            return carry
        lax.fori_loop(0, rows // 128, total_rows, 0)

    flush()


def fits(nfs, ntp, stream, gate, pool_in):
    ny, nz = fs_grid(nfs)
    tiles = gate.shape[1] // 128
    return (
        (ny, nz, ntp) == (2, 4, 4) and gate.shape[1] % 128 == 0 and tiles % 2 == 1 and tiles > 1
        and stream.shape[0] % SEQ == 0 and stream.shape[0] > SEQ and SEQ % 128 == 0 and pool_in.shape[1] % 128 == 0
        and gate.shape[0] % 128 == 0 and stream.shape[1] == 2 * gate.shape[0]
    )


def whole_layer(stream, weights, vectors):
    gate, up, down, pool_in, pool_out = weights
    rows, width = stream.shape
    block, units = gate.shape
    chans = pool_in.shape[1]
    features = 4 * width
    small = (units // 128 // 2) * 128
    extra = units - 2 * small
    big = small + extra
    every = 2 * rows
    f32, half = jnp.float32, jnp.bfloat16
    vmem = pl.BlockSpec(memory_space=pltpu.VMEM)
    hbm = pl.BlockSpec(memory_space=pltpu.HBM)
    dma = pltpu.SemaphoreType.DMA
    return pl.pallas_call(
        functools.partial(layer_kernel, (rows, small, extra)),
        name="whole_layer",
        out_shape=jax.ShapeDtypeStruct((rows, width), half),
        in_specs=[hbm] * (1 + len(weights) + len(vectors)),
        out_specs=vmem,
        scratch_shapes=[pltpu.VMEM((1, sum(v.shape[0] for v in vectors)), f32)] + [
            pltpu.VMEM(w.shape, half) for w in weights] + [pltpu.VMEM(w.shape, f32) for w in weights] + [
            pltpu.VMEM((features, big), half), pltpu.VMEM((features, big), half), pltpu.VMEM((big, features), half),
            pltpu.VMEM((features, 4 * chans), half), pltpu.VMEM((4 * chans, features), half),
            pltpu.VMEM((4, 1, chans + 2 * width), f32),
            pltpu.VMEM((every, features), half), pltpu.VMEM((every, features), half),
            pltpu.VMEM((every, features), half), pltpu.VMEM((every, features), half),
            pltpu.VMEM((every, big), f32), pltpu.VMEM((every, big), f32), pltpu.VMEM((every, big), half),
            pltpu.VMEM((rows, 4 * chans), half),
            pltpu.VMEM((8, every, block), half), pltpu.VMEM((2, 4, every, block), half),
            pltpu.VMEM((3, 2, rows, block), half), pltpu.VMEM((2, 4, rows, block), half),
            dma((5,)), dma((len(vectors),)), dma((10,)), dma((4, 3, 2)), dma((4, 3, 2)), dma((8, 3, 2)),
            dma((2, 4)), dma((2, 4)), dma((2, 8)), dma((2, 3)), dma((2, 4)),
            dma((3,)), dma((4,)), dma((2, 2, 7)), dma((2, 2, 4, 2)),
            dma((8, 2)), dma((4, 2)), dma((8, 2, 2)), dma((4, 2, 2)), dma((4, 3, 2)), dma((3, 2, 2)),
            dma((4, 5)), dma((4, 3)), dma((4, 2)),
        ],
        compiler_params=pltpu.CompilerParams(
            collective_id=0, has_side_effects=True, vmem_limit_bytes=55 << 20),
    )(stream, *weights, *vectors)


def body(
    nfs, ntp,
    stream, gain_first, gain_mixer, gain_second,
    gate_weight, gate_scale, up_weight, up_scale, down_weight, down_scale,
    pool_in_weight, pool_in_scale, pool_out_weight, pool_out_scale,
):
    half = jnp.bfloat16
    if fits(nfs, ntp, stream, gate_weight, pool_in_weight):
        return whole_layer(
            stream, (gate_weight, up_weight, down_weight, pool_in_weight, pool_out_weight),
            (pool_in_scale, pool_out_scale, down_scale, gain_first, gain_mixer, gain_second, gate_scale, up_scale))
    in_half, out_half = pool_in_weight.astype(half), pool_out_weight.astype(half)
    width, channels = stream.shape[1], in_half.shape[1]
    scales = jnp.concatenate([pool_in_scale, pool_out_scale]).reshape(1, -1)
    in_all, out_all, gate_all, up_all, down_all, stream_all, scales_all = gather_all(
        nfs, ntp, in_half, out_half, gate_weight.astype(half), up_weight.astype(half), down_weight.astype(half),
        stream, scales,
    )
    in_whole, out_whole = flat(in_all), flat(out_all)
    gate_whole, up_whole, down_whole = flat(gate_all), flat(up_all), flat(down_all)
    in_scale = scales_all[:, 0, :channels].reshape(-1)
    out_scale = scales_all[:, 0, channels:].reshape(-1)
    tp = lax.axis_index("tp")

    def feed_forward(rows):
        gate_sum = jnp.dot(rows, gate_whole, preferred_element_type=jnp.float32) * gate_scale
        up_sum = jnp.dot(rows, up_whole, preferred_element_type=jnp.float32) * up_scale
        hidden = (jax.nn.silu(gate_sum) * up_sum).astype(half)
        return jnp.dot(hidden, down_whole, preferred_element_type=jnp.float32).astype(half)

    first = rms(flat(stream_all).astype(jnp.float32), gain_first)
    after_first = summed(ntp, True, 1, feed_forward(first), stream, down_scale)
    mixer_normed = rms(after_first.astype(jnp.float32), gain_mixer)
    pool_input = (
        jnp.dot(mixer_normed, in_whole, preferred_element_type=jnp.float32) * in_scale
    ).astype(half)
    mixed = jnp.dot(pooling(pool_input), out_whole, preferred_element_type=jnp.float32)
    after_mix = (after_first.astype(jnp.float32) + mixed * out_scale).astype(half)
    second = rms(after_mix.astype(jnp.float32), gain_second)
    own = lax.dynamic_slice_in_dim(after_mix, tp * stream.shape[1], stream.shape[1], axis=1)
    return summed(ntp, False, 2, feed_forward(second), own, down_scale)


def solution(mesh):
    placed = (
        P("fs", "tp"), P(), P(), P(),
        P("fs", "tp"), P("tp"), P("fs", "tp"), P("tp"), P("tp", "fs"), P("tp"),
        P("fs", "tp"), P("tp"), P("tp", "fs"), P("tp"),
    )
    return jax.shard_map(
        functools.partial(body, mesh.shape["fs"], mesh.shape["tp"]),
        mesh=mesh, in_specs=placed, out_specs=P("fs", "tp"), check_vma=False,
    )
```

```python
import functools

import jax
import jax.numpy as jnp
from jax import lax
from jax.experimental import pallas as pl
from jax.experimental.pallas import tpu as pltpu
from jax.sharding import PartitionSpec as P

SEQ = 128
MESH = pl.DeviceIdType.MESH

eps = 1e-06
WINDOWS = (2, 4, 8, 16)
Z_FIRST = (3, 5, 7)


def fs_grid(count):
    ny = 1
    while (2 * ny) * (2 * ny) <= count and count % (2 * ny) == 0:
        ny *= 2
    return ny, count // ny


def grid_shape(row_blocks, col_blocks, block):
    rows, cols = block
    if cols % 128 == 0:
        return (row_blocks * rows, col_blocks * cols)
    return (row_blocks, col_blocks, rows, cols)


def place(whole, block, row_block, col_block, part=(0, None)):
    rows, cols = block
    first, count = part[0], rows if part[1] is None else part[1]
    if len(whole.shape) == 2:
        return whole.at[
            pl.ds(pl.multiple_of(row_block * rows + first, 16), count),
            pl.ds(pl.multiple_of(col_block * cols, 128), cols),
        ]
    return whole.at[row_block, col_block, pl.ds(first, count)]


def flat(whole):
    if whole.ndim == 2:
        return whole
    return whole.transpose(0, 2, 1, 3).reshape(whole.shape[0] * whole.shape[2], -1)


def gather_kernel(nfs, ntp, pool_in, pool_out, gate, up, down, stream, scales,
                  in_all, out_all, gate_all, up_all, down_all, stream_all, scales_all,
                  send_sem, recv_sem, local_sem, tsend, trecv, psend, precv, ssend, srecv):
    ny, nz = fs_grid(nfs)
    nx = ntp // 2
    fs, tp = lax.axis_index("fs"), lax.axis_index("tp")
    z, y = fs // ny, fs % ny
    x, core = tp // 2, tp % 2
    partner = x * 2 + (1 - core)
    alternate = ny == 2 and nz > 1

    barrier = pltpu.get_barrier_semaphore()

    def greet(cond, f, t):
        @pl.when(cond)
        def _():
            pl.semaphore_signal(barrier, inc=1, device_id={"fs": f, "tp": t}, device_id_type=MESH)

    greet(z > 0, fs - ny, tp)
    greet(z < nz - 1, fs + ny, tp)
    greet(y > 0, fs - 1, tp)
    greet(y < ny - 1, fs + 1, tp)
    for k in range(1, ntp):
        pl.semaphore_signal(
            barrier, inc=1, device_id={"fs": fs, "tp": (tp + k) % ntp}, device_id_type=MESH
        )
    peers = ntp - 1
    for cond in (z > 0, z < nz - 1, y > 0, y < ny - 1):
        peers = peers + jnp.where(cond, 1, 0)
    pl.semaphore_wait(barrier, peers)

    pieces = [
        (lambda: pool_in, lambda f: place(in_all, pool_in.shape, f, tp)),
        (lambda: pool_out, lambda f: place(out_all, pool_out.shape, tp, f)),
    ]
    npool = len(pieces)
    for own, whole, by_rows in ((gate, gate_all, True), (up, up_all, True), (down, down_all, False)):
        rows = own.shape[0]
        halves = 2 if alternate else 1
        for h in range(halves):
            part = (h * (rows // halves), rows // halves)

            def own_part(own=own, part=part):
                return own.at[pl.ds(*part)]

            def whole_part(f, own=own, whole=whole, part=part, by_rows=by_rows):
                return place(whole, own.shape, f if by_rows else 0, 0 if by_rows else f, part)

            pieces.append((own_part, whole_part))
    started = []

    def remote(piece, f, direction, target, mine=False):
        own, whole = pieces[piece]
        return pltpu.make_async_remote_copy(
            src_ref=own() if mine else whole(f),
            dst_ref=whole(f),
            send_sem=send_sem.at[piece, f, direction],
            recv_sem=recv_sem.at[piece, f],
            device_id={"fs": target, "tp": tp},
            device_id_type=MESH,
        )

    def send(cond, piece, f, direction, mine=False):
        target = fs + (-ny, ny, -1, 1)[direction]

        @pl.when(cond)
        def _():
            remote(piece, f, direction, target, mine).start()

        started.append((cond, piece, f, direction, target, mine))

    def arrived(cond, piece, f):
        @pl.when(cond)
        def _():
            remote(piece, f, 0, fs, False).wait_recv()

    def by_y(cond, piece, f, mine=False):
        send(cond & (y > 0), piece, f, 2, mine)
        send(cond & (y < ny - 1), piece, f, 3, mine)

    yes = z >= 0

    def stream_place(slot):
        return place(stream_all, stream.shape, 0, slot)

    def stream_copy(src, slot, t_target, k):
        return pltpu.make_async_remote_copy(
            src_ref=src, dst_ref=stream_place(slot), send_sem=tsend.at[k], recv_sem=trecv.at[slot],
            device_id={"fs": fs, "tp": t_target}, device_id_type=MESH)

    def slab(which, slot):
        if which == 0:
            if len(in_all.shape) == 2:
                cols = pool_in.shape[1]
                return in_all.at[:, pl.ds(pl.multiple_of(slot * cols, 128), cols)]
            return in_all.at[:, slot]
        if len(out_all.shape) == 2:
            rows = pool_out.shape[0]
            return out_all.at[pl.ds(pl.multiple_of(slot * rows, 16), rows)]
        return out_all.at[slot]

    def pool_copy(which, slot, t_target, k):
        return pltpu.make_async_remote_copy(
            src_ref=slab(which, slot), dst_ref=slab(which, slot),
            send_sem=psend.at[which, k], recv_sem=precv.at[which, slot],
            device_id={"fs": fs, "tp": t_target}, device_id_type=MESH)

    def scale_copy(k, slot, t_target):
        return pltpu.make_async_remote_copy(
            src_ref=scales, dst_ref=scales_all.at[slot], send_sem=ssend.at[k], recv_sem=srecv.at[slot],
            device_id={"fs": fs, "tp": t_target}, device_id_type=MESH)

    npieces = len(pieces)
    locals_ = [pltpu.make_async_copy(own(), whole(fs), local_sem.at[i]) for i, (own, whole) in enumerate(pieces)]
    locals_.append(pltpu.make_async_copy(stream, stream_place(tp), local_sem.at[npieces]))
    locals_.append(pltpu.make_async_copy(scales, scales_all.at[tp], local_sem.at[npieces + 1]))
    for piece in range(npieces):
        send(z > 0, piece, fs, 0, True)
        send(z < nz - 1, piece, fs, 1, True)
        by_y(yes, piece, fs, True)
    stream_sends = []
    for k in range(1, nx):
        stream_sends.append(stream_copy(stream, tp, (x + k) % nx * 2 + core, k - 1))
    stream_sends.append(stream_copy(stream, tp, partner, nx - 1))
    stream_sends += [scale_copy(k - 1, tp, (tp + k) % ntp) for k in range(1, ntp)]
    for copy in stream_sends:
        copy.start()
    for copy in locals_:
        copy.start()

    def row_arrivals(piece, d, alt):
        low, high = fs - d * ny, fs + d * ny
        has_low, has_high = z >= d, z + d <= nz - 1
        for cond, f, direction, ahead, end in (
            (has_low, low, 1, z < nz - 1, z == d),
            (has_high, high, 0, z > 0, z + d == nz - 1),
        ):
            arrived(cond, piece, f)
            send(cond & ahead, piece, f, direction)
            if alt:
                by_y(cond & jnp.logical_not(end), piece, f)
                other = f + 1 - 2 * y
                arrived(cond & end, piece, other)
                send(cond & end & ahead, piece, other, direction)
            else:
                by_y(cond, piece, f)

    def column_arrivals(piece, alt):
        for d in range(nz):
            for sign in ((1,) if d == 0 else (-1, 1)):
                row_ok = (z + sign * d >= 0) & (z + sign * d <= nz - 1)
                if alt:
                    at = z + sign * d
                    if d == 0:
                        continue
                    row_ok = row_ok & (at != 0) & (at != nz - 1)
                base = fs + sign * d * ny
                for e in range(1, ny):
                    for step, direction, ok, ahead in (
                        (-e, 3, y >= e, y < ny - 1),
                        (e, 2, y + e <= ny - 1, y > 0),
                    ):
                        arrived(row_ok & ok, piece, base + step)
                        if ny > 2:
                            send(row_ok & ok & ahead, piece, base + step, direction)

    is_alt = [alternate and p >= npool and p % 2 == 1 for p in range(npieces)]

    for d in range(1, nz):
        for p in range(npool):
            row_arrivals(p, d, False)
    pool_sends = []
    for p in range(npool):
        column_arrivals(p, False)
        locals_[p].wait()
        pool_sends += [pool_copy(p, tp, (x + k) % nx * 2 + core, k - 1) for k in range(1, nx)]
        pool_sends.append(pool_copy(p, tp, partner, nx - 1))
    for copy in pool_sends:
        copy.start()
    for k in range(1, nx):
        slot = (x + k) % nx * 2 + core
        stream_copy(stream, slot, partner, 0).wait_recv()
        copy = stream_copy(stream_place(slot), slot, partner, nx - 1 + k)
        copy.start()
        stream_sends.append(copy)

    for p in range(npieces):
        if is_alt[p]:
            other = fs + 1 - 2 * y
            arrived(yes, p, other)
            send(z == 0, p, other, 1)
            send(z == nz - 1, p, other, 0)
    for d in range(1, nz):
        for p in range(npool, npieces):
            row_arrivals(p, d, is_alt[p])
        if d == 1:
            for k in range(1, nx):
                slot = (x + k) % nx * 2 + core
                for p in range(npool):
                    pool_copy(p, slot, partner, 0).wait_recv()
                    copy = pool_copy(p, slot, partner, nx - 1 + k)
                    copy.start()
                    pool_sends.append(copy)
    for p in range(npool, npieces):
        column_arrivals(p, is_alt[p])
    for k in range(nx):
        slot = (x + k) % nx * 2 + (1 - core)
        stream_copy(stream, slot, partner, 0).wait_recv()
        for p in range(npool):
            pool_copy(p, slot, partner, 0).wait_recv()
    for k in range(1, ntp):
        scale_copy(0, (tp + k) % ntp, partner).wait_recv()
    for copy in locals_[npool:]:
        copy.wait()
    for copy in stream_sends + pool_sends:
        copy.wait_send()
    for cond, piece, f, direction, target, mine in started:
        @pl.when(cond)
        def _():
            remote(piece, f, direction, target, mine).wait_send()


def gather_all(nfs, ntp, pool_in, pool_out, gate, up, down, stream, scales):
    ny, nz = fs_grid(nfs)
    nx = ntp // 2
    npieces = 8 if (ny == 2 and nz > 1) else 5
    any_spec = pl.BlockSpec(memory_space=pl.ANY)
    shapes = (
        grid_shape(nfs, ntp, pool_in.shape),
        grid_shape(ntp, nfs, pool_out.shape),
        grid_shape(nfs, 1, gate.shape),
        grid_shape(nfs, 1, up.shape),
        grid_shape(1, nfs, down.shape),
        grid_shape(1, ntp, stream.shape),
    )
    dma = pltpu.SemaphoreType.DMA
    return pl.pallas_call(
        functools.partial(gather_kernel, nfs, ntp),
        name="collect_weights",
        out_shape=tuple(jax.ShapeDtypeStruct(shape, jnp.bfloat16) for shape in shapes)
        + (jax.ShapeDtypeStruct((ntp,) + scales.shape, jnp.float32),),
        in_specs=[any_spec] * 7,
        out_specs=[any_spec] * 7,
        scratch_shapes=[
            dma((npieces, nfs, 4)),
            dma((npieces, nfs)),
            dma((npieces + 2,)),
            dma((2 * nx,)),
            dma((ntp,)),
            dma((2, 2 * nx)),
            dma((2, ntp)),
            dma((ntp,)),
            dma((ntp,)),
        ],
        compiler_params=pltpu.CompilerParams(collective_id=0, has_side_effects=True, vmem_limit_bytes=1 << 20),
    )(pool_in, pool_out, gate, up, down, stream, scales)


def sum_kernel(ntp, gathers, pieces, partial, resid, scale, out, pair, pair_sum, cross, *sems):
    pair_send, pair_recv, cross_send, cross_recv = sems[:4]
    nx = ntp // 2
    tp, fs = lax.axis_index("tp"), lax.axis_index("fs")
    x, core = tp // 2, tp % 2
    partner = x * 2 + (1 - core)
    rows, width = resid.shape
    step = rows // pieces
    barrier = pltpu.get_barrier_semaphore()
    pl.semaphore_signal(barrier, inc=1, device_id={"fs": fs, "tp": partner}, device_id_type=MESH)
    for k in range(1, nx):
        pl.semaphore_signal(
            barrier, inc=1, device_id={"fs": fs, "tp": (x + k) % nx * 2 + core}, device_id_type=MESH
        )
    pl.semaphore_wait(barrier, nx)

    def remote(src, dst, send, recv, target):
        return pltpu.make_async_remote_copy(
            src_ref=src, dst_ref=dst, send_sem=send, recv_sem=recv,
            device_id={"fs": fs, "tp": target}, device_id_type=MESH)

    def columns(t):
        return pl.ds(pl.multiple_of(t * width, width), width)

    parts = [pl.ds(i * step, step) for i in range(pieces)]
    offsets = list(range(1, nx)) + [0]
    sends = []
    for k in offsets:
        for i, part in enumerate(parts):
            copy = remote(partial.at[part, columns((x + k) % nx * 2 + (1 - core))], pair.at[k, part],
                          pair_send.at[k, i], pair_recv.at[k, i], partner)
            copy.start()
            sends.append(copy)
    for k in offsets[:-1]:
        target = (x + k) % nx * 2 + core
        for i, part in enumerate(parts):
            remote(pair.at[k, part], pair.at[k, part], pair_send.at[k, i], pair_recv.at[k, i], partner).wait_recv()
            pair_sum[k - 1, part] = (
                partial[part, columns(target)].astype(jnp.float32) + pair[k, part].astype(jnp.float32)
            ).astype(jnp.bfloat16)
            copy = remote(pair_sum.at[k - 1, part], cross.at[k - 1, part],
                          cross_send.at[k - 1, i], cross_recv.at[k - 1, i], target)
            copy.start()
            sends.append(copy)
    factor = 0.5 * scale[...]
    for i, part in enumerate(parts):
        remote(pair.at[0, part], pair.at[0, part], pair_send.at[0, i], pair_recv.at[0, i], partner).wait_recv()
        total = partial[part, columns(tp)].astype(jnp.float32) + pair[0, part].astype(jnp.float32)
        for k in range(1, nx):
            remote(cross.at[k - 1, part], cross.at[k - 1, part], cross_send.at[k - 1, i],
                   cross_recv.at[k - 1, i], partner).wait_recv()
            total = total + cross[k - 1, part].astype(jnp.float32)
        result = (resid[part].astype(jnp.float32) + total * factor).astype(jnp.bfloat16)
        if not gathers:
            out[part] = result
            continue
        out[part, columns(tp)] = result
        gather_send, gather_recv = sems[4:]
        for k in range(1, nx):
            copy = remote(out.at[part, columns(tp)], out.at[part, columns(tp)], gather_send.at[k - 1, i], gather_recv.at[tp, i],
                          (x + k) % nx * 2 + core)
            copy.start()
            sends.append(copy)
        copy = remote(out.at[part, columns(tp)], out.at[part, columns(tp)], gather_send.at[nx - 1, i], gather_recv.at[tp, i], partner)
        copy.start()
        sends.append(copy)
    if gathers:
        for k in range(1, nx):
            slot = (x + k) % nx * 2 + core
            for i, part in enumerate(parts):
                remote(out.at[part, columns(slot)], out.at[part, columns(slot)], gather_send.at[0, i], gather_recv.at[slot, i],
                       partner).wait_recv()
                copy = remote(out.at[part, columns(slot)], out.at[part, columns(slot)], gather_send.at[nx - 1 + k, i],
                              gather_recv.at[slot, i], partner)
                copy.start()
                sends.append(copy)
        for k in range(nx):
            slot = (x + k) % nx * 2 + (1 - core)
            for i, part in enumerate(parts):
                remote(out.at[part, columns(slot)], out.at[part, columns(slot)], gather_send.at[0, i], gather_recv.at[slot, i],
                       partner).wait_recv()
    for copy in sends:
        copy.wait_send()


def summed(ntp, gathers, identity, partial, resid, scale):
    nx = ntp // 2
    rows, width = resid.shape
    pieces = 3 if rows % 48 == 0 else 1
    vmem = pl.BlockSpec(memory_space=pltpu.VMEM)
    dma = pltpu.SemaphoreType.DMA
    scratch = [
        pltpu.VMEM((nx, rows, width), jnp.bfloat16),
        pltpu.VMEM((max(nx - 1, 1), rows, width), jnp.bfloat16),
        pltpu.VMEM((max(nx - 1, 1), rows, width), jnp.bfloat16),
        dma((nx, pieces)), dma((nx, pieces)), dma((nx, pieces)), dma((nx, pieces)),
    ]
    if gathers:
        scratch += [dma((2 * nx, pieces)), dma((ntp, pieces))]
    return pl.pallas_call(
        functools.partial(sum_kernel, ntp, gathers, pieces),
        name="sum_and_share" if gathers else "sum_last",
        out_shape=jax.ShapeDtypeStruct((rows, width * (ntp if gathers else 1)), jnp.bfloat16),
        in_specs=[vmem] * 3,
        out_specs=vmem,
        scratch_shapes=scratch,
        compiler_params=pltpu.CompilerParams(
            collective_id=identity, has_side_effects=True, vmem_limit_bytes=32 << 20
        ),
    )(partial, resid, scale.reshape(1, width))


def rms(floats, norm_gain):
    scaled = floats * lax.rsqrt(jnp.mean(floats * floats, axis=-1, keepdims=True) + eps)
    return (scaled * norm_gain).astype(jnp.bfloat16)


def window_weights():
    position = jnp.arange(SEQ)
    rows, cols = position[:, None], position[None, :]
    mats = []
    for window in WINDOWS:
        low = jnp.maximum(rows - window // 2, 0)
        high = jnp.minimum(rows + window - window // 2, SEQ)
        mats.append(((cols >= low) & (cols < high)).astype(jnp.bfloat16))
    return mats


def pooling(pool_input):
    channels = pool_input.shape[1]
    group = channels // 4
    values = pool_input.reshape(-1, SEQ, channels)
    position = jnp.arange(SEQ)
    parts = []
    for index, (window, members) in enumerate(zip(WINDOWS, window_weights())):
        own = values[:, :, index * group:(index + 1) * group]
        sums = jnp.einsum("pq,sqc->spc", members, own, preferred_element_type=jnp.float32)
        before = window // 2
        counts = (
            jnp.minimum(position + window - before, SEQ) - jnp.maximum(position - before, 0)
        ).astype(jnp.float32)
        parts.append(sums / counts[None, :, None] - own.astype(jnp.float32))
    return jnp.concatenate(parts, axis=2).reshape(-1, channels).astype(jnp.bfloat16)


def layer_kernel(
    sizes, stream, gate_in, up_in, down_in, in_in, out_in, *refs):
    parts, (out, vectors, *rest) = refs[:8], refs[8:]
    layer_steps(sizes, stream, gate_in, up_in, down_in, in_in, out_in, parts, out, vectors, *rest)


def layer_steps(
    sizes, stream, gate_in, up_in, down_in, in_in, out_in, parts, out, vectors,
    gate, up, down, pool_in, pool_out, gate_wide, up_wide, down_wide, in_wide, out_wide,
    gate_all, up_all, down_all, in_all, out_all, scales_all, rows_all, first_all, mixed_all, normed,
    gate_sum, up_sum, hidden, pooled, partial, pair, shares, first_in,
    load_sem, vector_sem, local_sem, z_send, y_send, w_recv, pl_zsend, pl_ysend, pl_recv, slab_send, slab_recv,
    sc_send, sc_recv, ag_send, ag_recv, pair_send, pair_recv, two_send, two_recv, rs_send, rs_recv,
    fr_send, fr_recv, fr_core,
):
    rows, small, extra = sizes
    big = small + extra
    block = gate.shape[0]
    width = stream.shape[1]
    chans = pool_in.shape[1]
    units = gate.shape[1]
    features = gate_all.shape[0]
    starts = [0]
    for count in (chans, width, width, features, features, features, units, units):
        starts.append(starts[-1] + count)
    scales = vectors.at[:, :chans + 2 * width]

    def vector(at, first, count):
        return vectors[:, pl.ds(pl.multiple_of(starts[at] + first, 128), count)]

    every = 2 * rows
    f32, half = jnp.float32, jnp.bfloat16
    fs, tp = lax.axis_index("fs"), lax.axis_index("tp")
    z, y = fs // 2, fs % 2
    x, core = tp // 2, tp % 2
    low, pair_hi = z % 2, z // 2
    zp = z + 1 - 2 * low
    zs = [z, zp, 2 - pair_hi, 3 - 3 * pair_hi]
    fs_y, fs_z = fs + 1 - 2 * y, 2 * zp + y
    tp_c, tp_x = tp + 1 - 2 * core, (tp + 2) % 4
    tp_xc = tp_x + 1 - 2 * core

    def upper(at):
        return (((at + 1) // 2) % 2 + core) % 2

    own_rows = pl.ds(pl.multiple_of(low * rows, 16), rows)
    stream_own = pltpu.make_async_copy(
        stream, rows_all.at[own_rows, pl.ds(pl.multiple_of(tp * width, 128), width)], local_sem.at[0])
    stream_own.start()
    vector_copies = [
        pltpu.make_async_copy(ref, vectors.at[0, pl.ds(first, ref.shape[0])], vector_sem.at[i])
        for i, (ref, first) in enumerate(zip(parts, starts))]
    for copy in vector_copies:
        copy.start()
    loads = []
    for i, (wide, ref, narrow) in enumerate((
        (in_wide, in_in, pool_in), (out_wide, out_in, pool_out), (gate_wide, gate_in, gate),
        (up_wide, up_in, up), (down_wide, down_in, down),
    )):
        copy = pltpu.make_async_copy(ref, wide, load_sem.at[i])
        copy.start()
        loads.append((copy, wide, narrow))

    barrier = pltpu.get_barrier_semaphore()
    peers = [(2 * at + y, tp) for at in zs[1:]] + [
        (fs_y, tp), (fs, tp_c), (fs, tp_x), (fs, tp_xc), (fs_z, tp_x)]
    for f, t in peers:
        pl.semaphore_signal(barrier, inc=1, device_id={"fs": f, "tp": t}, device_id_type=MESH)

    def narrowed(copy, wide, narrow):
        copy.wait()
        count = wide.shape[0]
        each = 64 if count % 64 == 0 else 16

        def one(i, carry):
            part = pl.ds(pl.multiple_of(i * each, each), each)
            narrow[part, :] = wide[part, :].astype(half)
            return carry
        lax.fori_loop(0, count // each, one, 0)

    for load in loads:
        narrowed(*load)
    stream_own.wait()
    for copy in vector_copies:
        copy.wait()
    pl.semaphore_wait(barrier, len(peers))

    ends = []

    def remote(src, dst, send, recv, f, t):
        return pltpu.make_async_remote_copy(
            src_ref=src, dst_ref=dst, send_sem=send, recv_sem=recv,
            device_id={"fs": f, "tp": t}, device_id_type=MESH)

    def start(make, cond=None):
        if cond is None:
            make().start()
        else:
            pl.when(cond)(lambda: make().start())
        ends.append((make, cond))

    def flush():
        for make, cond in ends:
            if cond is None:
                make().wait_send()
            else:
                pl.when(cond)(lambda make=make: make().wait_send())
        ends.clear()

    def arrive(dst, recv, cond=None):
        def wait():
            remote(dst, dst, recv, recv, fs, tp_c).wait_recv()
        if cond is None:
            wait()
        else:
            pl.when(cond)(wait)

    def lanes(at, count):
        return pl.ds(pl.multiple_of(at, 128), count)

    def subs(at, count):
        return pl.ds(pl.multiple_of(at, 16), count)

    pieces = width // block

    def column_block(j, xx, cc):
        return (2 * xx + cc) * pieces + j

    def share_place(phase, ref, chip_low, j, xx, cc):
        return ref.at[subs(chip_low * rows, rows), lanes(column_block(j, xx, cc) * block, block)]

    def share_start(phase, ref, j, cond=None):
        here = share_place(phase, ref, low, j, x, core)
        for k, (f, t) in enumerate(((fs_z, tp), (fs, tp_x), (fs, tp_c))):
            start(lambda f=f, t=t, k=k: remote(
                here, here, ag_send.at[phase, j, k], ag_recv.at[phase, j, 2 * x + low, core], f, t), cond)

    def share_relay(phase, ref, j, k, chip_low, xx, targets, cond=None):
        here = share_place(phase, ref, chip_low, j, xx, core)
        flag = ag_recv.at[phase, j, 2 * xx + chip_low, core]
        arrive(here, flag, cond)
        for n, target in enumerate(targets):
            start(lambda n=n, target=target: remote(
                here, here, ag_send.at[phase, j, 3 + k + n], flag, fs, target), cond)

    def relay_own(phase, ref, j, cond=None):
        share_relay(phase, ref, j, 0, 1 - low, x, (tp_x, tp_c), cond)

    def relay_across(phase, ref, j, cond=None):
        share_relay(phase, ref, j, 2, low, 1 - x, (tp_c,), cond)
        share_relay(phase, ref, j, 3, 1 - low, 1 - x, (tp_c,), cond)

    def share_finish(phase, ref):
        for j in range(2):
            for xx in (x, 1 - x):
                for cl in (low, 1 - low):
                    arrive(share_place(phase, ref, cl, j, xx, 1 - core), ag_recv.at[phase, j, 2 * xx + cl, 1 - core])

    for j in range(2):
        share_start(0, rows_all, j)

    def scale_copy(k, slot, t):
        return remote(scales, scales_all.at[slot], sc_send.at[k], sc_recv.at[slot], fs, t)

    for k, t in enumerate((tp_c, tp_x, tp_xc)):
        start(lambda k=k, t=t: scale_copy(k, tp, t))
    locals_ = [pltpu.make_async_copy(scales, scales_all.at[tp], local_sem.at[1])]

    def pool_place(which, f, t):
        if which == 0:
            return in_all.at[subs(f * block, block), lanes(t * chans, chans)]
        return out_all.at[subs(t * chans, chans), lanes(f * block, block)]

    def pool_slab(which, t):
        if which == 0:
            return in_all.at[:, lanes(t * chans, chans)]
        return out_all.at[subs(t * chans, chans)]

    def pool_start():
        for which, own in enumerate((pool_in, pool_out)):
            for k in range(1, 4):
                start(lambda k=k, which=which, own=own: remote(
                    own, pool_place(which, fs, tp), pl_zsend.at[which, k], pl_recv.at[which, fs], 2 * zs[k] + y, tp))
            start(lambda which=which, own=own: remote(
                own, pool_place(which, fs, tp), pl_ysend.at[which, 0], pl_recv.at[which, fs], fs_y, tp))

    for which, own in enumerate((pool_in, pool_out)):
        locals_.append(pltpu.make_async_copy(own, pool_place(which, fs, tp), local_sem.at[2 + which]))

    PARTS = 3

    def own_part(piece, part, side):
        first = 2 * small if part == 2 else side * small
        if piece == 2:
            return down.at[subs(first + part % 2 * (small // 2), extra if part == 2 else small // 2)]
        ref = (gate, up)[piece]
        if part == 2:
            return ref.at[:, lanes(first, extra)]
        return ref.at[pl.ds(part * (block // 2), block // 2), lanes(first, small)]

    def all_part(piece, part, f):
        if piece == 2:
            at, count = (small, extra) if part == 2 else (part * (small // 2), small // 2)
            return down_all.at[pl.ds(at, count), lanes(f * block, block)]
        ref = (gate_all, up_all)[piece]
        if part == 2:
            return ref.at[subs(f * block, block), pl.ds(small, extra)]
        return ref.at[subs(f * block + part * (block // 2), block // 2), pl.ds(0, small)]

    def part_cond(part, wide, cond=None):
        if part < 2:
            return cond
        return wide == 1 if cond is None else cond & (wide == 1)

    def y_own(piece):
        for part in range(PARTS):
            start(lambda part=part: remote(
                own_part(piece, part, upper(z)), all_part(piece, part, fs), y_send.at[0, piece, part],
                w_recv.at[fs, piece, part], fs_y, tp), part_cond(part, upper(z)))

    def own_copy(piece, part):
        return pltpu.make_async_copy(
            own_part(piece, part, upper(z)), all_part(piece, part, fs), local_sem.at[4 + PARTS * piece + part])

    for copy in locals_:
        copy.start()
    inner = (z == 1) | (z == 2)

    def z_own(piece, cond=None, targets=(1, 2, 3)):
        for k in targets:
            at = zs[k]
            for part in range(PARTS):
                ok = part_cond(part, upper(at), cond)
                start(lambda k=k, at=at, part=part: remote(
                    own_part(piece, part, upper(at)), all_part(piece, part, fs), z_send.at[k, piece, part],
                    w_recv.at[fs, piece, part], 2 * at + y, tp), ok)

    outer = jnp.logical_not(inner)
    z_own(0, None, (1,))
    y_own(0)
    z_own(1, outer, (1,))
    z_own(0, None, (2, 3))
    pool_start()
    z_own(1, inner, (1,))
    z_own(1, None, (2, 3))
    y_own(1)
    y_own(2)
    z_own(2, None, (1,))
    for piece in range(3):
        own_copy(piece, 0).start()
        own_copy(piece, 1).start()
        pl.when(upper(z) == 1)(lambda piece=piece: own_copy(piece, 2).start())

    @pl.when(upper(z) == 0)
    def _():
        gate_all[:, small:big] = jnp.zeros((features, extra), half)
        up_all[:, small:big] = jnp.zeros((features, extra), half)
        down_all[small:big, :] = jnp.zeros((extra, features), half)

    def weights_here(piece, f):
        for part in range(PARTS):
            arrive(all_part(piece, part, f), w_recv.at[f, piece, part], part_cond(part, upper(z)))

    def by_z(piece, i):
        f = 2 * zs[i] + y
        for part in range(PARTS):
            cond = part_cond(part, upper(z))
            arrive(all_part(piece, part, f), w_recv.at[f, piece, part], cond)
            start(lambda part=part: remote(
                all_part(piece, part, f), all_part(piece, part, f), y_send.at[i, piece, part],
                w_recv.at[f, piece, part], fs_y, tp), cond)

    def own_here(piece):
        own_copy(piece, 0).wait()
        own_copy(piece, 1).wait()
        pl.when(upper(z) == 1)(lambda: own_copy(piece, 2).wait())

    step = 32
    lane_tiles = features // 128

    def norm_rows(source, gain_at, base=0):
        def one(i, carry):
            part = pl.ds(pl.multiple_of(base + i * 128, 128), 128)
            total = jnp.zeros((128, 128), f32)
            for c in range(lane_tiles):
                floats = source[part, c * 128:(c + 1) * 128].astype(f32)
                total = total + floats * floats
            scale = lax.rsqrt(jnp.sum(total, axis=-1, keepdims=True) * (1.0 / features) + eps)
            for c in range(lane_tiles):
                floats = source[part, c * 128:(c + 1) * 128].astype(f32)
                normed[part, c * 128:(c + 1) * 128] = ((floats * scale) * vector(gain_at, c * 128, 128)).astype(half)
            return carry
        return one

    for j in range(2):
        relay_own(0, rows_all, j)
    for j in range(2):
        relay_across(0, rows_all, j)
    share_finish(0, rows_all)
    lax.fori_loop(0, every // 128, norm_rows(rows_all, 3), 0)

    def pool_by_y():
        for k in range(1, 4):
            for which in range(2):
                f = 2 * zs[k] + y
                here = pool_place(which, f, tp)
                arrive(here, pl_recv.at[which, f])
                start(lambda k=k, which=which, here=here, f=f: remote(
                    here, here, pl_ysend.at[which, k], pl_recv.at[which, f], fs_y, tp))

    tile = 256

    def accumulate(weights, total, f, first):
        for n in range(big // 128 // 2 + 1):
            cols = slice(n * tile, min((n + 1) * tile, big))
            if cols.start < cols.stop:
                product = jnp.dot(normed[:, lanes(f * block, block)], weights[subs(f * block, block), cols],
                                  preferred_element_type=f32)
                total[:, cols] = product if first else total[:, cols] + product

    def pool_across():
        for which in range(2):
            locals_[1 + which].wait()
            for k in range(4):
                f = fs_y if k == 0 else 2 * zs[k] + 1 - y
                arrive(pool_place(which, f, tp), pl_recv.at[which, f])
            slab = pool_slab(which, tp)
            for n, t in enumerate((tp_x, tp_c)):
                start(lambda which=which, slab=slab, n=n, t=t: remote(
                    slab, slab, slab_send.at[which, n], slab_recv.at[which, tp], fs, t))

    ahead = [(piece, i) for piece in range(3) for i in range(1, 4)]
    for piece, (weights, total) in enumerate(((gate_all, gate_sum), (up_all, up_sum))):
        for i in range(4):
            f, g = 2 * zs[i] + y, 2 * zs[i] + 1 - y
            if i == 0:
                own_here(piece)
            accumulate(weights, total, f, i == 0)
            if 4 * piece + i < 7:
                by_z(*ahead[4 * piece + i])
            weights_here(piece, g)
            accumulate(weights, total, g, False)
            if (piece, i) == (0, 2):
                pool_by_y()
            if (piece, i) == (1, 0):
                z_own(2, inner, (2, 3))
                pool_across()
            if (piece, i) == (1, 1):
                z_own(2, outer, (2, 3))
    own_here(2)

    def hide(i, carry):
        part = pl.ds(pl.multiple_of(i * step, step), step)
        a = gate_sum[part, :] * vector(6, upper(z) * small, big)
        hidden[part, :] = (a / (1.0 + jnp.exp(-a)) * (up_sum[part, :] * vector(7, upper(z) * small, big))).astype(half)
        return carry

    lax.fori_loop(0, every // step, hide, 0)

    def block_send(f, r):
        zz = f // 2
        slot = 2 * (zz // 2) + f % 2
        part = subs(r * rows, rows)
        start(lambda: remote(
            partial.at[f, part], pair.at[0, slot, part], pair_send.at[f, r],
            pair_recv.at[slot, r], fs, tp_c), zz % 2 != core)

    def core_sum(f, r):
        slot = 2 * (f // 4) + f % 2

        @pl.when((f // 2) % 2 == core)
        def _():
            here = pair.at[0, slot, subs(r * rows, rows)]
            remote(here, here, pair_send.at[f, r], pair_recv.at[slot, r], fs, tp_c).wait_recv()

            def one(i, carry):
                at = pl.ds(pl.multiple_of(r * rows + i * 128, 128), 128)
                partial[f, at, :] = (
                    partial[f, at, :].astype(f32) + pair[0, slot, at, :].astype(f32)).astype(half)
                return carry
            lax.fori_loop(0, rows // 128, one, 0)

    pair_z = (jnp.where(low == core, zp, z), jnp.where(low == core, z, zp), zs[2], zs[3])
    blocks = [2 * zz + j for zz in pair_z for j in (y, 1 - y)]

    def ways(n):
        across_x, across_z = (fs, tp_x), (fs_z, tp)
        return (across_z, across_x, low) if n in Z_FIRST else (across_x, across_z, x)

    def first_send(n, k, src, dst, recv, to):
        f = blocks[n]
        start(lambda: remote(src, dst, fr_send.at[2 * (f // 4) + f % 2, k], recv, *to), (f // 2) % 2 == core)

    def first_sum(n):
        f = blocks[n]
        slot = 2 * (f // 4) + f % 2
        to, _, r = ways(n)
        core_sum(f, 1 - r)
        first_send(n, 0, partial.at[f, subs((1 - r) * rows, rows)], first_in.at[0, slot], fr_recv.at[slot, 0], to)
        core_sum(f, r)

    def first_add(n):
        f = blocks[n]
        slot = 2 * (f // 4) + f % 2
        _, to, r = ways(n)
        part = subs(r * rows, rows)

        @pl.when((f // 2) % 2 == core)
        def _():
            arrive(first_in.at[0, slot], fr_recv.at[slot, 0])

            def one(i, carry):
                at = pl.ds(pl.multiple_of(r * rows + i * 128, 128), 128)
                got = first_in[0, slot, pl.ds(pl.multiple_of(i * 128, 128), 128), :].astype(f32)
                partial[f, at, :] = (partial[f, at, :].astype(f32) + got).astype(half)
                return carry
            lax.fori_loop(0, rows // 128, one, 0)
        first_send(n, 1, partial.at[f, part], first_in.at[1, slot], fr_recv.at[slot, 1], to)

    def first_done(n):
        f = blocks[n]
        slot = 2 * (f // 4) + f % 2
        to, _, r = ways(n)
        cols = lanes(f * block, block)

        @pl.when((f // 2) % 2 == core)
        def _():
            arrive(first_in.at[1, slot], fr_recv.at[slot, 1])
            factor = 0.5 * scales_all[f // 2, :, pl.ds(pl.multiple_of(chans + width + (f % 2) * block, 128), block)]

            def one(i, carry):
                at = pl.ds(pl.multiple_of(r * rows + i * 128, 128), 128)
                total = partial[f, at, :].astype(f32) + first_in[
                    1, slot, pl.ds(pl.multiple_of(i * 128, 128), 128), :].astype(f32)
                first_all[at, cols] = (rows_all[at, cols].astype(f32) + total * factor).astype(half)
                return carry
            lax.fori_loop(0, rows // 128, one, 0)
        here = first_all.at[subs(r * rows, rows), cols]
        first_send(n, 2, here, here, fr_recv.at[slot, 2], to)
        first_send(n, 3, here, here, fr_core.at[slot, r], (fs, tp_c))

    def first_pass(n):
        f = blocks[n]
        slot = 2 * (f // 4) + f % 2
        r = 1 - ways(n)[2]
        here = first_all.at[subs(r * rows, rows), lanes(f * block, block)]
        arrive(here, fr_recv.at[slot, 2], (f // 2) % 2 == core)
        first_send(n, 4, here, here, fr_core.at[slot, r], (fs, tp_c))

    def first_finish():
        for f in blocks:
            slot = 2 * (f // 4) + f % 2
            for r in range(2):
                arrive(first_all.at[r * rows:(r + 1) * rows, lanes(f * block, block)], fr_core.at[slot, r],
                       (f // 2) % 2 != core)

    def part_send(f, h, c, base, count):
        slot = 2 * (f // 4) + f % 2
        part = subs(base, count)
        start(lambda: remote(
            partial.at[f, part], pair.at[1, slot, part], two_send.at[f, h, c], two_recv.at[slot, h, c], fs, tp_c),
            (f // 2) % 2 != core)

    def part_sum(f, h, c, base, first, count):
        slot = 2 * (f // 4) + f % 2
        part = subs(base, count)

        @pl.when((f // 2) % 2 == core)
        def _():
            arrive(pair.at[1, slot, part], two_recv.at[slot, h, c])

            def one(i, carry):
                at = pl.ds(pl.multiple_of(base + i * 128, 128), 128)
                partial[f, at, :] = (partial[f, at, :].astype(f32) + pair[1, slot, at, :].astype(f32)).astype(half)
                return carry
            lax.fori_loop(0, count // 128, one, 0)
        mine = f // 4 == x
        away = jnp.logical_not(mine)
        ways = ((1, fs_z, tp, mine), (2, fs_z, tp_x, away)) if h == 0 else ((0, fs, tp_x, away),)
        for k, fd, td, cond in ways:
            start(lambda k=k, fd=fd, td=td: remote(
                partial.at[f, part], shares.at[k, f % 2, pl.ds(first, count)], rs_send.at[slot, k, c],
                rs_recv.at[k, f % 2, c], fd, td), ((f // 2) % 2 == core) & cond)

    cuts = (((0, SEQ), (SEQ, rows - SEQ)), ((0, rows - SEQ), (rows - SEQ, SEQ)))

    def slab_across():
        for which in range(2):
            slab = pool_slab(which, tp_x)
            arrive(slab, slab_recv.at[which, tp_x])
            start(lambda which=which, slab=slab: remote(
                slab, slab, slab_send.at[which, 2], slab_recv.at[which, tp_x], fs, tp_c))

    locals_[0].wait()
    for t in (tp_c, tp_x, tp_xc):
        arrive(scales_all.at[t], sc_recv.at[t])
    def product_of(n):
        f = blocks[n]
        if n % 2:
            weights_here(2, f)
        partial[f, :, :] = jnp.dot(
            hidden[...], down_all[:, lanes(f * block, block)], preferred_element_type=f32).astype(half)
        for r in (1 - ways(n)[2], ways(n)[2]):
            block_send(f, r)

    def down_from(n):
        by_z(2, n)

    def slab(n):
        slab_across()

    for stage, members in (
        (product_of, (0, 1, 2, 3)), (first_sum, (2, 3)), (slab, (0,)), (first_add, (2, 3)), (down_from, (2,)),
        (product_of, (4,)), (down_from, (3,)), (product_of, (6,)), (first_sum, (4, 6)), (first_done, (2, 3)),
        (first_add, (4, 6)), (product_of, (5,)), (first_sum, (5,)), (first_pass, (2, 3)), (first_done, (4, 6)),
        (product_of, (7,)), (first_sum, (7,)), (first_add, (5,)), (first_pass, (4, 6)), (first_done, (5,)),
        (first_add, (7,)), (first_pass, (5,)), (first_done, (7,)), (first_pass, (7,)),
    ):
        for m in members:
            stage(m)
    for which in range(2):
        for t in (tp_c, tp_xc):
            arrive(pool_slab(which, t), slab_recv.at[which, t])
    first_finish()
    flush()

    in_scale = jnp.concatenate([scales_all[t, :, :chans] for t in range(4)], axis=1)
    group = 4 * chans // 4
    pos_row = lax.broadcasted_iota(jnp.int32, (SEQ, SEQ), 0)
    pos_col = lax.broadcasted_iota(jnp.int32, (SEQ, SEQ), 1)
    pos = lax.broadcasted_iota(jnp.int32, (SEQ, 1), 0)

    def mix(base, count):
        part = pl.ds(pl.multiple_of(base, 128), count)
        pool_input = (jnp.dot(normed[part, :], in_all[...], preferred_element_type=f32) * in_scale).astype(half)
        for index, window in enumerate(WINDOWS):
            before = window // 2
            first = jnp.maximum(pos_row - before, 0)
            last = jnp.minimum(pos_row + window - before, SEQ)
            members = jnp.where((pos_col >= first) & (pos_col < last), 1.0, 0.0).astype(half)
            counts = (jnp.minimum(pos + window - before, SEQ) - jnp.maximum(pos - before, 0)).astype(f32)
            for s in range(count // SEQ):
                own = pool_input[s * SEQ:(s + 1) * SEQ, index * group:(index + 1) * group]
                sums = jnp.dot(members, own, preferred_element_type=f32)
                pooled[s * SEQ:(s + 1) * SEQ, index * group:(index + 1) * group] = (
                    sums / counts - own.astype(f32)).astype(half)
        for t in range(4):
            cols = slice(t * width, (t + 1) * width)
            mixed = jnp.dot(pooled[:count, :], out_all[:, cols], preferred_element_type=f32)
            mixed_all[part, cols] = (
                first_all[part, cols].astype(f32) + mixed * scales_all[t, :, chans:chans + width]).astype(half)

    order = [2 * xx + cc for cc in (1 - core, core) for xx in (1 - x, x)]
    sides = (1 - low, low)
    for h in range(2):
        for c, (first, count) in enumerate(cuts[h]):
            base = sides[h] * rows + first
            part = subs(base, count)
            lax.fori_loop(0, count // 128, norm_rows(first_all, 4, base), 0)
            mix(base, count)
            lax.fori_loop(0, count // 128, norm_rows(mixed_all, 5, base), 0)
            a = jnp.dot(normed[part, :], gate_all[...], preferred_element_type=f32) * vector(6, upper(z) * small, big)
            b = jnp.dot(normed[part, :], up_all[...], preferred_element_type=f32) * vector(7, upper(z) * small, big)
            hidden[part, :] = (a / (1.0 + jnp.exp(-a)) * b).astype(half)
            for n, zz in enumerate(order):
                product = jnp.dot(hidden[part, :], down_all[:, lanes(zz * width, width)], preferred_element_type=f32)
                for j in range(2):
                    partial[2 * zz + j, part, :] = product[:, j * block:(j + 1) * block].astype(half)
                for j in range(2):
                    part_send(2 * zz + j, h, c, base, count)
                if n > 1:
                    for j in range(2):
                        part_sum(2 * zz + j, h, c, base, first, count)

    for j in range(2):
        for k, h in ((0, 1), (1, 0), (2, 0)):
            for c, (first, count) in enumerate(cuts[h]):
                arrive(shares.at[k, j, pl.ds(first, count)], rs_recv.at[k, j, c])
        f = 2 * tp + j

        def total_rows(i, carry, j=j, f=f):
            at = pl.multiple_of(i * 128, 128)
            here = pl.ds(pl.multiple_of(low * rows + at, 128), 128)
            total = partial[f, here, :].astype(f32)
            for k in range(3):
                total = total + shares[k, j, pl.ds(at, 128), :].astype(f32)
            value = mixed_all[here, lanes(f * block, block)].astype(f32)
            out[pl.ds(at, 128), j * block:(j + 1) * block] = (
                value + total * (0.5 * vector(2, j * block, block))).astype(half)
            return carry
        lax.fori_loop(0, rows // 128, total_rows, 0)

    flush()


def fits(nfs, ntp, stream, gate, pool_in):
    ny, nz = fs_grid(nfs)
    tiles = gate.shape[1] // 128
    return (
        (ny, nz, ntp) == (2, 4, 4) and gate.shape[1] % 128 == 0 and tiles % 2 == 1 and tiles > 1
        and stream.shape[0] % SEQ == 0 and stream.shape[0] > SEQ and SEQ % 128 == 0 and pool_in.shape[1] % 128 == 0
        and gate.shape[0] % 128 == 0 and stream.shape[1] == 2 * gate.shape[0]
    )


def whole_layer(stream, weights, vectors):
    gate, up, down, pool_in, pool_out = weights
    rows, width = stream.shape
    block, units = gate.shape
    chans = pool_in.shape[1]
    features = 4 * width
    small = (units // 128 // 2) * 128
    extra = units - 2 * small
    big = small + extra
    every = 2 * rows
    f32, half = jnp.float32, jnp.bfloat16
    vmem = pl.BlockSpec(memory_space=pltpu.VMEM)
    hbm = pl.BlockSpec(memory_space=pltpu.HBM)
    dma = pltpu.SemaphoreType.DMA
    return pl.pallas_call(
        functools.partial(layer_kernel, (rows, small, extra)),
        name="whole_layer",
        out_shape=jax.ShapeDtypeStruct((rows, width), half),
        in_specs=[hbm] * (1 + len(weights) + len(vectors)),
        out_specs=vmem,
        scratch_shapes=[pltpu.VMEM((1, sum(v.shape[0] for v in vectors)), f32)] + [
            pltpu.VMEM(w.shape, half) for w in weights] + [pltpu.VMEM(w.shape, f32) for w in weights] + [
            pltpu.VMEM((features, big), half), pltpu.VMEM((features, big), half), pltpu.VMEM((big, features), half),
            pltpu.VMEM((features, 4 * chans), half), pltpu.VMEM((4 * chans, features), half),
            pltpu.VMEM((4, 1, chans + 2 * width), f32),
            pltpu.VMEM((every, features), half), pltpu.VMEM((every, features), half),
            pltpu.VMEM((every, features), half), pltpu.VMEM((every, features), half),
            pltpu.VMEM((every, big), f32), pltpu.VMEM((every, big), f32), pltpu.VMEM((every, big), half),
            pltpu.VMEM((rows, 4 * chans), half),
            pltpu.VMEM((8, every, block), half), pltpu.VMEM((2, 4, every, block), half),
            pltpu.VMEM((3, 2, rows, block), half), pltpu.VMEM((2, 4, rows, block), half),
            dma((5,)), dma((len(vectors),)), dma((13,)), dma((4, 3, 3)), dma((4, 3, 3)), dma((8, 3, 3)),
            dma((2, 4)), dma((2, 4)), dma((2, 8)), dma((2, 3)), dma((2, 4)),
            dma((3,)), dma((4,)), dma((2, 2, 7)), dma((2, 2, 4, 2)),
            dma((8, 2)), dma((4, 2)), dma((8, 2, 2)), dma((4, 2, 2)), dma((4, 3, 2)), dma((3, 2, 2)),
            dma((4, 5)), dma((4, 3)), dma((4, 2)),
        ],
        compiler_params=pltpu.CompilerParams(
            collective_id=0, has_side_effects=True, vmem_limit_bytes=55 << 20),
    )(stream, *weights, *vectors)


def body(
    nfs, ntp,
    stream, gain_first, gain_mixer, gain_second,
    gate_weight, gate_scale, up_weight, up_scale, down_weight, down_scale,
    pool_in_weight, pool_in_scale, pool_out_weight, pool_out_scale,
):
    half = jnp.bfloat16
    if fits(nfs, ntp, stream, gate_weight, pool_in_weight):
        return whole_layer(
            stream, (gate_weight, up_weight, down_weight, pool_in_weight, pool_out_weight),
            (pool_in_scale, pool_out_scale, down_scale, gain_first, gain_mixer, gain_second, gate_scale, up_scale))
    in_half, out_half = pool_in_weight.astype(half), pool_out_weight.astype(half)
    width, channels = stream.shape[1], in_half.shape[1]
    scales = jnp.concatenate([pool_in_scale, pool_out_scale]).reshape(1, -1)
    in_all, out_all, gate_all, up_all, down_all, stream_all, scales_all = gather_all(
        nfs, ntp, in_half, out_half, gate_weight.astype(half), up_weight.astype(half), down_weight.astype(half),
        stream, scales,
    )
    in_whole, out_whole = flat(in_all), flat(out_all)
    gate_whole, up_whole, down_whole = flat(gate_all), flat(up_all), flat(down_all)
    in_scale = scales_all[:, 0, :channels].reshape(-1)
    out_scale = scales_all[:, 0, channels:].reshape(-1)
    tp = lax.axis_index("tp")

    def feed_forward(rows):
        gate_sum = jnp.dot(rows, gate_whole, preferred_element_type=jnp.float32) * gate_scale
        up_sum = jnp.dot(rows, up_whole, preferred_element_type=jnp.float32) * up_scale
        hidden = (jax.nn.silu(gate_sum) * up_sum).astype(half)
        return jnp.dot(hidden, down_whole, preferred_element_type=jnp.float32).astype(half)

    first = rms(flat(stream_all).astype(jnp.float32), gain_first)
    after_first = summed(ntp, True, 1, feed_forward(first), stream, down_scale)
    mixer_normed = rms(after_first.astype(jnp.float32), gain_mixer)
    pool_input = (
        jnp.dot(mixer_normed, in_whole, preferred_element_type=jnp.float32) * in_scale
    ).astype(half)
    mixed = jnp.dot(pooling(pool_input), out_whole, preferred_element_type=jnp.float32)
    after_mix = (after_first.astype(jnp.float32) + mixed * out_scale).astype(half)
    second = rms(after_mix.astype(jnp.float32), gain_second)
    own = lax.dynamic_slice_in_dim(after_mix, tp * stream.shape[1], stream.shape[1], axis=1)
    return summed(ntp, False, 2, feed_forward(second), own, down_scale)


def solution(mesh):
    placed = (
        P("fs", "tp"), P(), P(), P(),
        P("fs", "tp"), P("tp"), P("fs", "tp"), P("tp"), P("tp", "fs"), P("tp"),
        P("fs", "tp"), P("tp"), P("tp", "fs"), P("tp"),
    )
    return jax.shard_map(
        functools.partial(body, mesh.shape["fs"], mesh.shape["tp"]),
        mesh=mesh, in_specs=placed, out_specs=P("fs", "tp"), check_vma=False,
    )
```

```python
import functools

import jax
import jax.numpy as jnp
from jax import lax
from jax.experimental import pallas as pl
from jax.experimental.pallas import tpu as pltpu
from jax.sharding import PartitionSpec as P

SEQ = 128
MESH = pl.DeviceIdType.MESH

eps = 1e-06
WINDOWS = (2, 4, 8, 16)
Z_FIRST = (3, 5, 7)


def fs_grid(count):
    ny = 1
    while (2 * ny) * (2 * ny) <= count and count % (2 * ny) == 0:
        ny *= 2
    return ny, count // ny


def grid_shape(row_blocks, col_blocks, block):
    rows, cols = block
    if cols % 128 == 0:
        return (row_blocks * rows, col_blocks * cols)
    return (row_blocks, col_blocks, rows, cols)


def place(whole, block, row_block, col_block, part=(0, None)):
    rows, cols = block
    first, count = part[0], rows if part[1] is None else part[1]
    if len(whole.shape) == 2:
        return whole.at[
            pl.ds(pl.multiple_of(row_block * rows + first, 16), count),
            pl.ds(pl.multiple_of(col_block * cols, 128), cols),
        ]
    return whole.at[row_block, col_block, pl.ds(first, count)]


def flat(whole):
    if whole.ndim == 2:
        return whole
    return whole.transpose(0, 2, 1, 3).reshape(whole.shape[0] * whole.shape[2], -1)


def gather_kernel(nfs, ntp, pool_in, pool_out, gate, up, down, stream, scales,
                  in_all, out_all, gate_all, up_all, down_all, stream_all, scales_all,
                  send_sem, recv_sem, local_sem, tsend, trecv, psend, precv, ssend, srecv):
    ny, nz = fs_grid(nfs)
    nx = ntp // 2
    fs, tp = lax.axis_index("fs"), lax.axis_index("tp")
    z, y = fs // ny, fs % ny
    x, core = tp // 2, tp % 2
    partner = x * 2 + (1 - core)
    alternate = ny == 2 and nz > 1

    barrier = pltpu.get_barrier_semaphore()

    def greet(cond, f, t):
        @pl.when(cond)
        def _():
            pl.semaphore_signal(barrier, inc=1, device_id={"fs": f, "tp": t}, device_id_type=MESH)

    greet(z > 0, fs - ny, tp)
    greet(z < nz - 1, fs + ny, tp)
    greet(y > 0, fs - 1, tp)
    greet(y < ny - 1, fs + 1, tp)
    for k in range(1, ntp):
        pl.semaphore_signal(
            barrier, inc=1, device_id={"fs": fs, "tp": (tp + k) % ntp}, device_id_type=MESH
        )
    peers = ntp - 1
    for cond in (z > 0, z < nz - 1, y > 0, y < ny - 1):
        peers = peers + jnp.where(cond, 1, 0)
    pl.semaphore_wait(barrier, peers)

    pieces = [
        (lambda: pool_in, lambda f: place(in_all, pool_in.shape, f, tp)),
        (lambda: pool_out, lambda f: place(out_all, pool_out.shape, tp, f)),
    ]
    npool = len(pieces)
    for own, whole, by_rows in ((gate, gate_all, True), (up, up_all, True), (down, down_all, False)):
        rows = own.shape[0]
        halves = 2 if alternate else 1
        for h in range(halves):
            part = (h * (rows // halves), rows // halves)

            def own_part(own=own, part=part):
                return own.at[pl.ds(*part)]

            def whole_part(f, own=own, whole=whole, part=part, by_rows=by_rows):
                return place(whole, own.shape, f if by_rows else 0, 0 if by_rows else f, part)

            pieces.append((own_part, whole_part))
    started = []

    def remote(piece, f, direction, target, mine=False):
        own, whole = pieces[piece]
        return pltpu.make_async_remote_copy(
            src_ref=own() if mine else whole(f),
            dst_ref=whole(f),
            send_sem=send_sem.at[piece, f, direction],
            recv_sem=recv_sem.at[piece, f],
            device_id={"fs": target, "tp": tp},
            device_id_type=MESH,
        )

    def send(cond, piece, f, direction, mine=False):
        target = fs + (-ny, ny, -1, 1)[direction]

        @pl.when(cond)
        def _():
            remote(piece, f, direction, target, mine).start()

        started.append((cond, piece, f, direction, target, mine))

    def arrived(cond, piece, f):
        @pl.when(cond)
        def _():
            remote(piece, f, 0, fs, False).wait_recv()

    def by_y(cond, piece, f, mine=False):
        send(cond & (y > 0), piece, f, 2, mine)
        send(cond & (y < ny - 1), piece, f, 3, mine)

    yes = z >= 0

    def stream_place(slot):
        return place(stream_all, stream.shape, 0, slot)

    def stream_copy(src, slot, t_target, k):
        return pltpu.make_async_remote_copy(
            src_ref=src, dst_ref=stream_place(slot), send_sem=tsend.at[k], recv_sem=trecv.at[slot],
            device_id={"fs": fs, "tp": t_target}, device_id_type=MESH)

    def slab(which, slot):
        if which == 0:
            if len(in_all.shape) == 2:
                cols = pool_in.shape[1]
                return in_all.at[:, pl.ds(pl.multiple_of(slot * cols, 128), cols)]
            return in_all.at[:, slot]
        if len(out_all.shape) == 2:
            rows = pool_out.shape[0]
            return out_all.at[pl.ds(pl.multiple_of(slot * rows, 16), rows)]
        return out_all.at[slot]

    def pool_copy(which, slot, t_target, k):
        return pltpu.make_async_remote_copy(
            src_ref=slab(which, slot), dst_ref=slab(which, slot),
            send_sem=psend.at[which, k], recv_sem=precv.at[which, slot],
            device_id={"fs": fs, "tp": t_target}, device_id_type=MESH)

    def scale_copy(k, slot, t_target):
        return pltpu.make_async_remote_copy(
            src_ref=scales, dst_ref=scales_all.at[slot], send_sem=ssend.at[k], recv_sem=srecv.at[slot],
            device_id={"fs": fs, "tp": t_target}, device_id_type=MESH)

    npieces = len(pieces)
    locals_ = [pltpu.make_async_copy(own(), whole(fs), local_sem.at[i]) for i, (own, whole) in enumerate(pieces)]
    locals_.append(pltpu.make_async_copy(stream, stream_place(tp), local_sem.at[npieces]))
    locals_.append(pltpu.make_async_copy(scales, scales_all.at[tp], local_sem.at[npieces + 1]))
    for piece in range(npieces):
        send(z > 0, piece, fs, 0, True)
        send(z < nz - 1, piece, fs, 1, True)
        by_y(yes, piece, fs, True)
    stream_sends = []
    for k in range(1, nx):
        stream_sends.append(stream_copy(stream, tp, (x + k) % nx * 2 + core, k - 1))
    stream_sends.append(stream_copy(stream, tp, partner, nx - 1))
    stream_sends += [scale_copy(k - 1, tp, (tp + k) % ntp) for k in range(1, ntp)]
    for copy in stream_sends:
        copy.start()
    for copy in locals_:
        copy.start()

    def row_arrivals(piece, d, alt):
        low, high = fs - d * ny, fs + d * ny
        has_low, has_high = z >= d, z + d <= nz - 1
        for cond, f, direction, ahead, end in (
            (has_low, low, 1, z < nz - 1, z == d),
            (has_high, high, 0, z > 0, z + d == nz - 1),
        ):
            arrived(cond, piece, f)
            send(cond & ahead, piece, f, direction)
            if alt:
                by_y(cond & jnp.logical_not(end), piece, f)
                other = f + 1 - 2 * y
                arrived(cond & end, piece, other)
                send(cond & end & ahead, piece, other, direction)
            else:
                by_y(cond, piece, f)

    def column_arrivals(piece, alt):
        for d in range(nz):
            for sign in ((1,) if d == 0 else (-1, 1)):
                row_ok = (z + sign * d >= 0) & (z + sign * d <= nz - 1)
                if alt:
                    at = z + sign * d
                    if d == 0:
                        continue
                    row_ok = row_ok & (at != 0) & (at != nz - 1)
                base = fs + sign * d * ny
                for e in range(1, ny):
                    for step, direction, ok, ahead in (
                        (-e, 3, y >= e, y < ny - 1),
                        (e, 2, y + e <= ny - 1, y > 0),
                    ):
                        arrived(row_ok & ok, piece, base + step)
                        if ny > 2:
                            send(row_ok & ok & ahead, piece, base + step, direction)

    is_alt = [alternate and p >= npool and p % 2 == 1 for p in range(npieces)]

    for d in range(1, nz):
        for p in range(npool):
            row_arrivals(p, d, False)
    pool_sends = []
    for p in range(npool):
        column_arrivals(p, False)
        locals_[p].wait()
        pool_sends += [pool_copy(p, tp, (x + k) % nx * 2 + core, k - 1) for k in range(1, nx)]
        pool_sends.append(pool_copy(p, tp, partner, nx - 1))
    for copy in pool_sends:
        copy.start()
    for k in range(1, nx):
        slot = (x + k) % nx * 2 + core
        stream_copy(stream, slot, partner, 0).wait_recv()
        copy = stream_copy(stream_place(slot), slot, partner, nx - 1 + k)
        copy.start()
        stream_sends.append(copy)

    for p in range(npieces):
        if is_alt[p]:
            other = fs + 1 - 2 * y
            arrived(yes, p, other)
            send(z == 0, p, other, 1)
            send(z == nz - 1, p, other, 0)
    for d in range(1, nz):
        for p in range(npool, npieces):
            row_arrivals(p, d, is_alt[p])
        if d == 1:
            for k in range(1, nx):
                slot = (x + k) % nx * 2 + core
                for p in range(npool):
                    pool_copy(p, slot, partner, 0).wait_recv()
                    copy = pool_copy(p, slot, partner, nx - 1 + k)
                    copy.start()
                    pool_sends.append(copy)
    for p in range(npool, npieces):
        column_arrivals(p, is_alt[p])
    for k in range(nx):
        slot = (x + k) % nx * 2 + (1 - core)
        stream_copy(stream, slot, partner, 0).wait_recv()
        for p in range(npool):
            pool_copy(p, slot, partner, 0).wait_recv()
    for k in range(1, ntp):
        scale_copy(0, (tp + k) % ntp, partner).wait_recv()
    for copy in locals_[npool:]:
        copy.wait()
    for copy in stream_sends + pool_sends:
        copy.wait_send()
    for cond, piece, f, direction, target, mine in started:
        @pl.when(cond)
        def _():
            remote(piece, f, direction, target, mine).wait_send()


def gather_all(nfs, ntp, pool_in, pool_out, gate, up, down, stream, scales):
    ny, nz = fs_grid(nfs)
    nx = ntp // 2
    npieces = 8 if (ny == 2 and nz > 1) else 5
    any_spec = pl.BlockSpec(memory_space=pl.ANY)
    shapes = (
        grid_shape(nfs, ntp, pool_in.shape),
        grid_shape(ntp, nfs, pool_out.shape),
        grid_shape(nfs, 1, gate.shape),
        grid_shape(nfs, 1, up.shape),
        grid_shape(1, nfs, down.shape),
        grid_shape(1, ntp, stream.shape),
    )
    dma = pltpu.SemaphoreType.DMA
    return pl.pallas_call(
        functools.partial(gather_kernel, nfs, ntp),
        name="collect_weights",
        out_shape=tuple(jax.ShapeDtypeStruct(shape, jnp.bfloat16) for shape in shapes)
        + (jax.ShapeDtypeStruct((ntp,) + scales.shape, jnp.float32),),
        in_specs=[any_spec] * 7,
        out_specs=[any_spec] * 7,
        scratch_shapes=[
            dma((npieces, nfs, 4)),
            dma((npieces, nfs)),
            dma((npieces + 2,)),
            dma((2 * nx,)),
            dma((ntp,)),
            dma((2, 2 * nx)),
            dma((2, ntp)),
            dma((ntp,)),
            dma((ntp,)),
        ],
        compiler_params=pltpu.CompilerParams(collective_id=0, has_side_effects=True, vmem_limit_bytes=1 << 20),
    )(pool_in, pool_out, gate, up, down, stream, scales)


def sum_kernel(ntp, gathers, pieces, partial, resid, scale, out, pair, pair_sum, cross, *sems):
    pair_send, pair_recv, cross_send, cross_recv = sems[:4]
    nx = ntp // 2
    tp, fs = lax.axis_index("tp"), lax.axis_index("fs")
    x, core = tp // 2, tp % 2
    partner = x * 2 + (1 - core)
    rows, width = resid.shape
    step = rows // pieces
    barrier = pltpu.get_barrier_semaphore()
    pl.semaphore_signal(barrier, inc=1, device_id={"fs": fs, "tp": partner}, device_id_type=MESH)
    for k in range(1, nx):
        pl.semaphore_signal(
            barrier, inc=1, device_id={"fs": fs, "tp": (x + k) % nx * 2 + core}, device_id_type=MESH
        )
    pl.semaphore_wait(barrier, nx)

    def remote(src, dst, send, recv, target):
        return pltpu.make_async_remote_copy(
            src_ref=src, dst_ref=dst, send_sem=send, recv_sem=recv,
            device_id={"fs": fs, "tp": target}, device_id_type=MESH)

    def columns(t):
        return pl.ds(pl.multiple_of(t * width, width), width)

    parts = [pl.ds(i * step, step) for i in range(pieces)]
    offsets = list(range(1, nx)) + [0]
    sends = []
    for k in offsets:
        for i, part in enumerate(parts):
            copy = remote(partial.at[part, columns((x + k) % nx * 2 + (1 - core))], pair.at[k, part],
                          pair_send.at[k, i], pair_recv.at[k, i], partner)
            copy.start()
            sends.append(copy)
    for k in offsets[:-1]:
        target = (x + k) % nx * 2 + core
        for i, part in enumerate(parts):
            remote(pair.at[k, part], pair.at[k, part], pair_send.at[k, i], pair_recv.at[k, i], partner).wait_recv()
            pair_sum[k - 1, part] = (
                partial[part, columns(target)].astype(jnp.float32) + pair[k, part].astype(jnp.float32)
            ).astype(jnp.bfloat16)
            copy = remote(pair_sum.at[k - 1, part], cross.at[k - 1, part],
                          cross_send.at[k - 1, i], cross_recv.at[k - 1, i], target)
            copy.start()
            sends.append(copy)
    factor = 0.5 * scale[...]
    for i, part in enumerate(parts):
        remote(pair.at[0, part], pair.at[0, part], pair_send.at[0, i], pair_recv.at[0, i], partner).wait_recv()
        total = partial[part, columns(tp)].astype(jnp.float32) + pair[0, part].astype(jnp.float32)
        for k in range(1, nx):
            remote(cross.at[k - 1, part], cross.at[k - 1, part], cross_send.at[k - 1, i],
                   cross_recv.at[k - 1, i], partner).wait_recv()
            total = total + cross[k - 1, part].astype(jnp.float32)
        result = (resid[part].astype(jnp.float32) + total * factor).astype(jnp.bfloat16)
        if not gathers:
            out[part] = result
            continue
        out[part, columns(tp)] = result
        gather_send, gather_recv = sems[4:]
        for k in range(1, nx):
            copy = remote(out.at[part, columns(tp)], out.at[part, columns(tp)], gather_send.at[k - 1, i], gather_recv.at[tp, i],
                          (x + k) % nx * 2 + core)
            copy.start()
            sends.append(copy)
        copy = remote(out.at[part, columns(tp)], out.at[part, columns(tp)], gather_send.at[nx - 1, i], gather_recv.at[tp, i], partner)
        copy.start()
        sends.append(copy)
    if gathers:
        for k in range(1, nx):
            slot = (x + k) % nx * 2 + core
            for i, part in enumerate(parts):
                remote(out.at[part, columns(slot)], out.at[part, columns(slot)], gather_send.at[0, i], gather_recv.at[slot, i],
                       partner).wait_recv()
                copy = remote(out.at[part, columns(slot)], out.at[part, columns(slot)], gather_send.at[nx - 1 + k, i],
                              gather_recv.at[slot, i], partner)
                copy.start()
                sends.append(copy)
        for k in range(nx):
            slot = (x + k) % nx * 2 + (1 - core)
            for i, part in enumerate(parts):
                remote(out.at[part, columns(slot)], out.at[part, columns(slot)], gather_send.at[0, i], gather_recv.at[slot, i],
                       partner).wait_recv()
    for copy in sends:
        copy.wait_send()


def summed(ntp, gathers, identity, partial, resid, scale):
    nx = ntp // 2
    rows, width = resid.shape
    pieces = 3 if rows % 48 == 0 else 1
    vmem = pl.BlockSpec(memory_space=pltpu.VMEM)
    dma = pltpu.SemaphoreType.DMA
    scratch = [
        pltpu.VMEM((nx, rows, width), jnp.bfloat16),
        pltpu.VMEM((max(nx - 1, 1), rows, width), jnp.bfloat16),
        pltpu.VMEM((max(nx - 1, 1), rows, width), jnp.bfloat16),
        dma((nx, pieces)), dma((nx, pieces)), dma((nx, pieces)), dma((nx, pieces)),
    ]
    if gathers:
        scratch += [dma((2 * nx, pieces)), dma((ntp, pieces))]
    return pl.pallas_call(
        functools.partial(sum_kernel, ntp, gathers, pieces),
        name="sum_and_share" if gathers else "sum_last",
        out_shape=jax.ShapeDtypeStruct((rows, width * (ntp if gathers else 1)), jnp.bfloat16),
        in_specs=[vmem] * 3,
        out_specs=vmem,
        scratch_shapes=scratch,
        compiler_params=pltpu.CompilerParams(
            collective_id=identity, has_side_effects=True, vmem_limit_bytes=32 << 20
        ),
    )(partial, resid, scale.reshape(1, width))


def rms(floats, norm_gain):
    scaled = floats * lax.rsqrt(jnp.mean(floats * floats, axis=-1, keepdims=True) + eps)
    return (scaled * norm_gain).astype(jnp.bfloat16)


def window_weights():
    position = jnp.arange(SEQ)
    rows, cols = position[:, None], position[None, :]
    mats = []
    for window in WINDOWS:
        low = jnp.maximum(rows - window // 2, 0)
        high = jnp.minimum(rows + window - window // 2, SEQ)
        mats.append(((cols >= low) & (cols < high)).astype(jnp.bfloat16))
    return mats


def pooling(pool_input):
    channels = pool_input.shape[1]
    group = channels // 4
    values = pool_input.reshape(-1, SEQ, channels)
    position = jnp.arange(SEQ)
    parts = []
    for index, (window, members) in enumerate(zip(WINDOWS, window_weights())):
        own = values[:, :, index * group:(index + 1) * group]
        sums = jnp.einsum("pq,sqc->spc", members, own, preferred_element_type=jnp.float32)
        before = window // 2
        counts = (
            jnp.minimum(position + window - before, SEQ) - jnp.maximum(position - before, 0)
        ).astype(jnp.float32)
        parts.append(sums / counts[None, :, None] - own.astype(jnp.float32))
    return jnp.concatenate(parts, axis=2).reshape(-1, channels).astype(jnp.bfloat16)


def layer_kernel(
    sizes, stream, gate_in, up_in, down_in, in_in, out_in, *refs):
    parts, (out, vectors, *rest) = refs[:8], refs[8:]
    layer_steps(sizes, stream, gate_in, up_in, down_in, in_in, out_in, parts, out, vectors, *rest)


def layer_steps(
    sizes, stream, gate_in, up_in, down_in, in_in, out_in, parts, out, vectors,
    gate, up, down, pool_in, pool_out, gate_wide, up_wide, down_wide, in_wide, out_wide,
    gate_all, up_all, down_all, in_all, out_all, scales_all, rows_all, first_all, mixed_all, normed,
    gate_sum, up_sum, hidden, pooled, partial, pair, shares, first_in,
    load_sem, vector_sem, local_sem, z_send, y_send, w_recv, pl_zsend, pl_ysend, pl_recv, slab_send, slab_recv,
    sc_send, sc_recv, ag_send, ag_recv, pair_send, pair_recv, two_send, two_recv, rs_send, rs_recv,
    fr_send, fr_recv, fr_core,
):
    rows, small, extra = sizes
    big = small + extra
    block = gate.shape[0]
    width = stream.shape[1]
    chans = pool_in.shape[1]
    units = gate.shape[1]
    features = gate_all.shape[0]
    starts = [0]
    for count in (chans, width, width, features, features, features, units, units):
        starts.append(starts[-1] + count)
    scales = vectors.at[:, :chans + 2 * width]

    def vector(at, first, count):
        return vectors[:, pl.ds(pl.multiple_of(starts[at] + first, 128), count)]

    every = 2 * rows
    f32, half = jnp.float32, jnp.bfloat16
    fs, tp = lax.axis_index("fs"), lax.axis_index("tp")
    z, y = fs // 2, fs % 2
    x, core = tp // 2, tp % 2
    low, pair_hi = z % 2, z // 2
    zp = z + 1 - 2 * low
    zs = [z, zp, 2 - pair_hi, 3 - 3 * pair_hi]
    fs_y, fs_z = fs + 1 - 2 * y, 2 * zp + y
    tp_c, tp_x = tp + 1 - 2 * core, (tp + 2) % 4
    tp_xc = tp_x + 1 - 2 * core

    def upper(at):
        return (((at + 1) // 2) % 2 + core) % 2

    own_rows = pl.ds(pl.multiple_of(low * rows, 16), rows)
    stream_own = pltpu.make_async_copy(
        stream, rows_all.at[own_rows, pl.ds(pl.multiple_of(tp * width, 128), width)], local_sem.at[0])
    stream_own.start()
    vector_copies = [
        pltpu.make_async_copy(ref, vectors.at[0, pl.ds(first, ref.shape[0])], vector_sem.at[i])
        for i, (ref, first) in enumerate(zip(parts, starts))]
    for copy in vector_copies:
        copy.start()
    loads = []
    for i, (wide, ref, narrow) in enumerate((
        (in_wide, in_in, pool_in), (out_wide, out_in, pool_out), (gate_wide, gate_in, gate),
        (up_wide, up_in, up), (down_wide, down_in, down),
    )):
        copy = pltpu.make_async_copy(ref, wide, load_sem.at[i])
        copy.start()
        loads.append((copy, wide, narrow))

    barrier = pltpu.get_barrier_semaphore()
    peers = [(2 * at + y, tp) for at in zs[1:]] + [
        (fs_y, tp), (fs, tp_c), (fs, tp_x), (fs, tp_xc), (fs_z, tp_x)]
    for f, t in peers:
        pl.semaphore_signal(barrier, inc=1, device_id={"fs": f, "tp": t}, device_id_type=MESH)

    def narrowed(copy, wide, narrow):
        copy.wait()
        count = wide.shape[0]
        each = 64 if count % 64 == 0 else 16

        def one(i, carry):
            part = pl.ds(pl.multiple_of(i * each, each), each)
            narrow[part, :] = wide[part, :].astype(half)
            return carry
        lax.fori_loop(0, count // each, one, 0)

    for load in loads[:3]:
        narrowed(*load)
    stream_own.wait()
    for copy in vector_copies:
        copy.wait()
    pl.semaphore_wait(barrier, len(peers))

    ends = []

    def remote(src, dst, send, recv, f, t):
        return pltpu.make_async_remote_copy(
            src_ref=src, dst_ref=dst, send_sem=send, recv_sem=recv,
            device_id={"fs": f, "tp": t}, device_id_type=MESH)

    def start(make, cond=None):
        if cond is None:
            make().start()
        else:
            pl.when(cond)(lambda: make().start())
        ends.append((make, cond))

    def flush(count=None):
        for make, cond in ends[:count]:
            if cond is None:
                make().wait_send()
            else:
                pl.when(cond)(lambda make=make: make().wait_send())
        del ends[:count]

    def arrive(dst, recv, cond=None):
        def wait():
            remote(dst, dst, recv, recv, fs, tp_c).wait_recv()
        if cond is None:
            wait()
        else:
            pl.when(cond)(wait)

    def lanes(at, count):
        return pl.ds(pl.multiple_of(at, 128), count)

    def subs(at, count):
        return pl.ds(pl.multiple_of(at, 16), count)

    pieces = width // block

    def column_block(j, xx, cc):
        return (2 * xx + cc) * pieces + j

    def share_place(phase, ref, chip_low, j, xx, cc):
        return ref.at[subs(chip_low * rows, rows), lanes(column_block(j, xx, cc) * block, block)]

    def share_start(phase, ref, j, cond=None):
        here = share_place(phase, ref, low, j, x, core)
        for k, (f, t) in enumerate(((fs_z, tp), (fs, tp_x), (fs, tp_c))):
            start(lambda f=f, t=t, k=k: remote(
                here, here, ag_send.at[phase, j, k], ag_recv.at[phase, j, 2 * x + low, core], f, t), cond)

    def share_relay(phase, ref, j, k, chip_low, xx, targets, cond=None):
        here = share_place(phase, ref, chip_low, j, xx, core)
        flag = ag_recv.at[phase, j, 2 * xx + chip_low, core]
        arrive(here, flag, cond)
        for n, target in enumerate(targets):
            start(lambda n=n, target=target: remote(
                here, here, ag_send.at[phase, j, 3 + k + n], flag, fs, target), cond)

    def relay_own(phase, ref, j, cond=None):
        share_relay(phase, ref, j, 0, 1 - low, x, (tp_x, tp_c), cond)

    def relay_across(phase, ref, j, cond=None):
        share_relay(phase, ref, j, 2, low, 1 - x, (tp_c,), cond)
        share_relay(phase, ref, j, 3, 1 - low, 1 - x, (tp_c,), cond)

    def share_finish(phase, ref):
        for j in range(2):
            for xx in (x, 1 - x):
                for cl in (low, 1 - low):
                    arrive(share_place(phase, ref, cl, j, xx, 1 - core), ag_recv.at[phase, j, 2 * xx + cl, 1 - core])

    for j in range(2):
        share_start(0, rows_all, j)

    def scale_copy(k, slot, t):
        return remote(scales, scales_all.at[slot], sc_send.at[k], sc_recv.at[slot], fs, t)

    for k, t in enumerate((tp_c, tp_x, tp_xc)):
        start(lambda k=k, t=t: scale_copy(k, tp, t))
    locals_ = [pltpu.make_async_copy(scales, scales_all.at[tp], local_sem.at[1])]

    def pool_place(which, f, t):
        if which == 0:
            return in_all.at[subs(f * block, block), lanes(t * chans, chans)]
        return out_all.at[subs(t * chans, chans), lanes(f * block, block)]

    def pool_slab(which, t):
        if which == 0:
            return in_all.at[:, lanes(t * chans, chans)]
        return out_all.at[subs(t * chans, chans)]

    def pool_start():
        for which, own in enumerate((pool_in, pool_out)):
            for k in range(1, 4):
                start(lambda k=k, which=which, own=own: remote(
                    own, pool_place(which, fs, tp), pl_zsend.at[which, k], pl_recv.at[which, fs], 2 * zs[k] + y, tp))
            start(lambda which=which, own=own: remote(
                own, pool_place(which, fs, tp), pl_ysend.at[which, 0], pl_recv.at[which, fs], fs_y, tp))

    for which, own in enumerate((pool_in, pool_out)):
        locals_.append(pltpu.make_async_copy(own, pool_place(which, fs, tp), local_sem.at[2 + which]))

    PARTS = 3

    def own_part(piece, part, side):
        first = 2 * small if part == 2 else side * small
        if piece == 2:
            return down.at[subs(first + part % 2 * (small // 2), extra if part == 2 else small // 2)]
        ref = (gate, up)[piece]
        if part == 2:
            return ref.at[:, lanes(first, extra)]
        return ref.at[pl.ds(part * (block // 2), block // 2), lanes(first, small)]

    def all_part(piece, part, f):
        if piece == 2:
            at, count = (small, extra) if part == 2 else (part * (small // 2), small // 2)
            return down_all.at[pl.ds(at, count), lanes(f * block, block)]
        ref = (gate_all, up_all)[piece]
        if part == 2:
            return ref.at[subs(f * block, block), pl.ds(small, extra)]
        return ref.at[subs(f * block + part * (block // 2), block // 2), pl.ds(0, small)]

    def part_cond(part, wide, cond=None):
        if part < 2:
            return cond
        return wide == 1 if cond is None else cond & (wide == 1)

    def y_own(piece):
        for part in range(PARTS):
            start(lambda part=part: remote(
                own_part(piece, part, upper(z)), all_part(piece, part, fs), y_send.at[0, piece, part],
                w_recv.at[fs, piece, part], fs_y, tp), part_cond(part, upper(z)))

    def own_copy(piece, part):
        return pltpu.make_async_copy(
            own_part(piece, part, upper(z)), all_part(piece, part, fs), local_sem.at[4 + PARTS * piece + part])

    for copy in locals_:
        copy.start()
    inner = (z == 1) | (z == 2)

    def z_own(piece, cond=None, targets=(1, 2, 3)):
        for k in targets:
            at = zs[k]
            for part in range(PARTS):
                ok = part_cond(part, upper(at), cond)
                start(lambda k=k, at=at, part=part: remote(
                    own_part(piece, part, upper(at)), all_part(piece, part, fs), z_send.at[k, piece, part],
                    w_recv.at[fs, piece, part], 2 * at + y, tp), ok)

    outer = jnp.logical_not(inner)
    z_own(0, None, (1,))
    y_own(0)
    for load in loads[3:]:
        narrowed(*load)
    z_own(1, outer, (1,))
    z_own(0, None, (2, 3))
    pool_start()
    z_own(1, inner, (1,))
    z_own(1, None, (2, 3))
    y_own(1)
    y_own(2)
    z_own(2, None, (1,))
    for piece in range(3):
        own_copy(piece, 0).start()
        own_copy(piece, 1).start()
        pl.when(upper(z) == 1)(lambda piece=piece: own_copy(piece, 2).start())

    @pl.when(upper(z) == 0)
    def _():
        gate_all[:, small:big] = jnp.zeros((features, extra), half)
        up_all[:, small:big] = jnp.zeros((features, extra), half)
        down_all[small:big, :] = jnp.zeros((extra, features), half)

    def weights_here(piece, f):
        for part in range(PARTS):
            arrive(all_part(piece, part, f), w_recv.at[f, piece, part], part_cond(part, upper(z)))

    def by_z(piece, i):
        f = 2 * zs[i] + y
        for part in range(PARTS):
            cond = part_cond(part, upper(z))
            arrive(all_part(piece, part, f), w_recv.at[f, piece, part], cond)
            start(lambda part=part: remote(
                all_part(piece, part, f), all_part(piece, part, f), y_send.at[i, piece, part],
                w_recv.at[f, piece, part], fs_y, tp), cond)

    def own_here(piece):
        own_copy(piece, 0).wait()
        own_copy(piece, 1).wait()
        pl.when(upper(z) == 1)(lambda: own_copy(piece, 2).wait())

    step = 32
    lane_tiles = features // 128

    def norm_rows(source, gain_at, base=0):
        def one(i, carry):
            part = pl.ds(pl.multiple_of(base + i * 128, 128), 128)
            total = jnp.zeros((128, 128), f32)
            for c in range(lane_tiles):
                floats = source[part, c * 128:(c + 1) * 128].astype(f32)
                total = total + floats * floats
            scale = lax.rsqrt(jnp.sum(total, axis=-1, keepdims=True) * (1.0 / features) + eps)
            for c in range(lane_tiles):
                floats = source[part, c * 128:(c + 1) * 128].astype(f32)
                normed[part, c * 128:(c + 1) * 128] = ((floats * scale) * vector(gain_at, c * 128, 128)).astype(half)
            return carry
        return one

    for j in range(2):
        relay_own(0, rows_all, j)
    for j in range(2):
        relay_across(0, rows_all, j)
    share_finish(0, rows_all)
    lax.fori_loop(0, every // 128, norm_rows(rows_all, 3), 0)

    def pool_by_y():
        for k in range(1, 4):
            for which in range(2):
                f = 2 * zs[k] + y
                here = pool_place(which, f, tp)
                arrive(here, pl_recv.at[which, f])
                start(lambda k=k, which=which, here=here, f=f: remote(
                    here, here, pl_ysend.at[which, k], pl_recv.at[which, f], fs_y, tp))

    tile = 256

    def accumulate(weights, total, f, first):
        for n in range(big // 128 // 2 + 1):
            cols = slice(n * tile, min((n + 1) * tile, big))
            if cols.start < cols.stop:
                product = jnp.dot(normed[:, lanes(f * block, block)], weights[subs(f * block, block), cols],
                                  preferred_element_type=f32)
                total[:, cols] = product if first else total[:, cols] + product

    def pool_across():
        for which in range(2):
            locals_[1 + which].wait()
            for k in range(4):
                f = fs_y if k == 0 else 2 * zs[k] + 1 - y
                arrive(pool_place(which, f, tp), pl_recv.at[which, f])
            slab = pool_slab(which, tp)
            for n, t in enumerate((tp_x, tp_c)):
                start(lambda which=which, slab=slab, n=n, t=t: remote(
                    slab, slab, slab_send.at[which, n], slab_recv.at[which, tp], fs, t))

    early_sends = len(ends)
    ahead = [(piece, i) for piece in range(3) for i in range(1, 4)]
    for piece, (weights, total) in enumerate(((gate_all, gate_sum), (up_all, up_sum))):
        for i in range(4):
            f, g = 2 * zs[i] + y, 2 * zs[i] + 1 - y
            if i == 0:
                own_here(piece)
            accumulate(weights, total, f, i == 0)
            if 4 * piece + i < 7:
                by_z(*ahead[4 * piece + i])
            weights_here(piece, g)
            accumulate(weights, total, g, False)
            if (piece, i) == (0, 2):
                pool_by_y()
            if (piece, i) == (1, 0):
                z_own(2, inner, (2, 3))
                pool_across()
            if (piece, i) == (1, 1):
                z_own(2, outer, (2, 3))
    own_here(2)

    def hide(i, carry):
        part = pl.ds(pl.multiple_of(i * step, step), step)
        a = gate_sum[part, :] * vector(6, upper(z) * small, big)
        hidden[part, :] = (a / (1.0 + jnp.exp(-a)) * (up_sum[part, :] * vector(7, upper(z) * small, big))).astype(half)
        return carry

    lax.fori_loop(0, every // step, hide, 0)

    def block_send(f, r):
        zz = f // 2
        slot = 2 * (zz // 2) + f % 2
        part = subs(r * rows, rows)
        start(lambda: remote(
            partial.at[f, part], pair.at[0, slot, part], pair_send.at[f, r],
            pair_recv.at[slot, r], fs, tp_c), zz % 2 != core)

    def core_sum(f, r):
        slot = 2 * (f // 4) + f % 2

        @pl.when((f // 2) % 2 == core)
        def _():
            here = pair.at[0, slot, subs(r * rows, rows)]
            remote(here, here, pair_send.at[f, r], pair_recv.at[slot, r], fs, tp_c).wait_recv()

            def one(i, carry):
                at = pl.ds(pl.multiple_of(r * rows + i * 128, 128), 128)
                partial[f, at, :] = (
                    partial[f, at, :].astype(f32) + pair[0, slot, at, :].astype(f32)).astype(half)
                return carry
            lax.fori_loop(0, rows // 128, one, 0)

    pair_z = (jnp.where(low == core, zp, z), jnp.where(low == core, z, zp), zs[2], zs[3])
    blocks = [2 * zz + j for zz in pair_z for j in (y, 1 - y)]

    def ways(n):
        across_x, across_z = (fs, tp_x), (fs_z, tp)
        return (across_z, across_x, low) if n in Z_FIRST else (across_x, across_z, x)

    def first_send(n, k, src, dst, recv, to):
        f = blocks[n]
        start(lambda: remote(src, dst, fr_send.at[2 * (f // 4) + f % 2, k], recv, *to), (f // 2) % 2 == core)

    def first_sum(n):
        f = blocks[n]
        slot = 2 * (f // 4) + f % 2
        to, _, r = ways(n)
        core_sum(f, 1 - r)
        first_send(n, 0, partial.at[f, subs((1 - r) * rows, rows)], first_in.at[0, slot], fr_recv.at[slot, 0], to)
        core_sum(f, r)

    def first_add(n):
        f = blocks[n]
        slot = 2 * (f // 4) + f % 2
        _, to, r = ways(n)
        part = subs(r * rows, rows)

        @pl.when((f // 2) % 2 == core)
        def _():
            arrive(first_in.at[0, slot], fr_recv.at[slot, 0])

            def one(i, carry):
                at = pl.ds(pl.multiple_of(r * rows + i * 128, 128), 128)
                got = first_in[0, slot, pl.ds(pl.multiple_of(i * 128, 128), 128), :].astype(f32)
                partial[f, at, :] = (partial[f, at, :].astype(f32) + got).astype(half)
                return carry
            lax.fori_loop(0, rows // 128, one, 0)
        first_send(n, 1, partial.at[f, part], first_in.at[1, slot], fr_recv.at[slot, 1], to)

    def first_done(n):
        f = blocks[n]
        slot = 2 * (f // 4) + f % 2
        to, _, r = ways(n)
        cols = lanes(f * block, block)

        @pl.when((f // 2) % 2 == core)
        def _():
            arrive(first_in.at[1, slot], fr_recv.at[slot, 1])
            factor = 0.5 * scales_all[f // 2, :, pl.ds(pl.multiple_of(chans + width + (f % 2) * block, 128), block)]

            def one(i, carry):
                at = pl.ds(pl.multiple_of(r * rows + i * 128, 128), 128)
                total = partial[f, at, :].astype(f32) + first_in[
                    1, slot, pl.ds(pl.multiple_of(i * 128, 128), 128), :].astype(f32)
                first_all[at, cols] = (rows_all[at, cols].astype(f32) + total * factor).astype(half)
                return carry
            lax.fori_loop(0, rows // 128, one, 0)
        here = first_all.at[subs(r * rows, rows), cols]
        first_send(n, 2, here, here, fr_recv.at[slot, 2], to)
        first_send(n, 3, here, here, fr_core.at[slot, r], (fs, tp_c))

    def first_pass(n):
        f = blocks[n]
        slot = 2 * (f // 4) + f % 2
        r = 1 - ways(n)[2]
        here = first_all.at[subs(r * rows, rows), lanes(f * block, block)]
        arrive(here, fr_recv.at[slot, 2], (f // 2) % 2 == core)
        first_send(n, 4, here, here, fr_core.at[slot, r], (fs, tp_c))

    def first_finish():
        for f in blocks:
            slot = 2 * (f // 4) + f % 2
            for r in range(2):
                arrive(first_all.at[r * rows:(r + 1) * rows, lanes(f * block, block)], fr_core.at[slot, r],
                       (f // 2) % 2 != core)

    def part_send(f, h, c, base, count):
        slot = 2 * (f // 4) + f % 2
        part = subs(base, count)
        start(lambda: remote(
            partial.at[f, part], pair.at[1, slot, part], two_send.at[f, h, c], two_recv.at[slot, h, c], fs, tp_c),
            (f // 2) % 2 != core)

    def part_sum(f, h, c, base, first, count):
        slot = 2 * (f // 4) + f % 2
        part = subs(base, count)

        @pl.when((f // 2) % 2 == core)
        def _():
            arrive(pair.at[1, slot, part], two_recv.at[slot, h, c])

            def one(i, carry):
                at = pl.ds(pl.multiple_of(base + i * 128, 128), 128)
                partial[f, at, :] = (partial[f, at, :].astype(f32) + pair[1, slot, at, :].astype(f32)).astype(half)
                return carry
            lax.fori_loop(0, count // 128, one, 0)
        mine = f // 4 == x
        away = jnp.logical_not(mine)
        ways = ((1, fs_z, tp, mine), (2, fs_z, tp_x, away)) if h == 0 else ((0, fs, tp_x, away),)
        for k, fd, td, cond in ways:
            start(lambda k=k, fd=fd, td=td: remote(
                partial.at[f, part], shares.at[k, f % 2, pl.ds(first, count)], rs_send.at[slot, k, c],
                rs_recv.at[k, f % 2, c], fd, td), ((f // 2) % 2 == core) & cond)

    cuts = (((0, SEQ), (SEQ, rows - SEQ)), ((0, rows - SEQ), (rows - SEQ, SEQ)))

    def slab_across():
        for which in range(2):
            slab = pool_slab(which, tp_x)
            arrive(slab, slab_recv.at[which, tp_x])
            start(lambda which=which, slab=slab: remote(
                slab, slab, slab_send.at[which, 2], slab_recv.at[which, tp_x], fs, tp_c))

    locals_[0].wait()
    for t in (tp_c, tp_x, tp_xc):
        arrive(scales_all.at[t], sc_recv.at[t])
    def product_of(n):
        f = blocks[n]
        if n % 2:
            weights_here(2, f)
        partial[f, :, :] = jnp.dot(
            hidden[...], down_all[:, lanes(f * block, block)], preferred_element_type=f32).astype(half)
        for r in (1 - ways(n)[2], ways(n)[2]):
            block_send(f, r)

    def down_from(n):
        by_z(2, n)

    def slab(n):
        slab_across()
        flush(early_sends)

    for stage, members in (
        (product_of, (0, 1, 2, 3)), (first_sum, (2, 3)), (slab, (0,)), (first_add, (2, 3)), (down_from, (2,)),
        (product_of, (4,)), (down_from, (3,)), (product_of, (6,)), (first_sum, (4, 6)), (first_done, (2, 3)),
        (first_add, (4, 6)), (product_of, (5,)), (first_sum, (5,)), (first_pass, (2, 3)), (first_done, (4, 6)),
        (product_of, (7,)), (first_sum, (7,)), (first_add, (5,)), (first_pass, (4, 6)), (first_done, (5,)),
        (first_add, (7,)), (first_pass, (5,)), (first_done, (7,)), (first_pass, (7,)),
    ):
        for m in members:
            stage(m)
    for which in range(2):
        for t in (tp_c, tp_xc):
            arrive(pool_slab(which, t), slab_recv.at[which, t])
    flush()
    first_finish()

    in_scale = jnp.concatenate([scales_all[t, :, :chans] for t in range(4)], axis=1)
    group = 4 * chans // 4
    pos_row = lax.broadcasted_iota(jnp.int32, (SEQ, SEQ), 0)
    pos_col = lax.broadcasted_iota(jnp.int32, (SEQ, SEQ), 1)
    pos = lax.broadcasted_iota(jnp.int32, (SEQ, 1), 0)

    def row_scale(total):
        return lax.rsqrt(jnp.sum(total, axis=-1, keepdims=True) * (1.0 / features) + eps)

    def gained_rows(base, count):
        scale = []
        for i in range(count // 128):
            part = pl.ds(pl.multiple_of(base + i * 128, 128), 128)
            total = jnp.zeros((128, 128), f32)
            for c in range(lane_tiles):
                cols = slice(c * 128, (c + 1) * 128)
                floats = first_all[part, cols].astype(f32)
                total = total + floats * floats
                normed[part, cols] = (floats * vector(4, c * 128, 128)).astype(half)
            scale.append(row_scale(total))
        return jnp.concatenate(scale, axis=0)

    def mix(base, count):
        scale = gained_rows(base, count)
        part = pl.ds(pl.multiple_of(base, 128), count)
        pool_input = (
            jnp.dot(normed[part, :], in_all[...], preferred_element_type=f32) * scale * in_scale).astype(half)
        for index, window in enumerate(WINDOWS):
            before = window // 2
            first = jnp.maximum(pos_row - before, 0)
            last = jnp.minimum(pos_row + window - before, SEQ)
            members = jnp.where((pos_col >= first) & (pos_col < last), 1.0, 0.0).astype(half)
            counts = (jnp.minimum(pos + window - before, SEQ) - jnp.maximum(pos - before, 0)).astype(f32)
            for s in range(count // SEQ):
                own = pool_input[s * SEQ:(s + 1) * SEQ, index * group:(index + 1) * group]
                sums = jnp.dot(members, own, preferred_element_type=f32)
                pooled[s * SEQ:(s + 1) * SEQ, index * group:(index + 1) * group] = (
                    sums / counts - own.astype(f32)).astype(half)
        total = jnp.zeros((count, 128), f32)
        for t in range(4):
            cols = slice(t * width, (t + 1) * width)
            mixed = jnp.dot(pooled[:count, :], out_all[:, cols], preferred_element_type=f32)
            value = (first_all[part, cols].astype(f32) + mixed * scales_all[t, :, chans:chans + width]).astype(half)
            mixed_all[part, cols] = value
            value = value.astype(f32)
            normed[part, cols] = (value * vector(5, t * width, width)).astype(half)
            for c in range(width // 128):
                tile_of = value[:, c * 128:(c + 1) * 128]
                total = total + tile_of * tile_of
        return row_scale(total)

    order = [2 * xx + cc for cc in (1 - core, core) for xx in (1 - x, x)]
    sides = (1 - low, low)
    for h in range(2):
        for c, (first, count) in enumerate(cuts[h]):
            base = sides[h] * rows + first
            part = subs(base, count)
            scale = mix(base, count)
            a = jnp.dot(normed[part, :], gate_all[...], preferred_element_type=f32) * scale * vector(6, upper(z) * small, big)
            b = jnp.dot(normed[part, :], up_all[...], preferred_element_type=f32) * scale * vector(7, upper(z) * small, big)
            hidden[part, :] = (a / (1.0 + jnp.exp(-a)) * b).astype(half)
            for n, zz in enumerate(order):
                product = jnp.dot(hidden[part, :], down_all[:, lanes(zz * width, width)], preferred_element_type=f32)
                for j in range(2):
                    partial[2 * zz + j, part, :] = product[:, j * block:(j + 1) * block].astype(half)
                for j in range(2):
                    part_send(2 * zz + j, h, c, base, count)
                if n > 1:
                    for j in range(2):
                        part_sum(2 * zz + j, h, c, base, first, count)

    flush()
    for j in range(2):
        for k, h in ((0, 1), (1, 0), (2, 0)):
            for c, (first, count) in enumerate(cuts[h]):
                arrive(shares.at[k, j, pl.ds(first, count)], rs_recv.at[k, j, c])
        f = 2 * tp + j

        def total_rows(i, carry, j=j, f=f):
            at = pl.multiple_of(i * 128, 128)
            here = pl.ds(pl.multiple_of(low * rows + at, 128), 128)
            total = partial[f, here, :].astype(f32)
            for k in range(3):
                total = total + shares[k, j, pl.ds(at, 128), :].astype(f32)
            value = mixed_all[here, lanes(f * block, block)].astype(f32)
            out[pl.ds(at, 128), j * block:(j + 1) * block] = (
                value + total * (0.5 * vector(2, j * block, block))).astype(half)
            return carry
        lax.fori_loop(0, rows // 128, total_rows, 0)


def fits(nfs, ntp, stream, gate, pool_in):
    ny, nz = fs_grid(nfs)
    tiles = gate.shape[1] // 128
    return (
        (ny, nz, ntp) == (2, 4, 4) and gate.shape[1] % 128 == 0 and tiles % 2 == 1 and tiles > 1
        and stream.shape[0] % SEQ == 0 and stream.shape[0] > SEQ and SEQ % 128 == 0 and pool_in.shape[1] % 128 == 0
        and gate.shape[0] % 128 == 0 and stream.shape[1] == 2 * gate.shape[0]
    )


def whole_layer(stream, weights, vectors):
    gate, up, down, pool_in, pool_out = weights
    rows, width = stream.shape
    block, units = gate.shape
    chans = pool_in.shape[1]
    features = 4 * width
    small = (units // 128 // 2) * 128
    extra = units - 2 * small
    big = small + extra
    every = 2 * rows
    f32, half = jnp.float32, jnp.bfloat16
    vmem = pl.BlockSpec(memory_space=pltpu.VMEM)
    hbm = pl.BlockSpec(memory_space=pltpu.HBM)
    dma = pltpu.SemaphoreType.DMA
    return pl.pallas_call(
        functools.partial(layer_kernel, (rows, small, extra)),
        name="whole_layer",
        out_shape=jax.ShapeDtypeStruct((rows, width), half),
        in_specs=[hbm] * (1 + len(weights) + len(vectors)),
        out_specs=vmem,
        scratch_shapes=[pltpu.VMEM((1, sum(v.shape[0] for v in vectors)), f32)] + [
            pltpu.VMEM(w.shape, half) for w in weights] + [pltpu.VMEM(w.shape, f32) for w in weights] + [
            pltpu.VMEM((features, big), half), pltpu.VMEM((features, big), half), pltpu.VMEM((big, features), half),
            pltpu.VMEM((features, 4 * chans), half), pltpu.VMEM((4 * chans, features), half),
            pltpu.VMEM((4, 1, chans + 2 * width), f32),
            pltpu.VMEM((every, features), half), pltpu.VMEM((every, features), half),
            pltpu.VMEM((every, features), half), pltpu.VMEM((every, features), half),
            pltpu.VMEM((every, big), f32), pltpu.VMEM((every, big), f32), pltpu.VMEM((every, big), half),
            pltpu.VMEM((rows, 4 * chans), half),
            pltpu.VMEM((8, every, block), half), pltpu.VMEM((2, 4, every, block), half),
            pltpu.VMEM((3, 2, rows, block), half), pltpu.VMEM((2, 4, rows, block), half),
            dma((5,)), dma((len(vectors),)), dma((13,)), dma((4, 3, 3)), dma((4, 3, 3)), dma((8, 3, 3)),
            dma((2, 4)), dma((2, 4)), dma((2, 8)), dma((2, 3)), dma((2, 4)),
            dma((3,)), dma((4,)), dma((2, 2, 7)), dma((2, 2, 4, 2)),
            dma((8, 2)), dma((4, 2)), dma((8, 2, 2)), dma((4, 2, 2)), dma((4, 3, 2)), dma((3, 2, 2)),
            dma((4, 5)), dma((4, 3)), dma((4, 2)),
        ],
        compiler_params=pltpu.CompilerParams(
            collective_id=0, has_side_effects=True, vmem_limit_bytes=54 << 20),
    )(stream, *weights, *vectors)


def body(
    nfs, ntp,
    stream, gain_first, gain_mixer, gain_second,
    gate_weight, gate_scale, up_weight, up_scale, down_weight, down_scale,
    pool_in_weight, pool_in_scale, pool_out_weight, pool_out_scale,
):
    half = jnp.bfloat16
    if fits(nfs, ntp, stream, gate_weight, pool_in_weight):
        return whole_layer(
            stream, (gate_weight, up_weight, down_weight, pool_in_weight, pool_out_weight),
            (pool_in_scale, pool_out_scale, down_scale, gain_first, gain_mixer, gain_second, gate_scale, up_scale))
    in_half, out_half = pool_in_weight.astype(half), pool_out_weight.astype(half)
    width, channels = stream.shape[1], in_half.shape[1]
    scales = jnp.concatenate([pool_in_scale, pool_out_scale]).reshape(1, -1)
    in_all, out_all, gate_all, up_all, down_all, stream_all, scales_all = gather_all(
        nfs, ntp, in_half, out_half, gate_weight.astype(half), up_weight.astype(half), down_weight.astype(half),
        stream, scales,
    )
    in_whole, out_whole = flat(in_all), flat(out_all)
    gate_whole, up_whole, down_whole = flat(gate_all), flat(up_all), flat(down_all)
    in_scale = scales_all[:, 0, :channels].reshape(-1)
    out_scale = scales_all[:, 0, channels:].reshape(-1)
    tp = lax.axis_index("tp")

    def feed_forward(rows):
        gate_sum = jnp.dot(rows, gate_whole, preferred_element_type=jnp.float32) * gate_scale
        up_sum = jnp.dot(rows, up_whole, preferred_element_type=jnp.float32) * up_scale
        hidden = (jax.nn.silu(gate_sum) * up_sum).astype(half)
        return jnp.dot(hidden, down_whole, preferred_element_type=jnp.float32).astype(half)

    first = rms(flat(stream_all).astype(jnp.float32), gain_first)
    after_first = summed(ntp, True, 1, feed_forward(first), stream, down_scale)
    mixer_normed = rms(after_first.astype(jnp.float32), gain_mixer)
    pool_input = (
        jnp.dot(mixer_normed, in_whole, preferred_element_type=jnp.float32) * in_scale
    ).astype(half)
    mixed = jnp.dot(pooling(pool_input), out_whole, preferred_element_type=jnp.float32)
    after_mix = (after_first.astype(jnp.float32) + mixed * out_scale).astype(half)
    second = rms(after_mix.astype(jnp.float32), gain_second)
    own = lax.dynamic_slice_in_dim(after_mix, tp * stream.shape[1], stream.shape[1], axis=1)
    return summed(ntp, False, 2, feed_forward(second), own, down_scale)


def solution(mesh):
    placed = (
        P("fs", "tp"), P(), P(), P(),
        P("fs", "tp"), P("tp"), P("fs", "tp"), P("tp"), P("tp", "fs"), P("tp"),
        P("fs", "tp"), P("tp"), P("tp", "fs"), P("tp"),
    )
    return jax.shard_map(
        functools.partial(body, mesh.shape["fs"], mesh.shape["tp"]),
        mesh=mesh, in_specs=placed, out_specs=P("fs", "tp"), check_vma=False,
    )
```

```python
import functools

import jax
import jax.numpy as jnp
from jax import lax
from jax.experimental import pallas as pl
from jax.experimental.pallas import tpu as pltpu
from jax.sharding import PartitionSpec as P

SEQ = 128
MESH = pl.DeviceIdType.MESH

eps = 1e-06
WINDOWS = (2, 4, 8, 16)
Z_FIRST = (3, 5, 7)


def fs_grid(count):
    ny = 1
    while (2 * ny) * (2 * ny) <= count and count % (2 * ny) == 0:
        ny *= 2
    return ny, count // ny


def grid_shape(row_blocks, col_blocks, block):
    rows, cols = block
    if cols % 128 == 0:
        return (row_blocks * rows, col_blocks * cols)
    return (row_blocks, col_blocks, rows, cols)


def place(whole, block, row_block, col_block, part=(0, None)):
    rows, cols = block
    first, count = part[0], rows if part[1] is None else part[1]
    if len(whole.shape) == 2:
        return whole.at[
            pl.ds(pl.multiple_of(row_block * rows + first, 16), count),
            pl.ds(pl.multiple_of(col_block * cols, 128), cols),
        ]
    return whole.at[row_block, col_block, pl.ds(first, count)]


def flat(whole):
    if whole.ndim == 2:
        return whole
    return whole.transpose(0, 2, 1, 3).reshape(whole.shape[0] * whole.shape[2], -1)


def gather_kernel(nfs, ntp, pool_in, pool_out, gate, up, down, stream, scales,
                  in_all, out_all, gate_all, up_all, down_all, stream_all, scales_all,
                  send_sem, recv_sem, local_sem, tsend, trecv, psend, precv, ssend, srecv):
    ny, nz = fs_grid(nfs)
    nx = ntp // 2
    fs, tp = lax.axis_index("fs"), lax.axis_index("tp")
    z, y = fs // ny, fs % ny
    x, core = tp // 2, tp % 2
    partner = x * 2 + (1 - core)
    alternate = ny == 2 and nz > 1

    barrier = pltpu.get_barrier_semaphore()

    def greet(cond, f, t):
        @pl.when(cond)
        def _():
            pl.semaphore_signal(barrier, inc=1, device_id={"fs": f, "tp": t}, device_id_type=MESH)

    greet(z > 0, fs - ny, tp)
    greet(z < nz - 1, fs + ny, tp)
    greet(y > 0, fs - 1, tp)
    greet(y < ny - 1, fs + 1, tp)
    for k in range(1, ntp):
        pl.semaphore_signal(
            barrier, inc=1, device_id={"fs": fs, "tp": (tp + k) % ntp}, device_id_type=MESH
        )
    peers = ntp - 1
    for cond in (z > 0, z < nz - 1, y > 0, y < ny - 1):
        peers = peers + jnp.where(cond, 1, 0)
    pl.semaphore_wait(barrier, peers)

    pieces = [
        (lambda: pool_in, lambda f: place(in_all, pool_in.shape, f, tp)),
        (lambda: pool_out, lambda f: place(out_all, pool_out.shape, tp, f)),
    ]
    npool = len(pieces)
    for own, whole, by_rows in ((gate, gate_all, True), (up, up_all, True), (down, down_all, False)):
        rows = own.shape[0]
        halves = 2 if alternate else 1
        for h in range(halves):
            part = (h * (rows // halves), rows // halves)

            def own_part(own=own, part=part):
                return own.at[pl.ds(*part)]

            def whole_part(f, own=own, whole=whole, part=part, by_rows=by_rows):
                return place(whole, own.shape, f if by_rows else 0, 0 if by_rows else f, part)

            pieces.append((own_part, whole_part))
    started = []

    def remote(piece, f, direction, target, mine=False):
        own, whole = pieces[piece]
        return pltpu.make_async_remote_copy(
            src_ref=own() if mine else whole(f),
            dst_ref=whole(f),
            send_sem=send_sem.at[piece, f, direction],
            recv_sem=recv_sem.at[piece, f],
            device_id={"fs": target, "tp": tp},
            device_id_type=MESH,
        )

    def send(cond, piece, f, direction, mine=False):
        target = fs + (-ny, ny, -1, 1)[direction]

        @pl.when(cond)
        def _():
            remote(piece, f, direction, target, mine).start()

        started.append((cond, piece, f, direction, target, mine))

    def arrived(cond, piece, f):
        @pl.when(cond)
        def _():
            remote(piece, f, 0, fs, False).wait_recv()

    def by_y(cond, piece, f, mine=False):
        send(cond & (y > 0), piece, f, 2, mine)
        send(cond & (y < ny - 1), piece, f, 3, mine)

    yes = z >= 0

    def stream_place(slot):
        return place(stream_all, stream.shape, 0, slot)

    def stream_copy(src, slot, t_target, k):
        return pltpu.make_async_remote_copy(
            src_ref=src, dst_ref=stream_place(slot), send_sem=tsend.at[k], recv_sem=trecv.at[slot],
            device_id={"fs": fs, "tp": t_target}, device_id_type=MESH)

    def slab(which, slot):
        if which == 0:
            if len(in_all.shape) == 2:
                cols = pool_in.shape[1]
                return in_all.at[:, pl.ds(pl.multiple_of(slot * cols, 128), cols)]
            return in_all.at[:, slot]
        if len(out_all.shape) == 2:
            rows = pool_out.shape[0]
            return out_all.at[pl.ds(pl.multiple_of(slot * rows, 16), rows)]
        return out_all.at[slot]

    def pool_copy(which, slot, t_target, k):
        return pltpu.make_async_remote_copy(
            src_ref=slab(which, slot), dst_ref=slab(which, slot),
            send_sem=psend.at[which, k], recv_sem=precv.at[which, slot],
            device_id={"fs": fs, "tp": t_target}, device_id_type=MESH)

    def scale_copy(k, slot, t_target):
        return pltpu.make_async_remote_copy(
            src_ref=scales, dst_ref=scales_all.at[slot], send_sem=ssend.at[k], recv_sem=srecv.at[slot],
            device_id={"fs": fs, "tp": t_target}, device_id_type=MESH)

    npieces = len(pieces)
    locals_ = [pltpu.make_async_copy(own(), whole(fs), local_sem.at[i]) for i, (own, whole) in enumerate(pieces)]
    locals_.append(pltpu.make_async_copy(stream, stream_place(tp), local_sem.at[npieces]))
    locals_.append(pltpu.make_async_copy(scales, scales_all.at[tp], local_sem.at[npieces + 1]))
    for piece in range(npieces):
        send(z > 0, piece, fs, 0, True)
        send(z < nz - 1, piece, fs, 1, True)
        by_y(yes, piece, fs, True)
    stream_sends = []
    for k in range(1, nx):
        stream_sends.append(stream_copy(stream, tp, (x + k) % nx * 2 + core, k - 1))
    stream_sends.append(stream_copy(stream, tp, partner, nx - 1))
    stream_sends += [scale_copy(k - 1, tp, (tp + k) % ntp) for k in range(1, ntp)]
    for copy in stream_sends:
        copy.start()
    for copy in locals_:
        copy.start()

    def row_arrivals(piece, d, alt):
        low, high = fs - d * ny, fs + d * ny
        has_low, has_high = z >= d, z + d <= nz - 1
        for cond, f, direction, ahead, end in (
            (has_low, low, 1, z < nz - 1, z == d),
            (has_high, high, 0, z > 0, z + d == nz - 1),
        ):
            arrived(cond, piece, f)
            send(cond & ahead, piece, f, direction)
            if alt:
                by_y(cond & jnp.logical_not(end), piece, f)
                other = f + 1 - 2 * y
                arrived(cond & end, piece, other)
                send(cond & end & ahead, piece, other, direction)
            else:
                by_y(cond, piece, f)

    def column_arrivals(piece, alt):
        for d in range(nz):
            for sign in ((1,) if d == 0 else (-1, 1)):
                row_ok = (z + sign * d >= 0) & (z + sign * d <= nz - 1)
                if alt:
                    at = z + sign * d
                    if d == 0:
                        continue
                    row_ok = row_ok & (at != 0) & (at != nz - 1)
                base = fs + sign * d * ny
                for e in range(1, ny):
                    for step, direction, ok, ahead in (
                        (-e, 3, y >= e, y < ny - 1),
                        (e, 2, y + e <= ny - 1, y > 0),
                    ):
                        arrived(row_ok & ok, piece, base + step)
                        if ny > 2:
                            send(row_ok & ok & ahead, piece, base + step, direction)

    is_alt = [alternate and p >= npool and p % 2 == 1 for p in range(npieces)]

    for d in range(1, nz):
        for p in range(npool):
            row_arrivals(p, d, False)
    pool_sends = []
    for p in range(npool):
        column_arrivals(p, False)
        locals_[p].wait()
        pool_sends += [pool_copy(p, tp, (x + k) % nx * 2 + core, k - 1) for k in range(1, nx)]
        pool_sends.append(pool_copy(p, tp, partner, nx - 1))
    for copy in pool_sends:
        copy.start()
    for k in range(1, nx):
        slot = (x + k) % nx * 2 + core
        stream_copy(stream, slot, partner, 0).wait_recv()
        copy = stream_copy(stream_place(slot), slot, partner, nx - 1 + k)
        copy.start()
        stream_sends.append(copy)

    for p in range(npieces):
        if is_alt[p]:
            other = fs + 1 - 2 * y
            arrived(yes, p, other)
            send(z == 0, p, other, 1)
            send(z == nz - 1, p, other, 0)
    for d in range(1, nz):
        for p in range(npool, npieces):
            row_arrivals(p, d, is_alt[p])
        if d == 1:
            for k in range(1, nx):
                slot = (x + k) % nx * 2 + core
                for p in range(npool):
                    pool_copy(p, slot, partner, 0).wait_recv()
                    copy = pool_copy(p, slot, partner, nx - 1 + k)
                    copy.start()
                    pool_sends.append(copy)
    for p in range(npool, npieces):
        column_arrivals(p, is_alt[p])
    for k in range(nx):
        slot = (x + k) % nx * 2 + (1 - core)
        stream_copy(stream, slot, partner, 0).wait_recv()
        for p in range(npool):
            pool_copy(p, slot, partner, 0).wait_recv()
    for k in range(1, ntp):
        scale_copy(0, (tp + k) % ntp, partner).wait_recv()
    for copy in locals_[npool:]:
        copy.wait()
    for copy in stream_sends + pool_sends:
        copy.wait_send()
    for cond, piece, f, direction, target, mine in started:
        @pl.when(cond)
        def _():
            remote(piece, f, direction, target, mine).wait_send()


def gather_all(nfs, ntp, pool_in, pool_out, gate, up, down, stream, scales):
    ny, nz = fs_grid(nfs)
    nx = ntp // 2
    npieces = 8 if (ny == 2 and nz > 1) else 5
    any_spec = pl.BlockSpec(memory_space=pl.ANY)
    shapes = (
        grid_shape(nfs, ntp, pool_in.shape),
        grid_shape(ntp, nfs, pool_out.shape),
        grid_shape(nfs, 1, gate.shape),
        grid_shape(nfs, 1, up.shape),
        grid_shape(1, nfs, down.shape),
        grid_shape(1, ntp, stream.shape),
    )
    dma = pltpu.SemaphoreType.DMA
    return pl.pallas_call(
        functools.partial(gather_kernel, nfs, ntp),
        name="collect_weights",
        out_shape=tuple(jax.ShapeDtypeStruct(shape, jnp.bfloat16) for shape in shapes)
        + (jax.ShapeDtypeStruct((ntp,) + scales.shape, jnp.float32),),
        in_specs=[any_spec] * 7,
        out_specs=[any_spec] * 7,
        scratch_shapes=[
            dma((npieces, nfs, 4)),
            dma((npieces, nfs)),
            dma((npieces + 2,)),
            dma((2 * nx,)),
            dma((ntp,)),
            dma((2, 2 * nx)),
            dma((2, ntp)),
            dma((ntp,)),
            dma((ntp,)),
        ],
        compiler_params=pltpu.CompilerParams(collective_id=0, has_side_effects=True, vmem_limit_bytes=1 << 20),
    )(pool_in, pool_out, gate, up, down, stream, scales)


def sum_kernel(ntp, gathers, pieces, partial, resid, scale, out, pair, pair_sum, cross, *sems):
    pair_send, pair_recv, cross_send, cross_recv = sems[:4]
    nx = ntp // 2
    tp, fs = lax.axis_index("tp"), lax.axis_index("fs")
    x, core = tp // 2, tp % 2
    partner = x * 2 + (1 - core)
    rows, width = resid.shape
    step = rows // pieces
    barrier = pltpu.get_barrier_semaphore()
    pl.semaphore_signal(barrier, inc=1, device_id={"fs": fs, "tp": partner}, device_id_type=MESH)
    for k in range(1, nx):
        pl.semaphore_signal(
            barrier, inc=1, device_id={"fs": fs, "tp": (x + k) % nx * 2 + core}, device_id_type=MESH
        )
    pl.semaphore_wait(barrier, nx)

    def remote(src, dst, send, recv, target):
        return pltpu.make_async_remote_copy(
            src_ref=src, dst_ref=dst, send_sem=send, recv_sem=recv,
            device_id={"fs": fs, "tp": target}, device_id_type=MESH)

    def columns(t):
        return pl.ds(pl.multiple_of(t * width, width), width)

    parts = [pl.ds(i * step, step) for i in range(pieces)]
    offsets = list(range(1, nx)) + [0]
    sends = []
    for k in offsets:
        for i, part in enumerate(parts):
            copy = remote(partial.at[part, columns((x + k) % nx * 2 + (1 - core))], pair.at[k, part],
                          pair_send.at[k, i], pair_recv.at[k, i], partner)
            copy.start()
            sends.append(copy)
    for k in offsets[:-1]:
        target = (x + k) % nx * 2 + core
        for i, part in enumerate(parts):
            remote(pair.at[k, part], pair.at[k, part], pair_send.at[k, i], pair_recv.at[k, i], partner).wait_recv()
            pair_sum[k - 1, part] = (
                partial[part, columns(target)].astype(jnp.float32) + pair[k, part].astype(jnp.float32)
            ).astype(jnp.bfloat16)
            copy = remote(pair_sum.at[k - 1, part], cross.at[k - 1, part],
                          cross_send.at[k - 1, i], cross_recv.at[k - 1, i], target)
            copy.start()
            sends.append(copy)
    factor = 0.5 * scale[...]
    for i, part in enumerate(parts):
        remote(pair.at[0, part], pair.at[0, part], pair_send.at[0, i], pair_recv.at[0, i], partner).wait_recv()
        total = partial[part, columns(tp)].astype(jnp.float32) + pair[0, part].astype(jnp.float32)
        for k in range(1, nx):
            remote(cross.at[k - 1, part], cross.at[k - 1, part], cross_send.at[k - 1, i],
                   cross_recv.at[k - 1, i], partner).wait_recv()
            total = total + cross[k - 1, part].astype(jnp.float32)
        result = (resid[part].astype(jnp.float32) + total * factor).astype(jnp.bfloat16)
        if not gathers:
            out[part] = result
            continue
        out[part, columns(tp)] = result
        gather_send, gather_recv = sems[4:]
        for k in range(1, nx):
            copy = remote(out.at[part, columns(tp)], out.at[part, columns(tp)], gather_send.at[k - 1, i], gather_recv.at[tp, i],
                          (x + k) % nx * 2 + core)
            copy.start()
            sends.append(copy)
        copy = remote(out.at[part, columns(tp)], out.at[part, columns(tp)], gather_send.at[nx - 1, i], gather_recv.at[tp, i], partner)
        copy.start()
        sends.append(copy)
    if gathers:
        for k in range(1, nx):
            slot = (x + k) % nx * 2 + core
            for i, part in enumerate(parts):
                remote(out.at[part, columns(slot)], out.at[part, columns(slot)], gather_send.at[0, i], gather_recv.at[slot, i],
                       partner).wait_recv()
                copy = remote(out.at[part, columns(slot)], out.at[part, columns(slot)], gather_send.at[nx - 1 + k, i],
                              gather_recv.at[slot, i], partner)
                copy.start()
                sends.append(copy)
        for k in range(nx):
            slot = (x + k) % nx * 2 + (1 - core)
            for i, part in enumerate(parts):
                remote(out.at[part, columns(slot)], out.at[part, columns(slot)], gather_send.at[0, i], gather_recv.at[slot, i],
                       partner).wait_recv()
    for copy in sends:
        copy.wait_send()


def summed(ntp, gathers, identity, partial, resid, scale):
    nx = ntp // 2
    rows, width = resid.shape
    pieces = 3 if rows % 48 == 0 else 1
    vmem = pl.BlockSpec(memory_space=pltpu.VMEM)
    dma = pltpu.SemaphoreType.DMA
    scratch = [
        pltpu.VMEM((nx, rows, width), jnp.bfloat16),
        pltpu.VMEM((max(nx - 1, 1), rows, width), jnp.bfloat16),
        pltpu.VMEM((max(nx - 1, 1), rows, width), jnp.bfloat16),
        dma((nx, pieces)), dma((nx, pieces)), dma((nx, pieces)), dma((nx, pieces)),
    ]
    if gathers:
        scratch += [dma((2 * nx, pieces)), dma((ntp, pieces))]
    return pl.pallas_call(
        functools.partial(sum_kernel, ntp, gathers, pieces),
        name="sum_and_share" if gathers else "sum_last",
        out_shape=jax.ShapeDtypeStruct((rows, width * (ntp if gathers else 1)), jnp.bfloat16),
        in_specs=[vmem] * 3,
        out_specs=vmem,
        scratch_shapes=scratch,
        compiler_params=pltpu.CompilerParams(
            collective_id=identity, has_side_effects=True, vmem_limit_bytes=32 << 20
        ),
    )(partial, resid, scale.reshape(1, width))


def rms(floats, norm_gain):
    scaled = floats * lax.rsqrt(jnp.mean(floats * floats, axis=-1, keepdims=True) + eps)
    return (scaled * norm_gain).astype(jnp.bfloat16)


def window_weights():
    position = jnp.arange(SEQ)
    rows, cols = position[:, None], position[None, :]
    mats = []
    for window in WINDOWS:
        low = jnp.maximum(rows - window // 2, 0)
        high = jnp.minimum(rows + window - window // 2, SEQ)
        mats.append(((cols >= low) & (cols < high)).astype(jnp.bfloat16))
    return mats


def pooling(pool_input):
    channels = pool_input.shape[1]
    group = channels // 4
    values = pool_input.reshape(-1, SEQ, channels)
    position = jnp.arange(SEQ)
    parts = []
    for index, (window, members) in enumerate(zip(WINDOWS, window_weights())):
        own = values[:, :, index * group:(index + 1) * group]
        sums = jnp.einsum("pq,sqc->spc", members, own, preferred_element_type=jnp.float32)
        before = window // 2
        counts = (
            jnp.minimum(position + window - before, SEQ) - jnp.maximum(position - before, 0)
        ).astype(jnp.float32)
        parts.append(sums / counts[None, :, None] - own.astype(jnp.float32))
    return jnp.concatenate(parts, axis=2).reshape(-1, channels).astype(jnp.bfloat16)


def layer_kernel(
    sizes, stream, gate_in, up_in, down_in, in_in, out_in, *refs):
    parts, (out, vectors, *rest) = refs[:8], refs[8:]
    layer_steps(sizes, stream, gate_in, up_in, down_in, in_in, out_in, parts, out, vectors, *rest)


def layer_steps(
    sizes, stream, gate_in, up_in, down_in, in_in, out_in, parts, out, vectors,
    gate, up, down, pool_in, pool_out, gate_wide, up_wide, down_wide, in_wide, out_wide,
    gate_all, up_all, down_all, in_all, out_all, scales_all, rows_all, first_all, mixed_all, normed,
    gate_sum, up_sum, hidden, pooled, partial, pair, shares, first_in,
    load_sem, vector_sem, local_sem, z_send, y_send, w_recv, pl_zsend, pl_ysend, pl_recv, slab_send, slab_recv,
    sc_send, sc_recv, ag_send, ag_recv, pair_send, pair_recv, two_send, two_recv, rs_send, rs_recv,
    fr_send, fr_recv, fr_core,
):
    rows, small, extra = sizes
    big = small + extra
    block = gate.shape[0]
    width = stream.shape[1]
    chans = pool_in.shape[1]
    units = gate.shape[1]
    features = gate_all.shape[0]
    starts = [0]
    for count in (chans, width, width, features, features, features, units, units):
        starts.append(starts[-1] + count)
    scales = vectors.at[:, :chans + 2 * width]

    def vector(at, first, count):
        return vectors[:, pl.ds(pl.multiple_of(starts[at] + first, 128), count)]

    every = 2 * rows
    f32, half = jnp.float32, jnp.bfloat16
    fs, tp = lax.axis_index("fs"), lax.axis_index("tp")
    z, y = fs // 2, fs % 2
    x, core = tp // 2, tp % 2
    low, pair_hi = z % 2, z // 2
    zp = z + 1 - 2 * low
    zs = [z, zp, 2 - pair_hi, 3 - 3 * pair_hi]
    fs_y, fs_z = fs + 1 - 2 * y, 2 * zp + y
    tp_c, tp_x = tp + 1 - 2 * core, (tp + 2) % 4
    tp_xc = tp_x + 1 - 2 * core

    def upper(at):
        return (((at + 1) // 2) % 2 + core) % 2

    own_rows = pl.ds(pl.multiple_of(low * rows, 16), rows)
    stream_own = pltpu.make_async_copy(
        stream, rows_all.at[own_rows, pl.ds(pl.multiple_of(tp * width, 128), width)], local_sem.at[0])
    stream_own.start()
    vector_copies = [
        pltpu.make_async_copy(ref, vectors.at[0, pl.ds(first, ref.shape[0])], vector_sem.at[i])
        for i, (ref, first) in enumerate(zip(parts, starts))]
    for copy in vector_copies:
        copy.start()
    loads = []
    for i, (wide, ref, narrow) in enumerate((
        (in_wide, in_in, pool_in), (out_wide, out_in, pool_out), (gate_wide, gate_in, gate),
        (up_wide, up_in, up), (down_wide, down_in, down),
    )):
        copy = pltpu.make_async_copy(ref, wide, load_sem.at[i])
        copy.start()
        loads.append((copy, wide, narrow))

    barrier = pltpu.get_barrier_semaphore()
    peers = [(2 * at + y, tp) for at in zs[1:]] + [
        (fs_y, tp), (fs, tp_c), (fs, tp_x), (fs, tp_xc), (fs_z, tp_x)]
    for f, t in peers:
        pl.semaphore_signal(barrier, inc=1, device_id={"fs": f, "tp": t}, device_id_type=MESH)

    def narrowed(copy, wide, narrow):
        copy.wait()
        count = wide.shape[0]
        each = 64 if count % 64 == 0 else 16

        def one(i, carry):
            part = pl.ds(pl.multiple_of(i * each, each), each)
            narrow[part, :] = wide[part, :].astype(half)
            return carry
        lax.fori_loop(0, count // each, one, 0)

    for load in loads[:3]:
        narrowed(*load)
    stream_own.wait()
    for copy in vector_copies:
        copy.wait()
    pl.semaphore_wait(barrier, len(peers))

    ends = []

    def remote(src, dst, send, recv, f, t):
        return pltpu.make_async_remote_copy(
            src_ref=src, dst_ref=dst, send_sem=send, recv_sem=recv,
            device_id={"fs": f, "tp": t}, device_id_type=MESH)

    def start(make, cond=None):
        if cond is None:
            make().start()
        else:
            pl.when(cond)(lambda: make().start())
        ends.append((make, cond))

    def flush(count=None):
        for make, cond in ends[:count]:
            if cond is None:
                make().wait_send()
            else:
                pl.when(cond)(lambda make=make: make().wait_send())
        del ends[:count]

    def arrive(dst, recv, cond=None):
        def wait():
            remote(dst, dst, recv, recv, fs, tp_c).wait_recv()
        if cond is None:
            wait()
        else:
            pl.when(cond)(wait)

    def lanes(at, count):
        return pl.ds(pl.multiple_of(at, 128), count)

    def subs(at, count):
        return pl.ds(pl.multiple_of(at, 16), count)

    pieces = width // block

    def column_block(j, xx, cc):
        return (2 * xx + cc) * pieces + j

    def share_place(phase, ref, chip_low, j, xx, cc):
        return ref.at[subs(chip_low * rows, rows), lanes(column_block(j, xx, cc) * block, block)]

    def share_start(phase, ref, j, cond=None):
        here = share_place(phase, ref, low, j, x, core)
        for k, (f, t) in enumerate(((fs_z, tp), (fs, tp_x), (fs, tp_c))):
            start(lambda f=f, t=t, k=k: remote(
                here, here, ag_send.at[phase, j, k], ag_recv.at[phase, j, 2 * x + low, core], f, t), cond)

    def share_relay(phase, ref, j, k, chip_low, xx, targets, cond=None):
        here = share_place(phase, ref, chip_low, j, xx, core)
        flag = ag_recv.at[phase, j, 2 * xx + chip_low, core]
        arrive(here, flag, cond)
        for n, target in enumerate(targets):
            start(lambda n=n, target=target: remote(
                here, here, ag_send.at[phase, j, 3 + k + n], flag, fs, target), cond)

    def relay_own(phase, ref, j, cond=None):
        share_relay(phase, ref, j, 0, 1 - low, x, (tp_x, tp_c), cond)

    def relay_across(phase, ref, j, cond=None):
        share_relay(phase, ref, j, 2, low, 1 - x, (tp_c,), cond)
        share_relay(phase, ref, j, 3, 1 - low, 1 - x, (tp_c,), cond)

    def share_finish(phase, ref):
        for j in range(2):
            for xx in (x, 1 - x):
                for cl in (low, 1 - low):
                    arrive(share_place(phase, ref, cl, j, xx, 1 - core), ag_recv.at[phase, j, 2 * xx + cl, 1 - core])

    for j in range(2):
        share_start(0, rows_all, j)

    def scale_copy(k, slot, t):
        return remote(scales, scales_all.at[slot], sc_send.at[k], sc_recv.at[slot], fs, t)

    for k, t in enumerate((tp_c, tp_x, tp_xc)):
        start(lambda k=k, t=t: scale_copy(k, tp, t))
    locals_ = [pltpu.make_async_copy(scales, scales_all.at[tp], local_sem.at[1])]

    def pool_place(which, f, t):
        if which == 0:
            return in_all.at[subs(f * block, block), lanes(t * chans, chans)]
        return out_all.at[subs(t * chans, chans), lanes(f * block, block)]

    def pool_slab(which, t):
        if which == 0:
            return in_all.at[:, lanes(t * chans, chans)]
        return out_all.at[subs(t * chans, chans)]

    def pool_start():
        for which, own in enumerate((pool_in, pool_out)):
            for k in range(1, 4):
                start(lambda k=k, which=which, own=own: remote(
                    own, pool_place(which, fs, tp), pl_zsend.at[which, k], pl_recv.at[which, fs], 2 * zs[k] + y, tp))
            start(lambda which=which, own=own: remote(
                own, pool_place(which, fs, tp), pl_ysend.at[which, 0], pl_recv.at[which, fs], fs_y, tp))

    for which, own in enumerate((pool_in, pool_out)):
        locals_.append(pltpu.make_async_copy(own, pool_place(which, fs, tp), local_sem.at[2 + which]))

    PARTS = 3

    def own_part(piece, part, side):
        first = 2 * small if part == 2 else side * small
        if piece == 2:
            return down.at[subs(first + part % 2 * (small // 2), extra if part == 2 else small // 2)]
        ref = (gate, up)[piece]
        if part == 2:
            return ref.at[:, lanes(first, extra)]
        return ref.at[pl.ds(part * (block // 2), block // 2), lanes(first, small)]

    def all_part(piece, part, f):
        if piece == 2:
            at, count = (small, extra) if part == 2 else (part * (small // 2), small // 2)
            return down_all.at[pl.ds(at, count), lanes(f * block, block)]
        ref = (gate_all, up_all)[piece]
        if part == 2:
            return ref.at[subs(f * block, block), pl.ds(small, extra)]
        return ref.at[subs(f * block + part * (block // 2), block // 2), pl.ds(0, small)]

    def part_cond(part, wide, cond=None):
        if part < 2:
            return cond
        return wide == 1 if cond is None else cond & (wide == 1)

    def y_own(piece):
        for part in range(PARTS):
            start(lambda part=part: remote(
                own_part(piece, part, upper(z)), all_part(piece, part, fs), y_send.at[0, piece, part],
                w_recv.at[fs, piece, part], fs_y, tp), part_cond(part, upper(z)))

    def own_copy(piece, part):
        return pltpu.make_async_copy(
            own_part(piece, part, upper(z)), all_part(piece, part, fs), local_sem.at[4 + PARTS * piece + part])

    for copy in locals_:
        copy.start()
    inner = (z == 1) | (z == 2)

    def z_own(piece, cond=None, targets=(1, 2, 3)):
        for k in targets:
            at = zs[k]
            for part in range(PARTS):
                ok = part_cond(part, upper(at), cond)
                start(lambda k=k, at=at, part=part: remote(
                    own_part(piece, part, upper(at)), all_part(piece, part, fs), z_send.at[k, piece, part],
                    w_recv.at[fs, piece, part], 2 * at + y, tp), ok)

    outer = jnp.logical_not(inner)
    z_own(0, None, (1,))
    y_own(0)
    for load in loads[3:]:
        narrowed(*load)
    z_own(1, outer, (1,))
    z_own(0, None, (2, 3))
    pool_start()
    z_own(1, inner, (1,))
    z_own(1, None, (2, 3))
    y_own(1)
    y_own(2)
    z_own(2, None, (1,))
    for piece in range(3):
        own_copy(piece, 0).start()
        own_copy(piece, 1).start()
        pl.when(upper(z) == 1)(lambda piece=piece: own_copy(piece, 2).start())

    @pl.when(upper(z) == 0)
    def _():
        gate_all[:, small:big] = jnp.zeros((features, extra), half)
        up_all[:, small:big] = jnp.zeros((features, extra), half)
        down_all[small:big, :] = jnp.zeros((extra, features), half)

    def weights_here(piece, f):
        for part in range(PARTS):
            arrive(all_part(piece, part, f), w_recv.at[f, piece, part], part_cond(part, upper(z)))

    def by_z(piece, i):
        f = 2 * zs[i] + y
        for part in range(PARTS):
            cond = part_cond(part, upper(z))
            arrive(all_part(piece, part, f), w_recv.at[f, piece, part], cond)
            start(lambda part=part: remote(
                all_part(piece, part, f), all_part(piece, part, f), y_send.at[i, piece, part],
                w_recv.at[f, piece, part], fs_y, tp), cond)

    def own_here(piece):
        own_copy(piece, 0).wait()
        own_copy(piece, 1).wait()
        pl.when(upper(z) == 1)(lambda: own_copy(piece, 2).wait())

    step = 32
    lane_tiles = features // 128

    def norm_rows(source, gain_at, base=0):
        def one(i, carry):
            part = pl.ds(pl.multiple_of(base + i * 128, 128), 128)
            total = jnp.zeros((128, 128), f32)
            for c in range(lane_tiles):
                floats = source[part, c * 128:(c + 1) * 128].astype(f32)
                total = total + floats * floats
            scale = lax.rsqrt(jnp.sum(total, axis=-1, keepdims=True) * (1.0 / features) + eps)
            for c in range(lane_tiles):
                floats = source[part, c * 128:(c + 1) * 128].astype(f32)
                normed[part, c * 128:(c + 1) * 128] = ((floats * scale) * vector(gain_at, c * 128, 128)).astype(half)
            return carry
        return one

    for j in range(2):
        relay_own(0, rows_all, j)
    for j in range(2):
        relay_across(0, rows_all, j)
    share_finish(0, rows_all)
    lax.fori_loop(0, every // 128, norm_rows(rows_all, 3), 0)

    def pool_by_y():
        for k in range(1, 4):
            for which in range(2):
                f = 2 * zs[k] + y
                here = pool_place(which, f, tp)
                arrive(here, pl_recv.at[which, f])
                start(lambda k=k, which=which, here=here, f=f: remote(
                    here, here, pl_ysend.at[which, k], pl_recv.at[which, f], fs_y, tp))

    tile = 256

    def accumulate(weights, total, f, first):
        for n in range(big // 128 // 2 + 1):
            cols = slice(n * tile, min((n + 1) * tile, big))
            if cols.start < cols.stop:
                product = jnp.dot(normed[:, lanes(f * block, block)], weights[subs(f * block, block), cols],
                                  preferred_element_type=f32)
                total[:, cols] = product if first else total[:, cols] + product

    def pool_across():
        for which in range(2):
            locals_[1 + which].wait()
            for k in range(4):
                f = fs_y if k == 0 else 2 * zs[k] + 1 - y
                arrive(pool_place(which, f, tp), pl_recv.at[which, f])
            slab = pool_slab(which, tp)
            for n, t in enumerate((tp_x, tp_c)):
                start(lambda which=which, slab=slab, n=n, t=t: remote(
                    slab, slab, slab_send.at[which, n], slab_recv.at[which, tp], fs, t))

    early_sends = len(ends)
    ahead = [(piece, i) for piece in range(3) for i in range(1, 4)]
    for piece, (weights, total) in enumerate(((gate_all, gate_sum), (up_all, up_sum))):
        for i in range(4):
            f, g = 2 * zs[i] + y, 2 * zs[i] + 1 - y
            if i == 0:
                own_here(piece)
            accumulate(weights, total, f, i == 0)
            if 4 * piece + i < 7:
                by_z(*ahead[4 * piece + i])
            weights_here(piece, g)
            accumulate(weights, total, g, False)
            if (piece, i) == (0, 2):
                pool_by_y()
            if (piece, i) == (1, 0):
                z_own(2, outer, (2, 3))
                pool_across()
            if (piece, i) == (1, 1):
                z_own(2, inner, (2, 3))
    own_here(2)

    def hide(i, carry):
        part = pl.ds(pl.multiple_of(i * step, step), step)
        a = gate_sum[part, :] * vector(6, upper(z) * small, big)
        hidden[part, :] = (a / (1.0 + jnp.exp(-a)) * (up_sum[part, :] * vector(7, upper(z) * small, big))).astype(half)
        return carry

    lax.fori_loop(0, every // step, hide, 0)

    def block_send(f, r):
        zz = f // 2
        slot = 2 * (zz // 2) + f % 2
        part = subs(r * rows, rows)
        start(lambda: remote(
            partial.at[f, part], pair.at[0, slot, part], pair_send.at[f, r],
            pair_recv.at[slot, r], fs, tp_c), zz % 2 != core)

    def core_sum(f, r):
        slot = 2 * (f // 4) + f % 2

        @pl.when((f // 2) % 2 == core)
        def _():
            here = pair.at[0, slot, subs(r * rows, rows)]
            remote(here, here, pair_send.at[f, r], pair_recv.at[slot, r], fs, tp_c).wait_recv()

            def one(i, carry):
                at = pl.ds(pl.multiple_of(r * rows + i * 128, 128), 128)
                partial[f, at, :] = (
                    partial[f, at, :].astype(f32) + pair[0, slot, at, :].astype(f32)).astype(half)
                return carry
            lax.fori_loop(0, rows // 128, one, 0)

    pair_z = (jnp.where(low == core, zp, z), jnp.where(low == core, z, zp), zs[2], zs[3])
    blocks = [2 * zz + j for zz in pair_z for j in (y, 1 - y)]

    def ways(n):
        across_x, across_z = (fs, tp_x), (fs_z, tp)
        return (across_z, across_x, low) if n in Z_FIRST else (across_x, across_z, x)

    def first_send(n, k, src, dst, recv, to):
        f = blocks[n]
        start(lambda: remote(src, dst, fr_send.at[2 * (f // 4) + f % 2, k], recv, *to), (f // 2) % 2 == core)

    def first_sum(n):
        f = blocks[n]
        slot = 2 * (f // 4) + f % 2
        to, _, r = ways(n)
        core_sum(f, 1 - r)
        first_send(n, 0, partial.at[f, subs((1 - r) * rows, rows)], first_in.at[0, slot], fr_recv.at[slot, 0], to)
        core_sum(f, r)

    def first_add(n):
        f = blocks[n]
        slot = 2 * (f // 4) + f % 2
        _, to, r = ways(n)
        part = subs(r * rows, rows)

        @pl.when((f // 2) % 2 == core)
        def _():
            arrive(first_in.at[0, slot], fr_recv.at[slot, 0])

            def one(i, carry):
                at = pl.ds(pl.multiple_of(r * rows + i * 128, 128), 128)
                got = first_in[0, slot, pl.ds(pl.multiple_of(i * 128, 128), 128), :].astype(f32)
                partial[f, at, :] = (partial[f, at, :].astype(f32) + got).astype(half)
                return carry
            lax.fori_loop(0, rows // 128, one, 0)
        first_send(n, 1, partial.at[f, part], first_in.at[1, slot], fr_recv.at[slot, 1], to)

    def first_done(n):
        f = blocks[n]
        slot = 2 * (f // 4) + f % 2
        to, _, r = ways(n)
        cols = lanes(f * block, block)

        @pl.when((f // 2) % 2 == core)
        def _():
            arrive(first_in.at[1, slot], fr_recv.at[slot, 1])
            factor = 0.5 * scales_all[f // 2, :, pl.ds(pl.multiple_of(chans + width + (f % 2) * block, 128), block)]

            def one(i, carry):
                at = pl.ds(pl.multiple_of(r * rows + i * 128, 128), 128)
                total = partial[f, at, :].astype(f32) + first_in[
                    1, slot, pl.ds(pl.multiple_of(i * 128, 128), 128), :].astype(f32)
                first_all[at, cols] = (rows_all[at, cols].astype(f32) + total * factor).astype(half)
                return carry
            lax.fori_loop(0, rows // 128, one, 0)
        here = first_all.at[subs(r * rows, rows), cols]
        first_send(n, 2, here, here, fr_recv.at[slot, 2], to)
        first_send(n, 3, here, here, fr_core.at[slot, r], (fs, tp_c))

    def first_pass(n):
        f = blocks[n]
        slot = 2 * (f // 4) + f % 2
        r = 1 - ways(n)[2]
        here = first_all.at[subs(r * rows, rows), lanes(f * block, block)]
        arrive(here, fr_recv.at[slot, 2], (f // 2) % 2 == core)
        first_send(n, 4, here, here, fr_core.at[slot, r], (fs, tp_c))

    def first_finish():
        for f in blocks:
            slot = 2 * (f // 4) + f % 2
            for r in range(2):
                arrive(first_all.at[r * rows:(r + 1) * rows, lanes(f * block, block)], fr_core.at[slot, r],
                       (f // 2) % 2 != core)

    def part_send(f, h, c, base, count):
        slot = 2 * (f // 4) + f % 2
        part = subs(base, count)
        start(lambda: remote(
            partial.at[f, part], pair.at[1, slot, part], two_send.at[f, h, c], two_recv.at[slot, h, c], fs, tp_c),
            (f // 2) % 2 != core)

    def part_sum(f, h, c, base, first, count):
        slot = 2 * (f // 4) + f % 2
        part = subs(base, count)

        @pl.when((f // 2) % 2 == core)
        def _():
            arrive(pair.at[1, slot, part], two_recv.at[slot, h, c])

            def one(i, carry):
                at = pl.ds(pl.multiple_of(base + i * 128, 128), 128)
                partial[f, at, :] = (partial[f, at, :].astype(f32) + pair[1, slot, at, :].astype(f32)).astype(half)
                return carry
            lax.fori_loop(0, count // 128, one, 0)
        mine = f // 4 == x
        away = jnp.logical_not(mine)
        ways = ((1, fs_z, tp, mine), (2, fs_z, tp_x, away)) if h == 0 else ((0, fs, tp_x, away),)
        for k, fd, td, cond in ways:
            start(lambda k=k, fd=fd, td=td: remote(
                partial.at[f, part], shares.at[k, f % 2, pl.ds(first, count)], rs_send.at[slot, k, c],
                rs_recv.at[k, f % 2, c], fd, td), ((f // 2) % 2 == core) & cond)

    cuts = (((0, SEQ), (SEQ, rows - SEQ)), ((0, rows - SEQ), (rows - SEQ, SEQ)))

    def slab_across():
        for which in range(2):
            slab = pool_slab(which, tp_x)
            arrive(slab, slab_recv.at[which, tp_x])
            start(lambda which=which, slab=slab: remote(
                slab, slab, slab_send.at[which, 2], slab_recv.at[which, tp_x], fs, tp_c))

    locals_[0].wait()
    for t in (tp_c, tp_x, tp_xc):
        arrive(scales_all.at[t], sc_recv.at[t])
    def product_of(n):
        f = blocks[n]
        if n % 2:
            weights_here(2, f)
        partial[f, :, :] = jnp.dot(
            hidden[...], down_all[:, lanes(f * block, block)], preferred_element_type=f32).astype(half)
        for r in (1 - ways(n)[2], ways(n)[2]):
            block_send(f, r)

    def down_from(n):
        by_z(2, n)

    def slab(n):
        slab_across()
        flush(early_sends)

    for stage, members in (
        (product_of, (0, 1, 2, 3)), (first_sum, (2, 3)), (slab, (0,)), (first_add, (2, 3)), (down_from, (2,)),
        (product_of, (4,)), (down_from, (3,)), (product_of, (6,)), (first_sum, (4, 6)), (first_done, (2, 3)),
        (first_add, (4, 6)), (product_of, (5,)), (first_sum, (5,)), (first_pass, (2, 3)), (first_done, (4, 6)),
        (product_of, (7,)), (first_sum, (7,)), (first_add, (5,)), (first_pass, (4, 6)), (first_done, (5,)),
        (first_add, (7,)), (first_pass, (5,)), (first_done, (7,)), (first_pass, (7,)),
    ):
        for m in members:
            stage(m)
    for which in range(2):
        for t in (tp_c, tp_xc):
            arrive(pool_slab(which, t), slab_recv.at[which, t])
    flush()
    first_finish()

    in_scale = jnp.concatenate([scales_all[t, :, :chans] for t in range(4)], axis=1)
    group = 4 * chans // 4
    pos_row = lax.broadcasted_iota(jnp.int32, (SEQ, SEQ), 0)
    pos_col = lax.broadcasted_iota(jnp.int32, (SEQ, SEQ), 1)
    pos = lax.broadcasted_iota(jnp.int32, (SEQ, 1), 0)

    def row_scale(total):
        return lax.rsqrt(jnp.sum(total, axis=-1, keepdims=True) * (1.0 / features) + eps)

    def gained_rows(base, count):
        scale = []
        for i in range(count // 128):
            part = pl.ds(pl.multiple_of(base + i * 128, 128), 128)
            total = jnp.zeros((128, 128), f32)
            for c in range(lane_tiles):
                cols = slice(c * 128, (c + 1) * 128)
                floats = first_all[part, cols].astype(f32)
                total = total + floats * floats
                normed[part, cols] = (floats * vector(4, c * 128, 128)).astype(half)
            scale.append(row_scale(total))
        return jnp.concatenate(scale, axis=0)

    def mix(base, count):
        scale = gained_rows(base, count)
        part = pl.ds(pl.multiple_of(base, 128), count)
        pool_input = (
            jnp.dot(normed[part, :], in_all[...], preferred_element_type=f32) * scale * in_scale).astype(half)
        for index, window in enumerate(WINDOWS):
            before = window // 2
            first = jnp.maximum(pos_row - before, 0)
            last = jnp.minimum(pos_row + window - before, SEQ)
            members = jnp.where((pos_col >= first) & (pos_col < last), 1.0, 0.0).astype(half)
            counts = (jnp.minimum(pos + window - before, SEQ) - jnp.maximum(pos - before, 0)).astype(f32)
            for s in range(count // SEQ):
                own = pool_input[s * SEQ:(s + 1) * SEQ, index * group:(index + 1) * group]
                sums = jnp.dot(members, own, preferred_element_type=f32)
                pooled[s * SEQ:(s + 1) * SEQ, index * group:(index + 1) * group] = (
                    sums / counts - own.astype(f32)).astype(half)
        total = jnp.zeros((count, 128), f32)
        for t in range(4):
            cols = slice(t * width, (t + 1) * width)
            mixed = jnp.dot(pooled[:count, :], out_all[:, cols], preferred_element_type=f32)
            value = (first_all[part, cols].astype(f32) + mixed * scales_all[t, :, chans:chans + width]).astype(half)
            mixed_all[part, cols] = value
            value = value.astype(f32)
            normed[part, cols] = (value * vector(5, t * width, width)).astype(half)
            for c in range(width // 128):
                tile_of = value[:, c * 128:(c + 1) * 128]
                total = total + tile_of * tile_of
        return row_scale(total)

    order = [2 * xx + cc for cc in (1 - core, core) for xx in (1 - x, x)]
    sides = (1 - low, low)
    for h in range(2):
        for c, (first, count) in enumerate(cuts[h]):
            base = sides[h] * rows + first
            part = subs(base, count)
            scale = mix(base, count)
            a = jnp.dot(normed[part, :], gate_all[...], preferred_element_type=f32) * scale * vector(6, upper(z) * small, big)
            b = jnp.dot(normed[part, :], up_all[...], preferred_element_type=f32) * scale * vector(7, upper(z) * small, big)
            hidden[part, :] = (a / (1.0 + jnp.exp(-a)) * b).astype(half)
            for n, zz in enumerate(order):
                product = jnp.dot(hidden[part, :], down_all[:, lanes(zz * width, width)], preferred_element_type=f32)
                for j in range(2):
                    partial[2 * zz + j, part, :] = product[:, j * block:(j + 1) * block].astype(half)
                for j in range(2):
                    part_send(2 * zz + j, h, c, base, count)
                if n > 1:
                    for j in range(2):
                        part_sum(2 * zz + j, h, c, base, first, count)

    flush()
    for j in range(2):
        for k, h in ((0, 1), (1, 0), (2, 0)):
            for c, (first, count) in enumerate(cuts[h]):
                arrive(shares.at[k, j, pl.ds(first, count)], rs_recv.at[k, j, c])
        f = 2 * tp + j

        def total_rows(i, carry, j=j, f=f):
            at = pl.multiple_of(i * 128, 128)
            here = pl.ds(pl.multiple_of(low * rows + at, 128), 128)
            total = partial[f, here, :].astype(f32)
            for k in range(3):
                total = total + shares[k, j, pl.ds(at, 128), :].astype(f32)
            value = mixed_all[here, lanes(f * block, block)].astype(f32)
            out[pl.ds(at, 128), j * block:(j + 1) * block] = (
                value + total * (0.5 * vector(2, j * block, block))).astype(half)
            return carry
        lax.fori_loop(0, rows // 128, total_rows, 0)


def fits(nfs, ntp, stream, gate, pool_in):
    ny, nz = fs_grid(nfs)
    tiles = gate.shape[1] // 128
    return (
        (ny, nz, ntp) == (2, 4, 4) and gate.shape[1] % 128 == 0 and tiles % 2 == 1 and tiles > 1
        and stream.shape[0] % SEQ == 0 and stream.shape[0] > SEQ and SEQ % 128 == 0 and pool_in.shape[1] % 128 == 0
        and gate.shape[0] % 128 == 0 and stream.shape[1] == 2 * gate.shape[0]
    )


def whole_layer(stream, weights, vectors):
    gate, up, down, pool_in, pool_out = weights
    rows, width = stream.shape
    block, units = gate.shape
    chans = pool_in.shape[1]
    features = 4 * width
    small = (units // 128 // 2) * 128
    extra = units - 2 * small
    big = small + extra
    every = 2 * rows
    f32, half = jnp.float32, jnp.bfloat16
    vmem = pl.BlockSpec(memory_space=pltpu.VMEM)
    hbm = pl.BlockSpec(memory_space=pltpu.HBM)
    dma = pltpu.SemaphoreType.DMA
    return pl.pallas_call(
        functools.partial(layer_kernel, (rows, small, extra)),
        name="whole_layer",
        out_shape=jax.ShapeDtypeStruct((rows, width), half),
        in_specs=[hbm] * (1 + len(weights) + len(vectors)),
        out_specs=vmem,
        scratch_shapes=[pltpu.VMEM((1, sum(v.shape[0] for v in vectors)), f32)] + [
            pltpu.VMEM(w.shape, half) for w in weights] + [pltpu.VMEM(w.shape, f32) for w in weights] + [
            pltpu.VMEM((features, big), half), pltpu.VMEM((features, big), half), pltpu.VMEM((big, features), half),
            pltpu.VMEM((features, 4 * chans), half), pltpu.VMEM((4 * chans, features), half),
            pltpu.VMEM((4, 1, chans + 2 * width), f32),
            pltpu.VMEM((every, features), half), pltpu.VMEM((every, features), half),
            pltpu.VMEM((every, features), half), pltpu.VMEM((every, features), half),
            pltpu.VMEM((every, big), f32), pltpu.VMEM((every, big), f32), pltpu.VMEM((every, big), half),
            pltpu.VMEM((rows, 4 * chans), half),
            pltpu.VMEM((8, every, block), half), pltpu.VMEM((2, 4, every, block), half),
            pltpu.VMEM((3, 2, rows, block), half), pltpu.VMEM((2, 4, rows, block), half),
            dma((5,)), dma((len(vectors),)), dma((13,)), dma((4, 3, 3)), dma((4, 3, 3)), dma((8, 3, 3)),
            dma((2, 4)), dma((2, 4)), dma((2, 8)), dma((2, 3)), dma((2, 4)),
            dma((3,)), dma((4,)), dma((2, 2, 7)), dma((2, 2, 4, 2)),
            dma((8, 2)), dma((4, 2)), dma((8, 2, 2)), dma((4, 2, 2)), dma((4, 3, 2)), dma((3, 2, 2)),
            dma((4, 5)), dma((4, 3)), dma((4, 2)),
        ],
        compiler_params=pltpu.CompilerParams(
            collective_id=0, has_side_effects=True, vmem_limit_bytes=54 << 20),
    )(stream, *weights, *vectors)


def body(
    nfs, ntp,
    stream, gain_first, gain_mixer, gain_second,
    gate_weight, gate_scale, up_weight, up_scale, down_weight, down_scale,
    pool_in_weight, pool_in_scale, pool_out_weight, pool_out_scale,
):
    half = jnp.bfloat16
    if fits(nfs, ntp, stream, gate_weight, pool_in_weight):
        return whole_layer(
            stream, (gate_weight, up_weight, down_weight, pool_in_weight, pool_out_weight),
            (pool_in_scale, pool_out_scale, down_scale, gain_first, gain_mixer, gain_second, gate_scale, up_scale))
    in_half, out_half = pool_in_weight.astype(half), pool_out_weight.astype(half)
    width, channels = stream.shape[1], in_half.shape[1]
    scales = jnp.concatenate([pool_in_scale, pool_out_scale]).reshape(1, -1)
    in_all, out_all, gate_all, up_all, down_all, stream_all, scales_all = gather_all(
        nfs, ntp, in_half, out_half, gate_weight.astype(half), up_weight.astype(half), down_weight.astype(half),
        stream, scales,
    )
    in_whole, out_whole = flat(in_all), flat(out_all)
    gate_whole, up_whole, down_whole = flat(gate_all), flat(up_all), flat(down_all)
    in_scale = scales_all[:, 0, :channels].reshape(-1)
    out_scale = scales_all[:, 0, channels:].reshape(-1)
    tp = lax.axis_index("tp")

    def feed_forward(rows):
        gate_sum = jnp.dot(rows, gate_whole, preferred_element_type=jnp.float32) * gate_scale
        up_sum = jnp.dot(rows, up_whole, preferred_element_type=jnp.float32) * up_scale
        hidden = (jax.nn.silu(gate_sum) * up_sum).astype(half)
        return jnp.dot(hidden, down_whole, preferred_element_type=jnp.float32).astype(half)

    first = rms(flat(stream_all).astype(jnp.float32), gain_first)
    after_first = summed(ntp, True, 1, feed_forward(first), stream, down_scale)
    mixer_normed = rms(after_first.astype(jnp.float32), gain_mixer)
    pool_input = (
        jnp.dot(mixer_normed, in_whole, preferred_element_type=jnp.float32) * in_scale
    ).astype(half)
    mixed = jnp.dot(pooling(pool_input), out_whole, preferred_element_type=jnp.float32)
    after_mix = (after_first.astype(jnp.float32) + mixed * out_scale).astype(half)
    second = rms(after_mix.astype(jnp.float32), gain_second)
    own = lax.dynamic_slice_in_dim(after_mix, tp * stream.shape[1], stream.shape[1], axis=1)
    return summed(ntp, False, 2, feed_forward(second), own, down_scale)


def solution(mesh):
    placed = (
        P("fs", "tp"), P(), P(), P(),
        P("fs", "tp"), P("tp"), P("fs", "tp"), P("tp"), P("tp", "fs"), P("tp"),
        P("fs", "tp"), P("tp"), P("tp", "fs"), P("tp"),
    )
    return jax.shard_map(
        functools.partial(body, mesh.shape["fs"], mesh.shape["tp"]),
        mesh=mesh, in_specs=placed, out_specs=P("fs", "tp"), check_vma=False,
    )
```
